32 devices in a mesh: dp: 4 (over y, x), kv: 4 (over z), tp: 2 (over core).
Axes of the slice: x: 2, y: 2, z: 4, core: 2. Of those that a mesh axis runs over, the one named last changes fastest.
Arguments:
- tokens: bfloat16 [256, 2048], P('dp', ('kv', 'tp')), parts along dimension 0, may hold values from -64 to 64, as said below
- lengths: int32 [32], P(('dp', 'kv', 'tp')), parts along dimension 0, may hold values from 1 to 8, 28 in all
- state: float32 [32, 16, 128, 128], P(('dp', 'kv', 'tp')), parts along dimension 0, may hold values from -1.8 to 1.8
- gain_first: float32 [2048], replicated, may hold values from 0.1 to 1.9
- first_gate: bfloat16 [2048, 5632], P(None, 'kv'), may hold values from -0.125 to 0.125
- first_up: bfloat16 [2048, 5632], P(None, 'kv'), may hold values from -0.125 to 0.125
- first_down: bfloat16 [5632, 2048], P('kv'), may hold values from -0.109375 to 0.109375
- gain_mix: float32 [2048], replicated, may hold values from 0.1 to 1.9
- query_weight: bfloat16 [2048, 2048], P(None, ('kv', 'tp')), may hold values from -0.125 to 0.125
- key_weight: bfloat16 [2048, 2048], P(None, ('kv', 'tp')), may hold values from -0.125 to 0.125
- value_weight: bfloat16 [2048, 2048], P(None, ('kv', 'tp')), may hold values from -0.125 to 0.125
- gating_weight: bfloat16 [2048, 2048], P(None, ('kv', 'tp')), may hold values from -0.125 to 0.125
- write_weight: bfloat16 [2048, 16], replicated, may hold values from -0.125 to 0.125
- forget_weight: bfloat16 [2048, 16], replicated, may hold values from -0.125 to 0.125
- forget_rate: float32 [16], replicated, may hold values from -4 to 1.5
- out_weight: bfloat16 [2048, 2048], P(None, ('kv', 'tp')), may hold values from -0.125 to 0.125
- gain_second: float32 [2048], replicated, may hold values from 0.1 to 1.9
- second_gate: bfloat16 [2048, 5632], P(None, 'kv'), may hold values from -0.125 to 0.125
- second_up: bfloat16 [2048, 5632], P(None, 'kv'), may hold values from -0.125 to 0.125
- second_down: bfloat16 [5632, 2048], P('kv'), may hold values from -0.109375 to 0.109375
Outputs:
- mixed_out: bfloat16 [256, 2048], P('dp', ('kv', 'tp')), parts along dimension 0
- new_state: float32 [32, 16, 128, 128], P(('dp', 'kv', 'tp')), parts along dimension 0
The draws below stay inside these ranges and needn't reach their ends.
There are 4 independent parts, one for each index of `dp`. The reference program is written for one: setup_inputs(seed, part) draws one part's arguments, and reference() takes and returns one part's arrays. A program takes and returns all parts, laid end to end along the dimension named above; an argument that names none is the same for every part. Nothing has to cross between parts.
Inputs may be any that keep to these rules, and one draw needn't show every extreme that they name: Activations of the new tokens. `lengths`: the live new tokens of each sequence; within each independent group of 8 sequences (one part along dp) they sum to seven halves of 8, rounded down, and some sequence of each group has all 8 live.
All inputs are finite; a program needn't handle non-finite values.
Results may differ from the reference program's by a relative error of at most 0.0058.
Values may be sent and summed in bfloat16 or wider, within the bound.
A program may use at most 128 MiB of HBM per device.

```python
import math
import jax
import jax.numpy as jnp
import numpy as np
from jax import lax

D = 2048
HEADS = 16
HEAD = 128
FF = 5632
BLK = 8
SEQS = 8
ROWS = 64


def draw_tokens(key, part):
    key_base = jax.random.fold_in(key, 17)
    key_one, key_two, key_three = jax.random.split(key_base, 3)
    columns = jnp.arange(D, dtype=jnp.float32)
    rough_cols = jnp.exp(jax.random.uniform(key_two, (1, D), jnp.float32, -0.35, 0.35))
    col_scale = jnp.exp(math.log(5.0) * (columns[None, :] / D - 0.5)) * rough_cols
    base = jnp.clip(jax.random.normal(key_one, (ROWS, D), jnp.float32), -5.0, 5.0)
    row_scale = jnp.exp(jax.random.uniform(key_three, (ROWS, 1), jnp.float32, math.log(0.4), math.log(4.0)))
    return (base * row_scale * col_scale).astype(jnp.bfloat16)


def spiked(array, key, source, target, blocks, factor):
    owner, partner = [(jnp.arange(array.shape[position]) // (array.shape[position] // blocks)).reshape([-1 if axis == position else 1 for axis in range(array.ndim)]) for position in (source, target)]
    chosen = jax.random.permutation(key, blocks)[partner]
    strong = (owner == chosen) | (owner == (partner + blocks // 2) % blocks)
    return jnp.where(strong, factor * array, array)


def steps_of(own_key, dims, pieces, smallest, high):
    level = 1.0
    for axis_at, parts in pieces:
        heights = jax.random.uniform(jax.random.fold_in(jax.random.fold_in(own_key, 6), axis_at), (parts,), jnp.float32, smallest / len(pieces), high / len(pieces))
        level = level * jnp.repeat(jnp.exp(heights), dims[axis_at] // parts).reshape((-1,) + (1,) * (len(dims) - 1 - axis_at))
    return level


def profile(count, total, most, skew):
    loads = [(1 << 20) // math.isqrt(standing ** skew) + 1 for standing in range(2, count + 1)]
    spare, given = total - most - (count - 1), [1] * (count - 1)
    while spare > 0:
        free = [i for i in range(count - 1) if given[i] < most]
        whole, left = sum([loads[i] for i in free]), spare
        for i in free:
            addition = min(most - given[i], max(1, left * loads[i] // whole), spare)
            given[i] = given[i] + addition
            spare = spare - addition
    return np.array([most] + given)


def uneven_parts(stream_key, number_of, total, most, slope):
    if number_of == 2:
        one = jax.random.randint(stream_key, (), max(1, total - most), min(most, total - 1) + 1)
        return jnp.stack([one, total - one])
    tallies = jnp.asarray(profile(number_of, total, most, slope), jnp.int32)
    pairs = (number_of - 1) // 2
    source_of, taker = tallies[1:1 + 2 * pairs:2], tallies[2:2 + 2 * pairs:2]
    slack = jnp.minimum(source_of - 1, most - taker)
    passed = jax.random.randint(jax.random.fold_in(stream_key, 1), (pairs,), 0, 1 << 20) % (slack + 1)
    tallies = tallies.at[1:1 + 2 * pairs:2].set(source_of - passed).at[2:2 + 2 * pairs:2].set(taker + passed)
    return tallies[jax.random.permutation(jax.random.fold_in(stream_key, 2), number_of)]


def gaussian(own_key, extent, spread, most, shards=(), kind=jnp.bfloat16):
    loudness = steps_of(own_key, extent, shards, -0.22, 0.18) if shards else 1.0
    values = jax.random.normal(own_key, extent, jnp.float32) * spread * loudness
    return jnp.minimum(jnp.maximum(values, -most), most).astype(kind)


def gaussian_with(stream_key, shape, scale, most, cuts, heavy, held_as=jnp.bfloat16):
    values = scale * jax.random.normal(stream_key, shape, jnp.float32)
    if cuts:
        values = values * steps_of(stream_key, shape, cuts, -0.22, 0.18)
    return jnp.clip(spiked(values, jax.random.fold_in(stream_key, 3), *heavy), -most, most).astype(held_as)


def setup_inputs(seed: int = 0, part: int = 0) -> dict:
    keys = jax.random.split(jax.random.key(seed), 21)
    part_splits = jax.random.split(jax.random.fold_in(keys[20], part), 21)
    tokens = draw_tokens(jax.random.fold_in(jax.random.fold_in(keys[20], part), 71), part)
    lengths = uneven_parts(part_splits[1], SEQS, SEQS * 7 // 2, BLK, 2).astype(jnp.int32)
    state = gaussian(part_splits[2], (SEQS, HEADS, HEAD, HEAD), 0.3, 1.8, ((0, 8),), jnp.float32)
    gain_first = jnp.clip(1.0 + 0.18 * jax.random.normal(keys[3], (D,), jnp.float32), 0.1, 1.9)
    first_gate = gaussian(keys[4], (D, FF), D ** -0.5, 0.125, ((1, 4),))
    first_up = gaussian(keys[5], (D, FF), D ** -0.5, 0.125, ((1, 4),))
    first_down = gaussian_with(keys[6], (FF, D), FF ** -0.5, 0.109375, ((0, 4),), (0, 1, 4, 2.0))
    gain_mix = jnp.clip(1.0 + 0.18 * jax.random.normal(keys[7], (D,), jnp.float32), 0.1, 1.9)
    query_weight = gaussian(keys[8], (D, HEADS * HEAD), D ** -0.5, 0.125, ((1, 8),))
    key_weight = gaussian(keys[9], (D, HEADS * HEAD), D ** -0.5, 0.125, ((1, 8),))
    value_weight = gaussian(keys[10], (D, HEADS * HEAD), D ** -0.5, 0.125, ((1, 8),))
    gating_weight = gaussian(keys[11], (D, HEADS * HEAD), D ** -0.5, 0.125, ((1, 8),))
    write_weight = gaussian(keys[12], (D, HEADS), D ** -0.5, 0.125)
    forget_weight = gaussian(keys[13], (D, HEADS), D ** -0.5, 0.125)
    forget_rate = jnp.clip(jax.random.uniform(keys[14], (HEADS,), jnp.float32, -4.0, 1.5), -4.0, 1.5)
    out_weight = gaussian(keys[15], (HEADS * HEAD, D), (HEADS * HEAD) ** -0.5, 0.125, ((1, 8),))
    gain_second = jnp.clip(1.0 + 0.18 * jax.random.normal(keys[16], (D,), jnp.float32), 0.1, 1.9)
    second_gate = gaussian(keys[17], (D, FF), D ** -0.5, 0.125, ((1, 4),))
    second_up = gaussian(keys[18], (D, FF), D ** -0.5, 0.125, ((1, 4),))
    second_down = gaussian_with(keys[19], (FF, D), FF ** -0.5, 0.109375, ((0, 4),), (0, 1, 4, 2.0))
    return {"tokens": tokens, "lengths": lengths, "state": state, "gain_first": gain_first, "first_gate": first_gate, "first_up": first_up, "first_down": first_down, "gain_mix": gain_mix, "query_weight": query_weight, "key_weight": key_weight, "value_weight": value_weight, "gating_weight": gating_weight, "write_weight": write_weight, "forget_weight": forget_weight, "forget_rate": forget_rate, "out_weight": out_weight, "gain_second": gain_second, "second_gate": second_gate, "second_up": second_up, "second_down": second_down}


EPSILON = 1e-06

def feed_forward(hidden_in, gain, w_gate, w_up, w_down):
    values = hidden_in.astype(jnp.float32)
    row_scale = lax.rsqrt(lax.optimization_barrier(jnp.mean(values * values, axis=1, keepdims=True)) + EPSILON)
    scaled = (values * gain).astype(jnp.bfloat16)
    gate_act = jnp.dot(scaled, w_gate, preferred_element_type=jnp.float32) * row_scale
    up_act = jnp.dot(scaled, w_up, preferred_element_type=jnp.float32) * row_scale
    hidden = (jax.nn.silu(gate_act) * up_act).astype(jnp.bfloat16)
    result = jnp.dot(hidden, w_down, preferred_element_type=jnp.float32)
    return (values + 0.5 * result).astype(jnp.bfloat16)

def delta_block(query, key_in, value, gating, write_pre, forget_pre, rates, live, state):
    seq_count, block_len, head_count, head_size = query.shape
    precise = lax.Precision.HIGHEST
    query_unit = query * lax.rsqrt(lax.optimization_barrier(jnp.sum(query * query, axis=-1, keepdims=True)) + EPSILON) / math.sqrt(head_size)
    key_unit = key_in * lax.rsqrt(lax.optimization_barrier(jnp.sum(key_in * key_in, axis=-1, keepdims=True)) + EPSILON)
    live_rows = live[:, :, None]
    write_gate = jax.nn.sigmoid(write_pre) * live_rows
    forget = -jnp.exp(rates)[None, None, :] * jax.nn.softplus(forget_pre) * live_rows
    cumulative = jnp.cumsum(forget, axis=1)
    cum_heads = jnp.transpose(cumulative, (0, 2, 1))
    positions = jnp.arange(block_len)
    causal = positions[:, None] >= positions[None, :]
    strict = positions[:, None] > positions[None, :]
    differ = jnp.minimum(cum_heads[:, :, :, None] - cum_heads[:, :, None, :], 0.0)
    decay_mat = jnp.where(causal, jnp.exp(differ), 0.0)
    key_dots = jnp.einsum('sthd,suhd->shtu', key_unit, key_unit, precision=precise)
    write_heads = jnp.transpose(write_gate, (0, 2, 1))
    strict_part = jnp.where(strict, write_heads[:, :, :, None] * decay_mat * key_dots, 0.0)
    identity = jnp.eye(block_len, dtype=jnp.float32)
    squared = jnp.einsum('shtu,shuv->shtv', strict_part, strict_part, precision=precise)
    fourth = jnp.einsum('shtu,shuv->shtv', squared, squared, precision=precise)
    inverse = jnp.einsum('shtu,shuv->shtv', identity - strict_part, identity + squared, precision=precise)
    inverse = jnp.einsum('shtu,shuv->shtv', inverse, identity + fourth, precision=precise)
    growth = jnp.exp(cumulative)
    target = jnp.einsum('shtu,suhv->sthv', inverse, write_gate[..., None] * value, precision=precise)
    key_mix = jnp.einsum('shtu,suhk->sthk', inverse, (write_gate * growth)[..., None] * key_unit, precision=precise)
    update = target - jnp.einsum('sthk,shkv->sthv', key_mix, state, precision=precise)
    scores = jnp.einsum('sthd,suhd->shtu', query_unit, key_unit, precision=precise) * decay_mat
    attend = jnp.einsum('sthk,shkv->sthv', query_unit * growth[..., None], state, precision=precise)
    attend = attend + jnp.einsum('shtu,suhv->sthv', scores, update, precision=precise)
    final_cum = cumulative[:, -1:, :]
    fading = jnp.exp(final_cum - cumulative)
    new_state = jnp.exp(final_cum[:, 0, :])[:, :, None, None] * state
    new_state = new_state + jnp.einsum('sthk,sthv->shkv', key_unit * fading[..., None], update, precision=precise)
    normed = attend * lax.rsqrt(lax.optimization_barrier(jnp.mean(attend * attend, axis=-1, keepdims=True)) + EPSILON)
    normed = normed * jax.nn.silu(gating) * live[:, :, None, None]
    mixed_heads = normed.reshape(seq_count * block_len, head_count * head_size).astype(jnp.bfloat16)
    return (mixed_heads, new_state)

def reference(tokens, lengths, state, gain_first, first_gate, first_up, first_down, gain_mix, query_weight, key_weight, value_weight, gating_weight, write_weight, forget_weight, forget_rate, out_weight, gain_second, second_gate, second_up, second_down):
    after_first = feed_forward(tokens, gain_first, first_gate, first_up, first_down)
    values = after_first.astype(jnp.float32)
    mix_scale = lax.rsqrt(lax.optimization_barrier(jnp.mean(values * values, axis=1, keepdims=True)) + EPSILON)
    mix_in = (values * gain_mix).astype(jnp.bfloat16)

    def project(matrix):
        return jnp.dot(mix_in, matrix, preferred_element_type=jnp.float32) * mix_scale
    query = project(query_weight).reshape(SEQS, BLK, HEADS, HEAD)
    key_in = project(key_weight).reshape(SEQS, BLK, HEADS, HEAD)
    value = project(value_weight).reshape(SEQS, BLK, HEADS, HEAD)
    gating = project(gating_weight).reshape(SEQS, BLK, HEADS, HEAD)
    write_pre = project(write_weight).reshape(SEQS, BLK, HEADS)
    forget_pre = project(forget_weight).reshape(SEQS, BLK, HEADS)
    positions = jnp.arange(BLK, dtype=jnp.int32)
    live = (positions[None, :] < lengths[:, None]).astype(jnp.float32)
    mixed_heads, new_state = delta_block(query, key_in, value, gating, write_pre, forget_pre, forget_rate, live, state)
    half_cols = HEADS * HEAD // 2
    running = values
    for half_index in range(2):
        portion = jnp.dot(mixed_heads[:, half_index * half_cols:(half_index + 1) * half_cols], out_weight[half_index * half_cols:(half_index + 1) * half_cols], preferred_element_type=jnp.float32)
        rounded = lax.optimization_barrier(portion.astype(jnp.bfloat16)).astype(jnp.float32)
        running = running + rounded
    after_mix = running.astype(jnp.bfloat16)
    mixed_out = feed_forward(after_mix, gain_second, second_gate, second_up, second_down)
    return (mixed_out, new_state)
```

```python
import functools
import math

import jax
import jax.numpy as jnp
from jax import lax
from jax.experimental import pallas as pl
from jax.experimental.pallas import tpu as pltpu
from jax.sharding import PartitionSpec as P

HEADS = 16
HEAD = 128
BLK = 8


EPSILON = 1e-06


def fold_step(gain, gate_cols, up_cols, portion):
    values = portion.astype(jnp.float32)
    scaled = (values * gain).astype(jnp.bfloat16)
    gate_acc = jnp.dot(scaled, gate_cols, preferred_element_type=jnp.float32)
    up_acc = jnp.dot(scaled, up_cols, preferred_element_type=jnp.float32)
    squares = jnp.sum(values * values, axis=1)
    return (gate_acc, up_acc, squares)


def finish_units(gate_acc, up_acc, squares, channels, down_rows):
    row_scale = lax.rsqrt(squares / channels + EPSILON)[:, None]
    hidden = (jax.nn.silu(gate_acc * row_scale) * (up_acc * row_scale)).astype(jnp.bfloat16)
    return jnp.dot(hidden, down_rows, preferred_element_type=jnp.float32)


def feed_forward(hidden_in, gain, w_gate, w_up, w_down):
    channels = gain.shape[0]
    paired = lax.all_to_all(hidden_in, "tp", split_axis=0, concat_axis=1, tiled=True)
    gate_acc, up_acc, squares = fold_step(
        gain, w_gate, w_up, lax.all_gather(paired, "kv", axis=1, tiled=True)
    )
    ffn_term = finish_units(gate_acc, up_acc, squares, channels, w_down)
    partial_value = lax.psum_scatter(ffn_term, "kv", scatter_dimension=1, tiled=True)
    summed = lax.all_to_all(partial_value, "tp", split_axis=1, concat_axis=0, tiled=True)
    return (hidden_in.astype(jnp.float32) + 0.5 * summed).astype(jnp.bfloat16)


def delta_block(query, key_in, value, gating, write_pre, forget_pre, rates, live, state):
    seq_count, block_len, head_count, head_size = query.shape
    precise = lax.Precision.HIGHEST
    query_unit = (
        query
        * lax.rsqrt(jnp.sum(query * query, axis=-1, keepdims=True) + EPSILON)
        / math.sqrt(head_size)
    )
    key_unit = key_in * lax.rsqrt(jnp.sum(key_in * key_in, axis=-1, keepdims=True) + EPSILON)
    live_rows = live[:, :, None]
    write_gate = jax.nn.sigmoid(write_pre) * live_rows
    forget = -jnp.exp(rates)[None, None, :] * jax.nn.softplus(forget_pre) * live_rows
    cumulative = jnp.cumsum(forget, axis=1)
    cum_heads = jnp.transpose(cumulative, (0, 2, 1))
    positions = jnp.arange(block_len)
    causal = positions[:, None] >= positions[None, :]
    strict = positions[:, None] > positions[None, :]
    differ = jnp.minimum(cum_heads[:, :, :, None] - cum_heads[:, :, None, :], 0.0)
    decay_mat = jnp.where(causal, jnp.exp(differ), 0.0)
    key_dots = jnp.einsum("sthd,suhd->shtu", key_unit, key_unit, precision=precise)
    write_heads = jnp.transpose(write_gate, (0, 2, 1))
    strict_part = jnp.where(strict, write_heads[:, :, :, None] * decay_mat * key_dots, 0.0)
    identity = jnp.eye(block_len, dtype=jnp.float32)
    squared = jnp.einsum("shtu,shuv->shtv", strict_part, strict_part, precision=precise)
    fourth = jnp.einsum("shtu,shuv->shtv", squared, squared, precision=precise)
    inverse = jnp.einsum(
        "shtu,shuv->shtv", identity - strict_part, identity + squared, precision=precise
    )
    inverse = jnp.einsum("shtu,shuv->shtv", inverse, identity + fourth, precision=precise)
    growth = jnp.exp(cumulative)
    target = jnp.einsum(
        "shtu,suhv->sthv", inverse, write_gate[..., None] * value, precision=precise
    )
    key_mix = jnp.einsum(
        "shtu,suhk->sthk", inverse, (write_gate * growth)[..., None] * key_unit, precision=precise
    )
    update = target - jnp.einsum("sthk,shkv->sthv", key_mix, state, precision=precise)
    scores = jnp.einsum("sthd,suhd->shtu", query_unit, key_unit, precision=precise) * decay_mat
    attend = jnp.einsum("sthk,shkv->sthv", query_unit * growth[..., None], state, precision=precise)
    attend = attend + jnp.einsum("shtu,suhv->sthv", scores, update, precision=precise)
    final_cum = cumulative[:, -1:, :]
    fading = jnp.exp(final_cum - cumulative)
    new_state = jnp.exp(final_cum[:, 0, :])[:, :, None, None] * state
    new_state = new_state + jnp.einsum(
        "sthk,sthv->shkv", key_unit * fading[..., None], update, precision=precise
    )
    normed = attend * lax.rsqrt(jnp.mean(attend * attend, axis=-1, keepdims=True) + EPSILON)
    normed = normed * jax.nn.silu(gating) * live[:, :, None, None]
    mixed_heads = normed.reshape(seq_count * block_len, head_count * head_size).astype(jnp.bfloat16)
    return (mixed_heads, new_state)


def per_device(
    tokens,
    lengths,
    state,
    gain_first,
    first_gate,
    first_up,
    first_down,
    gain_mix,
    query_weight,
    key_weight,
    value_weight,
    gating_weight,
    write_weight,
    forget_weight,
    forget_rate,
    out_weight,
    gain_second,
    second_gate,
    second_up,
    second_down,
):
    after_first = feed_forward(tokens, gain_first, first_gate, first_up, first_down)
    seq_count = lengths.shape[0]
    own_count = seq_count * BLK
    whole_rows = lax.all_gather(after_first, ("kv", "tp"), axis=1, tiled=True)
    scaled_all = (whole_rows.astype(jnp.float32) * gain_mix).astype(jnp.bfloat16)
    stacked = jnp.stack(
        [
            jnp.dot(scaled_all, matrix, preferred_element_type=jnp.float32)
            for matrix in (query_weight, key_weight, value_weight, gating_weight)
        ]
    )
    owned = lax.all_to_all(
        stacked.astype(jnp.bfloat16), ("kv", "tp"), split_axis=1, concat_axis=2, tiled=True
    ).astype(stacked.dtype)
    row_start = lax.axis_index(("kv", "tp")) * own_count
    own_values = lax.dynamic_slice_in_dim(whole_rows, row_start, own_count, 0).astype(jnp.float32)
    own_scaled = lax.dynamic_slice_in_dim(scaled_all, row_start, own_count, 0)
    mix_scale = lax.rsqrt(jnp.mean(own_values * own_values, axis=1, keepdims=True) + EPSILON)
    query = (owned[0] * mix_scale).reshape(seq_count, BLK, HEADS, HEAD)
    key_in = (owned[1] * mix_scale).reshape(seq_count, BLK, HEADS, HEAD)
    value = (owned[2] * mix_scale).reshape(seq_count, BLK, HEADS, HEAD)
    gating = (owned[3] * mix_scale).reshape(seq_count, BLK, HEADS, HEAD)
    write_pre = (
        jnp.dot(own_scaled, write_weight, preferred_element_type=jnp.float32) * mix_scale
    ).reshape(seq_count, BLK, HEADS)
    forget_pre = (
        jnp.dot(own_scaled, forget_weight, preferred_element_type=jnp.float32) * mix_scale
    ).reshape(seq_count, BLK, HEADS)
    positions = jnp.arange(BLK, dtype=jnp.int32)
    live = (positions[None, :] < lengths[:, None]).astype(jnp.float32)
    mixed_heads, new_state = delta_block(
        query, key_in, value, gating, write_pre, forget_pre, forget_rate, live, state
    )
    half_cols = mixed_heads.shape[1] // 2
    portion = lax.all_gather(mixed_heads, ("kv", "tp"), axis=0, tiled=True)
    first_half = jnp.dot(
        portion[:, :half_cols], out_weight[:half_cols], preferred_element_type=jnp.float32
    ).astype(jnp.bfloat16)
    second_half = jnp.dot(
        portion[:, half_cols:], out_weight[half_cols:], preferred_element_type=jnp.float32
    ).astype(jnp.bfloat16)
    first_half, second_half = lax.optimization_barrier((first_half, second_half))
    mixed_sum = first_half.astype(jnp.float32) + second_half.astype(jnp.float32)
    after_mix = (after_first.astype(jnp.float32) + mixed_sum).astype(jnp.bfloat16)
    mixed_out = feed_forward(after_mix, gain_second, second_gate, second_up, second_down)
    return (mixed_out, new_state)


F32 = jnp.float32
BF16 = jnp.bfloat16
MESH = pl.DeviceIdType.MESH
VMEM_LIMIT = 58 * 1024 * 1024


def fused_kernel(
    kv_size,
    channels,
    tokens_hbm,
    lengths_hbm,
    gains1_hbm,
    gains_mix_hbm,
    gains2_hbm,
    rates_hbm,
    state_hbm,
    gate1_hbm,
    up1_hbm,
    down1_hbm,
    query_hbm,
    key_hbm,
    value_hbm,
    gating_hbm,
    write_hbm,
    forget_hbm,
    out_hbm,
    gate2_hbm,
    up2_hbm,
    down2_hbm,
    mixed_out_ref,
    state_out,
    units1,
    down1,
    units2,
    down2,
    proj,
    out_w,
    small_w,
    state,
    state_high,
    state_low,
    gains1_ref,
    gains_mix_ref,
    gains2_ref,
    rates_ref,
    tokens_ref,
    length_ref,
    lens_all,
    picked,
    entered,
    unit_acc,
    live_acc,
    dead_acc,
    proj_acc,
    small_acc,
    middle,
    second_in,
    heads_send,
    heads_recv,
    red_send,
    red_recv,
    part_send,
    part_recv,
    small_recv,
    fin_send,
    fin_recv,
    own_send,
    own_recv,
    load_sems,
    send_sems,
    recv_sems,
):
    kv = lax.axis_index("kv")
    tp = lax.axis_index("tp")
    devices = 2 * kv_size
    me = kv * 2 + tp
    cls = lax.rem(kv + tp, 2)
    rows, cols = tokens_ref.shape
    wide = 2 * cols
    slots = BLK // 2
    half = rows // 2
    pack = rows // 4
    hidden_local = gate1_hbm.shape[1]
    own_cols = pl.ds(pl.multiple_of(tp * cols, cols), cols)
    far_first = list(range(kv_size - 1, 0, -1))

    loads = {}

    def load(name, src, dst):
        loads[name] = pltpu.make_async_copy(src, dst, load_sems.at[len(loads)])

    def swapped(off):
        chip, bit = kv, 1
        while bit < kv_size:
            if off & bit:
                chip = chip + bit - 2 * bit * lax.rem(kv // bit, 2)
            bit *= 2
        return chip

    def core_of(chip, other):
        return lax.rem(chip + cls + other, 2)

    def chip_rows(chip):
        return pl.ds(pl.multiple_of(chip * wide, wide), wide)

    load("length", lengths_hbm, length_ref)
    load("tokens", tokens_hbm, tokens_ref)
    load("gains1", gains1_hbm, gains1_ref)
    for off in range(kv_size):
        at = chip_rows(swapped(off))
        load(f"gate1{off}", gate1_hbm.at[at, :], units1.at[at, 0:hidden_local])
        load(f"up1{off}", up1_hbm.at[at, :], units1.at[at, hidden_local : 2 * hidden_local])
    early = list(loads)
    load("down1", down1_hbm, down1)
    for kind, ref in enumerate((query_hbm, key_hbm, value_hbm, gating_hbm)):
        at = pl.ds(pl.multiple_of(kind * wide + tp * cols, cols), cols)
        load(f"proj{kind}", ref, proj.at[:, at])
    load("write", write_hbm, small_w.at[0:HEADS])
    load("forget", forget_hbm, small_w.at[HEADS : 2 * HEADS])
    load("gains_mix", gains_mix_hbm, gains_mix_ref)
    load("rates", rates_hbm, rates_ref)
    load("out", out_hbm, out_w.at[:, own_cols])
    load("state", state_hbm.at[0], state)
    load("gains2", gains2_hbm, gains2_ref)
    load("gate2", gate2_hbm, units2.at[:, 0:hidden_local])
    load("up2", up2_hbm, units2.at[:, hidden_local : 2 * hidden_local])
    load("down2", down2_hbm, down2)
    late = [name for name in loads if name not in early]
    for name in early[:2]:
        loads[name].start()

    barrier = pltpu.get_barrier_semaphore()
    for off in range(1, devices):
        peer = lax.rem(me + off, devices)
        pl.semaphore_signal(
            barrier,
            inc=1,
            device_id={"kv": peer // 2, "tp": lax.rem(peer, 2)},
            device_id_type=MESH,
        )
    for name in early[2:]:
        loads[name].start()

    sent = []
    used = [0]

    def remote(src, dst, chip, core):
        copy = pltpu.make_async_remote_copy(
            src_ref=src,
            dst_ref=dst,
            send_sem=send_sems.at[used[0]],
            recv_sem=recv_sems.at[used[0]],
            device_id={"kv": chip, "tp": core},
            device_id_type=MESH,
        )
        used[0] += 1
        copy.start()
        sent.append(copy)
        return copy

    def to_class(src, dst):
        copies = {}
        for off in far_first:
            chip = swapped(off)
            copies[off] = remote(src(off), dst(off), chip, core_of(chip, 0))
        return copies

    def to_all(src, dst):
        copies = {}
        for off in far_first + [0]:
            chip = swapped(off)
            for other in (0, 1):
                if off or other:
                    core = core_of(chip, other)
                    copies[off, other] = remote(
                        src(off, other, chip * 2 + core), dst(off, other), chip, core
                    )
        return copies

    def to_partner(src, dst):
        return remote(src, dst, kv, 1 - tp)

    def iota(shape, axis):
        return lax.broadcasted_iota(jnp.int32, shape, axis)

    def dot(a, b):
        return jnp.dot(a, b, preferred_element_type=F32)

    def one_hot(mask):
        return jnp.where(mask, 1.0, 0.0).astype(BF16)

    row = iota((rows, rows), 0)
    col = iota((rows, rows), 1)
    at_class = lax.rem(row, half)
    at_seq = at_class // slots
    which = lax.rem(cls + row // half + at_seq, 2)
    picks = one_hot(col == at_seq * BLK + 2 * lax.rem(at_class, slots) + which)
    small_w[2 * HEADS :] = jnp.zeros((HEAD - 2 * HEADS, channels), BF16)
    with jax.named_scope("small_wait"):
        loads["length"].wait()
        loads["tokens"].wait()
    lens_all[me] = jnp.broadcast_to(length_ref[...], (1, HEAD))
    chosen = dot(picks, tokens_ref[...]).astype(BF16)
    picked[...] = chosen.reshape(2, half, cols)
    entered[me] = chosen[:half]
    with jax.named_scope("barrier"):
        pl.semaphore_wait(barrier, devices - 1)
    len_copies = to_all(lambda off, other, peer: lens_all.at[me], lambda off, other: lens_all.at[me])
    copies = to_all(lambda off, other, peer: picked.at[other], lambda off, other: entered.at[me])
    for name in late:
        loads[name].start()

    def ffn_slot(acc, units, gain_ref, chip, portion, first):
        at = chip_rows(chip)
        values = portion.astype(F32)
        scaled = (values * gain_ref[:, at]).astype(BF16)
        term = dot(scaled, units[at, :])
        if first:
            acc[...] = term
        else:
            acc[...] += term
        return jnp.sum(values * values, axis=1, keepdims=True)

    def finish(acc, squares):
        row_scale = lax.rsqrt(squares / channels + EPSILON)
        gate = acc[:, 0:hidden_local] * row_scale
        up = acc[:, hidden_local : 2 * hidden_local] * row_scale
        return (jax.nn.silu(gate) * up).astype(BF16)

    def lengths_by(seq):
        found = jnp.zeros(seq.shape, jnp.int32)
        for index in range(devices):
            found = jnp.where(seq == index, lens_all[index], found)
        return found

    def is_live(seq, slot, klass):
        return 2 * slot + lax.rem(klass + seq, 2) < lengths_by(seq)

    def live_column(klass):
        at = iota((half, HEAD), 0)
        return jnp.where(is_live(at // slots, lax.rem(at, slots), klass), 1.0, 0.0)

    def live_row(klass):
        at = iota((1, HEAD), 1)
        live = is_live(at // slots, lax.rem(at, slots), klass) & (at < half)
        return jnp.where(live, 1.0, 0.0)

    def place_lanes(seq, slot, column):
        target = seq * slots + slot
        before = jnp.sum(
            jnp.where(iota((half, HEAD), 0) < target, column, 0.0), axis=0, keepdims=True
        )
        count = jnp.sum(column, axis=0, keepdims=True)
        rest = count + target.astype(F32) - before
        return jnp.where(is_live(seq, slot, cls), before, rest).astype(jnp.int32)

    def place_rows(seq, slot, klass, flags):
        target = seq * slots + slot
        before = jnp.sum(
            jnp.where(iota(seq.shape, 1) < target, flags, 0.0), axis=1, keepdims=True
        )
        count = jnp.sum(flags, axis=1, keepdims=True)
        rest = count + target.astype(F32) - before
        return jnp.where(is_live(seq, slot, klass), before, rest).astype(jnp.int32)

    def chip_tokens(chip):
        return jnp.concatenate([entered[chip * 2], entered[chip * 2 + 1]], axis=1)

    loads["gains1"].wait()
    squares = jnp.zeros((half, 1), F32)
    with jax.named_scope("gather0"):
        for off in range(kv_size):
            for other in (0, 1):
                if off or other:
                    copies[off, other].wait_recv()
            loads[f"gate1{off}"].wait()
            loads[f"up1{off}"].wait()
            chip = swapped(off)
            if off == kv_size - 1:
                with jax.named_scope("order"):
                    for copy in len_copies.values():
                        copy.wait_recv()
                    column = live_column(cls)
                    lane = iota((1, HEAD), 1)
                    place = place_lanes(
                        jnp.minimum(lane // slots, devices - 1), lax.rem(lane, slots), column
                    )
                    reorder = one_hot(iota((half, HEAD), 0) == place)[:, :half]
            squares = squares + ffn_slot(
                unit_acc, units1, gains1_ref, chip, chip_tokens(chip), off == 0
            )
    with jax.named_scope("finish0"):
        hidden = dot(reorder, finish(unit_acc, squares)).astype(BF16)
    with jax.named_scope("down_wait"):
        loads["down1"].wait()
    with jax.named_scope("down0"):
        copies = {}
        for off in far_first + [0]:
            chip = swapped(off)
            own_term = dot(hidden, down1[:, chip_rows(chip)])
            if off:
                red_send[0, off] = own_term[:pack].astype(BF16)
                red_send[1, off] = own_term[pack:].astype(BF16)
                copies[0, off] = remote(
                    red_send.at[0, off], red_recv.at[0, off], chip, core_of(chip, 0)
                )
        for off in far_first:
            chip = swapped(off)
            copies[1, off] = remote(
                red_send.at[1, off], red_recv.at[1, off], chip, core_of(chip, 0)
            )
    with jax.named_scope("exchange"):
        proj_copies = []
        for kind in range(4):
            loads[f"proj{kind}"].wait()
            at = pl.ds(pl.multiple_of(kind * wide + tp * cols, cols), cols)
            proj_copies.append(to_partner(proj.at[:, at], proj.at[:, at]))
        loads["out"].wait()
        out_copy = to_partner(out_w.at[:, own_cols], out_w.at[:, own_cols])
    with jax.named_scope("tables"):
        residual = dot(reorder, chip_tokens(kv))
        flags = live_row(cls)
        other_flags = live_row(1 - cls)
        at = iota((devices * 2 * BLK, HEAD), 0)
        slot = lax.rem(at, slots)
        place = place_rows(at // (2 * BLK), slot, cls, flags)
        kind = lax.rem(at // slots, 4)
        kind = kind + cls * (1 - 2 * lax.rem(kind, 2))
        lane = iota((devices * 2 * BLK, HEAD), 1)
        spread = one_hot(
            (lane // pack == kind) & (lax.rem(lane, pack) == place) & (lane < 4 * pack)
        )[:, : 4 * pack]
        lane = iota((1, devices * 2 * BLK), 1)
        place = place_lanes(lane // (2 * BLK), lax.rem(lane, slots), column)
        at = iota((kv_size * pack, devices * 2 * BLK), 0)
        chip_at = lax.rem(iota((kv_size * pack, devices * 2 * BLK), 1) // slots, kv_size)
        gather_heads = one_hot((at // pack == chip_at) & (lax.rem(at, pack) == place))
        at = iota((BLK, HEAD), 0)
        klass = at // slots
        place = place_rows(
            jnp.zeros((BLK, HEAD), jnp.int32) + me,
            lax.rem(at, slots),
            klass,
            jnp.where(klass == cls, flags, other_flags),
        )
        lane = iota((BLK, HEAD), 1)
        pick_small = jnp.where(
            (lax.rem(lane // pack + cls, 2) == klass)
            & (lax.rem(lane, pack) == place)
            & (lane < 2 * pack),
            1.0,
            0.0,
        )[:, : 2 * pack]
        at = iota((rows, HEAD), 0)
        seq, token = at // BLK, lax.rem(at, BLK)
        klass = lax.rem(seq + token, 2)
        place = place_rows(seq, token // 2, klass, jnp.where(klass == cls, flags, other_flags))
        lane = iota((rows, HEAD), 1)
        restore = one_hot(
            (lax.rem(lane // half + cls, 2) == klass)
            & (lax.rem(lane, half) == place)
            & (lane < rows)
        )[:, :rows]
    with jax.named_scope("statecut"):
        loads["state"].wait()
        for head in range(HEADS):
            high = state[head].astype(BF16)
            state_high[head] = high
            state_low[head] = (state[head] - high.astype(F32)).astype(BF16)
    gathered = []
    for group in range(2):
        with jax.named_scope(f"red0_{group}"):
            at = slice(group * pack, (group + 1) * pack)
            for off in far_first:
                copies[group, off].wait_recv()
            total = own_term[at]
            for off in far_first:
                total = total + red_recv[group, off].astype(F32)
            middle[group, kv] = (residual[at] + 0.5 * total).astype(BF16)
            gathered.append(
                to_class(
                    lambda off: middle.at[group, kv], lambda off: middle.at[group, kv]
                )
            )

    with jax.named_scope("proj_wait"):
        for copy in proj_copies:
            copy.wait_recv()
        for name in ("write", "forget", "gains_mix", "rates"):
            loads[name].wait()
    squares = jnp.zeros((pack, 1), F32)
    with jax.named_scope("gather1"):
        for off in range(kv_size):
            if off:
                gathered[0][off].wait_recv()
            chip = swapped(off)
            at = chip_rows(chip)
            values = middle[0, chip].astype(F32)
            squares = squares + jnp.sum(values * values, axis=1, keepdims=True)
            scaled = (values * gains_mix_ref[:, at]).astype(BF16)
            term = dot(scaled, proj[at, :])
            small_term = lax.dot_general(
                scaled, small_w[:, at], (((1,), (1,)), ((), ())), preferred_element_type=F32
            )
            if off == 0:
                proj_acc[...] = term
                small_acc[0] = small_term
            else:
                proj_acc[...] += term
                small_acc[0] += small_term
    with jax.named_scope("partsend"):
        mix_scale = lax.rsqrt(squares / channels + EPSILON)
        small_acc[0] = small_acc[0] * mix_scale
        small_copy = to_partner(small_acc.at[0], small_recv.at[0])
        projected = (proj_acc[...] * mix_scale).astype(BF16)
        stacked = jnp.concatenate(
            [projected[:, kind * wide : (kind + 1) * wide] for kind in range(4)], axis=0
        )
        part_send[...] = dot(spread, stacked).astype(BF16).reshape(devices, 2 * BLK, wide)
        part_copies = to_all(
            lambda off, other, peer: part_send.at[peer],
            lambda off, other: part_recv.at[kv, cls],
        )
        part_recv[kv, cls] = part_send[me]

    with jax.named_scope("dead_units"):
        loads["gains2"].wait()
        loads["gate2"].wait()
        loads["up2"].wait()
        squares = jnp.zeros((pack, 1), F32)
        for off in range(kv_size):
            if off:
                gathered[1][off].wait_recv()
            chip = swapped(off)
            squares = squares + ffn_slot(
                dead_acc, units2, gains2_ref, chip, middle[1, chip], off == 0
            )
        dead_hidden = finish(dead_acc, squares)

    def cut_terms(a):
        high = a.astype(BF16).astype(F32)
        return high, a - high

    def dot_fine(a, b, across=False):
        high_a, low_a = cut_terms(a)
        high_b, low_b = cut_terms(b)
        axis = 1 if across else 0
        left = jnp.concatenate([high_a, high_a, low_a], axis=1).astype(BF16)
        right = jnp.concatenate([high_b, low_b, high_b], axis=axis).astype(BF16)
        return lax.dot_general(
            left, right, (((1,), (axis,)), ((), ())), preferred_element_type=F32
        )

    with jax.named_scope("premix"):
        small_copy.wait_recv()
        small_all = jnp.concatenate([small_acc[0], small_recv[0]], axis=0)
        high, low = cut_terms(small_all)
        picked_small = dot(pick_small.astype(BF16), high.astype(BF16)) + dot(
            pick_small.astype(BF16), low.astype(BF16)
        )
        write_pre = picked_small[:, 0:HEADS]
        forget_pre = picked_small[:, HEADS : 2 * HEADS]

        size = HEADS * BLK

        def token_of(at):
            at = lax.rem(at, BLK)
            return 2 * lax.rem(at, slots) + lax.rem(at // slots + me, 2)

        row = iota((size, size), 0)
        col = iota((size, size), 1)
        same = (row // BLK) == (col // BLK)
        causal = same & (token_of(row) >= token_of(col))
        strict = same & (token_of(row) > token_of(col))
        diagonal = row == col
        identity = jnp.where(diagonal, 1.0, 0.0)
        pick = iota((size, HEADS), 0) // BLK == iota((size, HEADS), 1)

        def as_column(block):
            return jnp.sum(jnp.where(pick, block, 0.0), axis=1, keepdims=True)

        def to_row(column):
            return jnp.sum(jnp.where(diagonal, column, 0.0), axis=0, keepdims=True)

        live = jnp.where(token_of(iota((size, 1), 0)) < length_ref[...], 1.0, 0.0)
        write_col = as_column(jnp.concatenate([write_pre] * HEADS, axis=0))
        forget_col = as_column(jnp.concatenate([forget_pre] * HEADS, axis=0))
        rate_col = as_column(jnp.broadcast_to(rates_ref[...], (size, HEADS)))
        write_gate = jax.nn.sigmoid(write_col) * live
        softplus = jnp.maximum(forget_col, 0.0) + jnp.log1p(jnp.exp(-jnp.abs(forget_col)))
        forget = -jnp.exp(rate_col) * softplus * live
        forget_row = to_row(forget)
        cumulative = jnp.sum(jnp.where(causal, forget_row, 0.0), axis=1, keepdims=True)
        final = jnp.sum(jnp.where(same, forget_row, 0.0), axis=1, keepdims=True)
        decay = jnp.where(
            causal, jnp.exp(jnp.minimum(cumulative - to_row(cumulative), 0.0)), 0.0
        )
        growth = jnp.exp(cumulative)
        fading = jnp.exp(final - cumulative)
        shrink = jnp.exp(final)

    with jax.named_scope("partwait"):
        for copy in part_copies.values():
            copy.wait_recv()
    scope = jax.named_scope("mix")
    scope.__enter__()
    upper = iota((BLK, wide), 0) < slots

    def by_head(pair):
        ahead, behind = [], []
        for chip in range(kv_size):
            at = slice(pair * BLK, (pair + 1) * BLK)
            mine = part_recv[chip, 0, at].astype(F32)
            theirs = part_recv[chip, 1, at].astype(F32)
            front = jnp.where(upper, mine, theirs)
            back = pltpu.roll(jnp.where(upper, theirs, mine), slots, 0)
            for start in range(0, wide, HEAD):
                ahead.append(front[:, start : start + HEAD])
                behind.append(back[:, start : start + HEAD])
        return jnp.concatenate(ahead, axis=0), jnp.concatenate(behind, axis=0)

    query, key_in = by_head(0)
    value, gating = by_head(1)
    query_unit = (
        query
        * lax.rsqrt(jnp.sum(query * query, axis=1, keepdims=True) + EPSILON)
        * (1.0 / math.sqrt(HEAD))
    )
    key_unit = key_in * lax.rsqrt(jnp.sum(key_in * key_in, axis=1, keepdims=True) + EPSILON)
    products = dot_fine(jnp.concatenate([key_unit, query_unit], axis=0), key_unit, True)
    lower = products[:size]
    lower = jnp.where(strict, write_gate * decay * lower, 0.0)
    squared = dot_fine(lower, lower)
    fourth = dot_fine(squared, squared)
    inverse = dot_fine(identity - lower, identity + squared)
    inverse = dot_fine(inverse, identity + fourth)
    key_grown = (write_gate * growth) * key_unit
    query_grown = query_unit * growth
    scores = products[size:] * decay

    key_terms, query_terms = [], []
    for head in range(HEADS):
        at = slice(head * BLK, (head + 1) * BLK)
        high, low = cut_terms(jnp.concatenate([key_grown[at], query_grown[at]], axis=0))
        both = jnp.concatenate([high, low], axis=0).astype(BF16)
        result = dot(both, state_high[head])
        result = result[: 2 * BLK] + result[2 * BLK :]
        result = result + dot(both[: 2 * BLK], state_low[head])
        key_terms.append(result[:BLK])
        query_terms.append(result[BLK:])
    update = dot_fine(inverse, write_gate * value - jnp.concatenate(key_terms, axis=0))
    attend = jnp.concatenate(query_terms, axis=0) + dot_fine(scores, update)
    normed = attend * lax.rsqrt(jnp.mean(attend * attend, axis=1, keepdims=True) + EPSILON)
    normed = normed * jax.nn.silu(gating) * live

    per_chip = wide // HEAD

    def lanes_of(chip):
        first = chip * per_chip
        return jnp.concatenate(
            [normed[(first + at) * BLK : (first + at + 1) * BLK] for at in range(per_chip)], axis=1
        )

    fronts, backs = [], []
    for chip in range(0, kv_size, 2):
        even, odd = lanes_of(chip), lanes_of(chip + 1)
        fronts.append(jnp.where(upper, even, pltpu.roll(odd, slots, 0)))
        backs.append(jnp.where(upper, pltpu.roll(even, slots, 0), odd))
    heads_send[0] = jnp.concatenate(fronts, axis=0).astype(BF16)
    heads_send[1] = jnp.concatenate(backs, axis=0).astype(BF16)
    copies = to_all(
        lambda off, other, peer: heads_send.at[lax.rem(cls + other, 2)],
        lambda off, other: heads_recv.at[me],
    )
    heads_recv[me] = heads_send[cls]
    scope.__exit__(None, None, None)

    with jax.named_scope("newstate"):
        faded = key_unit * fading
        for head in range(HEADS):
            at = slice(head * BLK, (head + 1) * BLK)
            key_high, key_low = cut_terms(faded[at])
            value_high, value_low = cut_terms(update[at])
            outer = lax.dot_general(
                jnp.concatenate([key_high, key_high, key_low], axis=0).astype(BF16),
                jnp.concatenate([value_high, value_low, value_high], axis=0).astype(BF16),
                (((0,), (0,)), ((), ())),
                preferred_element_type=F32,
            )
            state_out[0, head] = shrink[head * BLK : head * BLK + 1] * state[head] + outer

    def hand_over(group, hidden, source):
        outgoing = {}

        def term_of(chip, core):
            at = pl.ds(pl.multiple_of((chip * 2 + core) * cols, cols), cols)
            return dot(hidden, down2[:, at])

        for off in far_first:
            chip = swapped(off)
            for other in (0, 1):
                core = core_of(chip, other)
                fin_send[group, off, other] = term_of(chip, core).astype(BF16)
                outgoing[off, other] = remote(
                    fin_send.at[group, off, other], fin_recv.at[group, off, other], chip, core
                )
        theirs = pl.ds(pl.multiple_of((1 - tp) * cols, cols), cols)
        own_send[group] = source[:, theirs].astype(F32) + 0.5 * term_of(kv, 1 - tp)
        outgoing[0, 1] = to_partner(own_send.at[group], own_recv.at[group])
        own = source[:, own_cols].astype(F32) + 0.5 * term_of(kv, tp)
        return own, outgoing

    def take_in(group, own, outgoing):
        outgoing[0, 1].wait_recv()
        sums = [own, own_recv[group]]
        for other in (0, 1):
            total = None
            for off in far_first[::-1]:
                outgoing[off, other].wait_recv()
                term = fin_recv[group, off, other].astype(F32)
                total = term if total is None else total + term
            sums[other] = sums[other] + 0.5 * total
        return [total.astype(BF16) for total in sums]

    with jax.named_scope("dead_down"):
        loads["down2"].wait()
        dead_own, dead_out = hand_over(1, dead_hidden, middle.at[1, kv])

    with jax.named_scope("gather2"):
        for copy in copies.values():
            copy.wait_recv()
        out_copy.wait_recv()
    with jax.named_scope("outproj"):
        blocks = heads_recv[...].reshape(devices * 2 * BLK, wide)
        mixed = dot(gather_heads, blocks).astype(BF16)
        terms = []
        for part in range(2):
            chips = range(part * kv_size // 2, (part + 1) * kv_size // 2)
            left = jnp.concatenate([mixed[chip * pack : (chip + 1) * pack] for chip in chips], axis=1)
            right = out_w[chips[0] * wide : (chips[-1] + 1) * wide, :]
            terms.append(dot(left, right).astype(BF16).astype(F32))
        second_in[kv] = (middle[0, kv].astype(F32) + (terms[0] + terms[1])).astype(BF16)
        copies = to_class(lambda off: second_in.at[kv], lambda off: second_in.at[kv])

    squares = jnp.zeros((pack, 1), F32)
    with jax.named_scope("gather3"):
        for off in range(kv_size):
            if off:
                copies[off].wait_recv()
            chip = swapped(off)
            squares = squares + ffn_slot(
                live_acc, units2, gains2_ref, chip, second_in[chip], off == 0
            )
    with jax.named_scope("finish1"):
        hidden = finish(live_acc, squares)
    with jax.named_scope("down1"):
        live_own, live_out = hand_over(0, hidden, second_in.at[kv])
    with jax.named_scope("dead_in"):
        dead_sums = take_in(1, dead_own, dead_out)
    with jax.named_scope("live_in"):
        live_sums = take_in(0, live_own, live_out)
    with jax.named_scope("last"):
        packed = jnp.concatenate(
            [live_sums[0], dead_sums[0], live_sums[1], dead_sums[1]], axis=0
        )
        mixed_out_ref[...] = dot(restore, packed).astype(BF16)
    with jax.named_scope("tail"):
        for copy in sent:
            copy.wait_send()


def fused_call(mesh, *args):
    (
        tokens, lengths, state, gain_first, first_gate, first_up, first_down, gain_mix,
        query_weight, key_weight, value_weight, gating_weight, write_weight, forget_weight,
        forget_rate, out_weight, gain_second, second_gate, second_up, second_down,
    ) = args
    kv_size = mesh.shape["kv"]
    devices = kv_size * mesh.shape["tp"]
    rows, cols = tokens.shape
    wide = 2 * cols
    channels = gain_first.shape[0]
    hidden_local = first_gate.shape[1]
    half, pack = rows // 2, rows // 4
    in_hbm = pl.BlockSpec(memory_space=pltpu.HBM)
    in_vmem = pl.BlockSpec(memory_space=pltpu.VMEM)
    dma = pltpu.SemaphoreType.DMA
    remotes = 7 * (devices - 1) + 6 * (kv_size - 1) + 10
    operands = (
        tokens, lengths.reshape(1, 1), gain_first.reshape(1, -1), gain_mix.reshape(1, -1),
        gain_second.reshape(1, -1), forget_rate.reshape(1, -1), state,
        first_gate, first_up, first_down, query_weight, key_weight, value_weight,
        gating_weight, write_weight.T, forget_weight.T, out_weight, second_gate, second_up,
        second_down,
    )
    operands = [
        array if array.dtype == jnp.int32 else pltpu.with_memory_space_constraint(array, pltpu.HBM)
        for array in operands
    ]
    mixed_out, new_state = pl.pallas_call(
        functools.partial(fused_kernel, kv_size, channels),
        out_shape=(
            pltpu.VMEM(tokens.shape, tokens.dtype),
            pltpu.VMEM(state.shape, state.dtype),
        ),
        in_specs=[in_hbm] * len(operands),
        out_specs=(in_vmem, in_vmem),
        scratch_shapes=[
            pltpu.VMEM((channels, 2 * hidden_local), BF16),
            pltpu.VMEM((hidden_local, channels), BF16),
            pltpu.VMEM((channels, 2 * hidden_local), BF16),
            pltpu.VMEM((hidden_local, channels), BF16),
            pltpu.VMEM((channels, 4 * wide), BF16),
            pltpu.VMEM((channels, wide), BF16),
            pltpu.VMEM((HEAD, channels), BF16),
            pltpu.VMEM(state.shape[1:], F32),
            pltpu.VMEM(state.shape[1:], BF16),
            pltpu.VMEM(state.shape[1:], BF16),
            pltpu.VMEM((1, channels), F32),
            pltpu.VMEM((1, channels), F32),
            pltpu.VMEM((1, channels), F32),
            pltpu.VMEM((1, HEADS), F32),
            pltpu.VMEM((rows, cols), BF16),
            pltpu.VMEM((1, 1), jnp.int32),
            pltpu.VMEM((devices, 1, HEAD), jnp.int32),
            pltpu.VMEM((2, half, cols), BF16),
            pltpu.VMEM((devices, half, cols), BF16),
            pltpu.VMEM((half, 2 * hidden_local), F32),
            pltpu.VMEM((pack, 2 * hidden_local), F32),
            pltpu.VMEM((pack, 2 * hidden_local), F32),
            pltpu.VMEM((pack, 4 * wide), F32),
            pltpu.VMEM((1, pack, HEAD), F32),
            pltpu.VMEM((2, kv_size, pack, wide), BF16),
            pltpu.VMEM((kv_size, pack, wide), BF16),
            pltpu.VMEM((2, 2 * BLK, wide), BF16),
            pltpu.VMEM((devices, 2 * BLK, wide), BF16),
            pltpu.VMEM((2, kv_size, pack, wide), BF16),
            pltpu.VMEM((2, kv_size, pack, wide), BF16),
            pltpu.VMEM((devices, 2 * BLK, wide), BF16),
            pltpu.VMEM((kv_size, 2, 2 * BLK, wide), BF16),
            pltpu.VMEM((1, pack, HEAD), F32),
            pltpu.VMEM((2, kv_size, 2, pack, cols), BF16),
            pltpu.VMEM((2, kv_size, 2, pack, cols), BF16),
            pltpu.VMEM((2, pack, cols), F32),
            pltpu.VMEM((2, pack, cols), F32),
            dma((3 + 2 * kv_size + 15,)),
            dma((remotes,)),
            dma((remotes,)),
        ],
        compiler_params=pltpu.CompilerParams(
            collective_id=0, has_side_effects=True, vmem_limit_bytes=VMEM_LIMIT
        ),
    )(*operands)
    return hand_out(mixed_out, new_state)


def hand_out_kernel(mixed, state, mixed_out_hbm, state_out_hbm, sems):
    puts = [
        pltpu.make_async_copy(mixed, mixed_out_hbm, sems.at[0]),
        pltpu.make_async_copy(state, state_out_hbm, sems.at[1]),
    ]
    for put in puts:
        put.start()
    for put in puts:
        put.wait()


def hand_out(mixed_out, new_state):
    in_hbm = pl.BlockSpec(memory_space=pltpu.HBM)
    in_vmem = pl.BlockSpec(memory_space=pltpu.VMEM)
    arrays = [
        pltpu.with_memory_space_constraint(array, pltpu.VMEM) for array in (mixed_out, new_state)
    ]
    return pl.pallas_call(
        hand_out_kernel,
        out_shape=tuple(jax.ShapeDtypeStruct(array.shape, array.dtype) for array in arrays),
        in_specs=[in_vmem, in_vmem],
        out_specs=(in_hbm, in_hbm),
        scratch_shapes=[pltpu.SemaphoreType.DMA((2,))],
        compiler_params=pltpu.CompilerParams(vmem_limit_bytes=8 * 1024 * 1024),
    )(*arrays)


def fits_fused(mesh, args):
    tokens, lengths, state, first_gate = args[0], args[1], args[2], args[4]
    rows, cols = tokens.shape
    kv_size = mesh.shape["kv"]
    devices = kv_size * mesh.shape["tp"]
    return (
        mesh.shape["tp"] == 2
        and mesh.shape["kv"] & (mesh.shape["kv"] - 1) == 0
        and lengths.shape[0] == 1
        and rows == devices * BLK
        and devices * 2 * BLK == HEAD
        and kv_size * BLK // 2 == 2 * BLK
        and devices * cols == HEADS * HEAD
        and cols % 256 == 0
        and first_gate.shape[1] % 128 == 0
        and state.shape[1:] == (HEADS, HEAD, HEAD)
    )


def solution(mesh):
    in_specs = (
        P("dp", ("kv", "tp")),
        P(("dp", "kv", "tp")),
        P(("dp", "kv", "tp"), None, None, None),
        P(),
        P(None, "kv"),
        P(None, "kv"),
        P("kv", None),
        P(),
        P(None, ("kv", "tp")),
        P(None, ("kv", "tp")),
        P(None, ("kv", "tp")),
        P(None, ("kv", "tp")),
        P(),
        P(),
        P(),
        P(None, ("kv", "tp")),
        P(),
        P(None, "kv"),
        P(None, "kv"),
        P("kv", None),
    )
    out_specs = (P("dp", ("kv", "tp")), P(("dp", "kv", "tp"), None, None, None))

    def body(*args):
        if fits_fused(mesh, args):
            return fused_call(mesh, *args)
        return per_device(*args)

    return jax.shard_map(
        body, mesh=mesh, in_specs=in_specs, out_specs=out_specs, check_vma=False
    )
```

```python
import functools
import math

import jax
import jax.numpy as jnp
from jax import lax
from jax.experimental import pallas as pl
from jax.experimental.pallas import tpu as pltpu
from jax.sharding import PartitionSpec as P

HEADS = 16
HEAD = 128
BLK = 8


EPSILON = 1e-06


def fold_step(gain, gate_cols, up_cols, portion):
    values = portion.astype(jnp.float32)
    scaled = (values * gain).astype(jnp.bfloat16)
    gate_acc = jnp.dot(scaled, gate_cols, preferred_element_type=jnp.float32)
    up_acc = jnp.dot(scaled, up_cols, preferred_element_type=jnp.float32)
    squares = jnp.sum(values * values, axis=1)
    return (gate_acc, up_acc, squares)


def finish_units(gate_acc, up_acc, squares, channels, down_rows):
    row_scale = lax.rsqrt(squares / channels + EPSILON)[:, None]
    hidden = (jax.nn.silu(gate_acc * row_scale) * (up_acc * row_scale)).astype(jnp.bfloat16)
    return jnp.dot(hidden, down_rows, preferred_element_type=jnp.float32)


def feed_forward(hidden_in, gain, w_gate, w_up, w_down):
    channels = gain.shape[0]
    paired = lax.all_to_all(hidden_in, "tp", split_axis=0, concat_axis=1, tiled=True)
    gate_acc, up_acc, squares = fold_step(
        gain, w_gate, w_up, lax.all_gather(paired, "kv", axis=1, tiled=True)
    )
    ffn_term = finish_units(gate_acc, up_acc, squares, channels, w_down)
    partial_value = lax.psum_scatter(ffn_term, "kv", scatter_dimension=1, tiled=True)
    summed = lax.all_to_all(partial_value, "tp", split_axis=1, concat_axis=0, tiled=True)
    return (hidden_in.astype(jnp.float32) + 0.5 * summed).astype(jnp.bfloat16)


def delta_block(query, key_in, value, gating, write_pre, forget_pre, rates, live, state):
    seq_count, block_len, head_count, head_size = query.shape
    precise = lax.Precision.HIGHEST
    query_unit = (
        query
        * lax.rsqrt(jnp.sum(query * query, axis=-1, keepdims=True) + EPSILON)
        / math.sqrt(head_size)
    )
    key_unit = key_in * lax.rsqrt(jnp.sum(key_in * key_in, axis=-1, keepdims=True) + EPSILON)
    live_rows = live[:, :, None]
    write_gate = jax.nn.sigmoid(write_pre) * live_rows
    forget = -jnp.exp(rates)[None, None, :] * jax.nn.softplus(forget_pre) * live_rows
    cumulative = jnp.cumsum(forget, axis=1)
    cum_heads = jnp.transpose(cumulative, (0, 2, 1))
    positions = jnp.arange(block_len)
    causal = positions[:, None] >= positions[None, :]
    strict = positions[:, None] > positions[None, :]
    differ = jnp.minimum(cum_heads[:, :, :, None] - cum_heads[:, :, None, :], 0.0)
    decay_mat = jnp.where(causal, jnp.exp(differ), 0.0)
    key_dots = jnp.einsum("sthd,suhd->shtu", key_unit, key_unit, precision=precise)
    write_heads = jnp.transpose(write_gate, (0, 2, 1))
    strict_part = jnp.where(strict, write_heads[:, :, :, None] * decay_mat * key_dots, 0.0)
    identity = jnp.eye(block_len, dtype=jnp.float32)
    squared = jnp.einsum("shtu,shuv->shtv", strict_part, strict_part, precision=precise)
    fourth = jnp.einsum("shtu,shuv->shtv", squared, squared, precision=precise)
    inverse = jnp.einsum(
        "shtu,shuv->shtv", identity - strict_part, identity + squared, precision=precise
    )
    inverse = jnp.einsum("shtu,shuv->shtv", inverse, identity + fourth, precision=precise)
    growth = jnp.exp(cumulative)
    target = jnp.einsum(
        "shtu,suhv->sthv", inverse, write_gate[..., None] * value, precision=precise
    )
    key_mix = jnp.einsum(
        "shtu,suhk->sthk", inverse, (write_gate * growth)[..., None] * key_unit, precision=precise
    )
    update = target - jnp.einsum("sthk,shkv->sthv", key_mix, state, precision=precise)
    scores = jnp.einsum("sthd,suhd->shtu", query_unit, key_unit, precision=precise) * decay_mat
    attend = jnp.einsum("sthk,shkv->sthv", query_unit * growth[..., None], state, precision=precise)
    attend = attend + jnp.einsum("shtu,suhv->sthv", scores, update, precision=precise)
    final_cum = cumulative[:, -1:, :]
    fading = jnp.exp(final_cum - cumulative)
    new_state = jnp.exp(final_cum[:, 0, :])[:, :, None, None] * state
    new_state = new_state + jnp.einsum(
        "sthk,sthv->shkv", key_unit * fading[..., None], update, precision=precise
    )
    normed = attend * lax.rsqrt(jnp.mean(attend * attend, axis=-1, keepdims=True) + EPSILON)
    normed = normed * jax.nn.silu(gating) * live[:, :, None, None]
    mixed_heads = normed.reshape(seq_count * block_len, head_count * head_size).astype(jnp.bfloat16)
    return (mixed_heads, new_state)


def per_device(
    tokens,
    lengths,
    state,
    gain_first,
    first_gate,
    first_up,
    first_down,
    gain_mix,
    query_weight,
    key_weight,
    value_weight,
    gating_weight,
    write_weight,
    forget_weight,
    forget_rate,
    out_weight,
    gain_second,
    second_gate,
    second_up,
    second_down,
):
    after_first = feed_forward(tokens, gain_first, first_gate, first_up, first_down)
    seq_count = lengths.shape[0]
    own_count = seq_count * BLK
    whole_rows = lax.all_gather(after_first, ("kv", "tp"), axis=1, tiled=True)
    scaled_all = (whole_rows.astype(jnp.float32) * gain_mix).astype(jnp.bfloat16)
    stacked = jnp.stack(
        [
            jnp.dot(scaled_all, matrix, preferred_element_type=jnp.float32)
            for matrix in (query_weight, key_weight, value_weight, gating_weight)
        ]
    )
    owned = lax.all_to_all(
        stacked.astype(jnp.bfloat16), ("kv", "tp"), split_axis=1, concat_axis=2, tiled=True
    ).astype(stacked.dtype)
    row_start = lax.axis_index(("kv", "tp")) * own_count
    own_values = lax.dynamic_slice_in_dim(whole_rows, row_start, own_count, 0).astype(jnp.float32)
    own_scaled = lax.dynamic_slice_in_dim(scaled_all, row_start, own_count, 0)
    mix_scale = lax.rsqrt(jnp.mean(own_values * own_values, axis=1, keepdims=True) + EPSILON)
    query = (owned[0] * mix_scale).reshape(seq_count, BLK, HEADS, HEAD)
    key_in = (owned[1] * mix_scale).reshape(seq_count, BLK, HEADS, HEAD)
    value = (owned[2] * mix_scale).reshape(seq_count, BLK, HEADS, HEAD)
    gating = (owned[3] * mix_scale).reshape(seq_count, BLK, HEADS, HEAD)
    write_pre = (
        jnp.dot(own_scaled, write_weight, preferred_element_type=jnp.float32) * mix_scale
    ).reshape(seq_count, BLK, HEADS)
    forget_pre = (
        jnp.dot(own_scaled, forget_weight, preferred_element_type=jnp.float32) * mix_scale
    ).reshape(seq_count, BLK, HEADS)
    positions = jnp.arange(BLK, dtype=jnp.int32)
    live = (positions[None, :] < lengths[:, None]).astype(jnp.float32)
    mixed_heads, new_state = delta_block(
        query, key_in, value, gating, write_pre, forget_pre, forget_rate, live, state
    )
    half_cols = mixed_heads.shape[1] // 2
    portion = lax.all_gather(mixed_heads, ("kv", "tp"), axis=0, tiled=True)
    first_half = jnp.dot(
        portion[:, :half_cols], out_weight[:half_cols], preferred_element_type=jnp.float32
    ).astype(jnp.bfloat16)
    second_half = jnp.dot(
        portion[:, half_cols:], out_weight[half_cols:], preferred_element_type=jnp.float32
    ).astype(jnp.bfloat16)
    first_half, second_half = lax.optimization_barrier((first_half, second_half))
    mixed_sum = first_half.astype(jnp.float32) + second_half.astype(jnp.float32)
    after_mix = (after_first.astype(jnp.float32) + mixed_sum).astype(jnp.bfloat16)
    mixed_out = feed_forward(after_mix, gain_second, second_gate, second_up, second_down)
    return (mixed_out, new_state)


F32 = jnp.float32
BF16 = jnp.bfloat16
MESH = pl.DeviceIdType.MESH
VMEM_LIMIT = 58 * 1024 * 1024


def fused_kernel(
    kv_size,
    channels,
    tokens_hbm,
    lengths_hbm,
    gains1_hbm,
    gains_mix_hbm,
    gains2_hbm,
    rates_hbm,
    state_hbm,
    gate1_hbm,
    up1_hbm,
    down1_hbm,
    query_hbm,
    key_hbm,
    value_hbm,
    gating_hbm,
    write_hbm,
    forget_hbm,
    out_hbm,
    gate2_hbm,
    up2_hbm,
    down2_hbm,
    mixed_out_ref,
    state_out,
    units1,
    down1,
    units2,
    down2,
    proj,
    out_w,
    small_w,
    state,
    state_high,
    state_low,
    gains1_ref,
    gains_mix_ref,
    gains2_ref,
    rates_ref,
    tokens_ref,
    length_ref,
    lens_all,
    picked,
    entered,
    unit_acc,
    live_acc,
    dead_acc,
    proj_acc,
    small_acc,
    middle,
    second_in,
    heads_send,
    heads_recv,
    red_send,
    red_recv,
    part_send,
    part_recv,
    small_recv,
    fin_send,
    fin_recv,
    own_send,
    own_recv,
    load_sems,
    send_sems,
    recv_sems,
):
    kv = lax.axis_index("kv")
    tp = lax.axis_index("tp")
    devices = 2 * kv_size
    me = kv * 2 + tp
    cls = lax.rem(kv + tp, 2)
    rows, cols = tokens_ref.shape
    wide = 2 * cols
    slots = BLK // 2
    half = rows // 2
    pack = rows // 4
    hidden_local = gate1_hbm.shape[1]
    own_cols = pl.ds(pl.multiple_of(tp * cols, cols), cols)
    inner = lax.rem((kv + 1) // 2, 2)
    near_first = [1, 2 + inner, 3 - inner]
    far_first = near_first[::-1]

    loads = {}

    def load(name, *pairs):
        sem = load_sems.at[len(loads)]
        loads[name] = [pltpu.make_async_copy(src, dst, sem) for src, dst in pairs]

    def start(name):
        for copy in loads[name]:
            copy.start()

    def loaded(name, ref=None):
        if ref is None:
            loads[name][0].wait()
        else:
            sem = load_sems.at[list(loads).index(name)]
            pltpu.make_async_copy(ref, ref, sem).wait()

    def swapped(off):
        chip, bit = 0, 1
        while bit < kv_size:
            chip = chip + bit * lax.rem(kv // bit + off // bit, 2)
            bit *= 2
        return chip

    def core_of(chip, other):
        return lax.rem(chip + cls + other, 2)

    def chip_rows(chip):
        return pl.ds(pl.multiple_of(chip * wide, wide), wide)

    def kind_cols(kind):
        return pl.ds(pl.multiple_of(kind * wide + tp * cols, cols), cols)

    load("length", (lengths_hbm, length_ref))
    load("tokens", (tokens_hbm, tokens_ref))
    load("gains1", (gains1_hbm, gains1_ref))
    for index, off in enumerate([0] + near_first):
        at = chip_rows(swapped(off))
        load(
            f"units1{index}",
            (gate1_hbm.at[at, :], units1.at[at, 0:hidden_local]),
            (up1_hbm.at[at, :], units1.at[at, hidden_local : 2 * hidden_local]),
        )
    early = list(loads)
    load("down1", (down1_hbm, down1))
    kinds = (query_hbm, key_hbm, value_hbm, gating_hbm)
    load("proj", *[(ref, proj.at[:, kind_cols(kind)]) for kind, ref in enumerate(kinds)])
    load(
        "small",
        (write_hbm, small_w.at[0:HEADS]),
        (forget_hbm, small_w.at[HEADS : 2 * HEADS]),
    )
    load("gains_mix", (gains_mix_hbm, gains_mix_ref))
    load("rates", (rates_hbm, rates_ref))
    load("out", (out_hbm, out_w.at[:, own_cols]))
    load("state", (state_hbm.at[0], state))
    load("gains2", (gains2_hbm, gains2_ref))
    load(
        "units2",
        (gate2_hbm, units2.at[:, 0:hidden_local]),
        (up2_hbm, units2.at[:, hidden_local : 2 * hidden_local]),
    )
    load("down2", (down2_hbm, down2))
    late = [name for name in loads if name not in early]
    for name in early[:2]:
        start(name)

    barrier = pltpu.get_barrier_semaphore()
    for off in range(1, devices):
        peer = lax.rem(me + off, devices)
        pl.semaphore_signal(
            barrier,
            inc=1,
            device_id={"kv": peer // 2, "tp": lax.rem(peer, 2)},
            device_id_type=MESH,
        )
    for name in early[2:]:
        start(name)

    sends, receives, width = {}, {}, [0]

    def remote(name, src, dst, chip, core, at=0, spread=1):
        if name not in sends:
            sends[name] = len(sends)
            receives[name] = width[0]
            width[0] += spread
        copy = pltpu.make_async_remote_copy(
            src_ref=src,
            dst_ref=dst,
            send_sem=send_sems.at[sends[name]],
            recv_sem=recv_sems.at[receives[name] + at],
            device_id={"kv": chip, "tp": core},
            device_id_type=MESH,
        )
        copy.start()

    def of_phase(name, ref, at=0):
        return pltpu.make_async_remote_copy(
            src_ref=ref,
            dst_ref=ref,
            send_sem=send_sems.at[sends[name]],
            recv_sem=recv_sems.at[receives[name] + at],
            device_id={"kv": kv, "tp": 1 - tp},
            device_id_type=MESH,
        )

    def arrived(name, ref, at=0):
        of_phase(name, ref, at).wait_recv()

    def to_class(name, src, dst, spread=1):
        for off in far_first:
            chip = swapped(off)
            remote(name, src(off), dst(off), chip, core_of(chip, 0), off if spread > 1 else 0, spread)

    def to_all(name, src, dst, spread=1):
        for off in far_first + [0]:
            chip = swapped(off)
            for other in (0, 1):
                if other == 0 and isinstance(off, int) and off == 0:
                    continue
                core = core_of(chip, other)
                remote(
                    name, src(other, chip * 2 + core), dst(other), chip, core,
                    off if spread > 1 else 0, spread,
                )

    def to_partner(name, src, dst):
        remote(name, src, dst, kv, 1 - tp)

    def iota(shape, axis):
        return lax.broadcasted_iota(jnp.int32, shape, axis)

    def dot(a, b):
        return jnp.dot(a, b, preferred_element_type=F32)

    def one_hot(mask):
        return jnp.where(mask, 1.0, 0.0).astype(BF16)

    row = iota((rows, rows), 0)
    col = iota((rows, rows), 1)
    at_class = lax.rem(row, half)
    at_seq = at_class // slots
    which = lax.rem(cls + row // half + at_seq, 2)
    picks = one_hot(col == at_seq * BLK + 2 * lax.rem(at_class, slots) + which)
    with jax.named_scope("small_wait"):
        loaded("length")
        loaded("tokens")
    lens_all[me] = jnp.broadcast_to(length_ref[...], (1, HEAD))
    chosen = dot(picks, tokens_ref[...]).astype(BF16)
    picked[...] = chosen.reshape(2, half, cols)
    entered[me] = chosen[:half]
    with jax.named_scope("barrier"):
        pl.semaphore_wait(barrier, devices - 1)
    to_all("tokens", lambda other, peer: picked.at[other], lambda other: entered.at[me], kv_size)
    to_all("lens", lambda other, peer: lens_all.at[me], lambda other: lens_all.at[me])
    for name in late:
        start(name)
    small_w[2 * HEADS :] = jnp.zeros((HEAD - 2 * HEADS, channels), BF16)

    def ffn_slot(acc, units, gain_ref, chip, portion, first):
        at = chip_rows(chip)
        values = portion.astype(F32)
        scaled = (values * gain_ref[:, at]).astype(BF16)
        term = dot(scaled, units[at, :])
        if first:
            acc[...] = term
        else:
            acc[...] += term
        return jnp.sum(values * values, axis=1, keepdims=True)

    def finish(acc, squares):
        row_scale = lax.rsqrt(squares / channels + EPSILON)
        gate = acc[:, 0:hidden_local] * row_scale
        up = acc[:, hidden_local : 2 * hidden_local] * row_scale
        return (jax.nn.silu(gate) * up).astype(BF16)

    def lengths_by(seq):
        found = jnp.zeros(seq.shape, jnp.int32)
        for index in range(devices):
            found = jnp.where(seq == index, lens_all[index], found)
        return found

    def is_live(seq, slot, klass):
        return 2 * slot + lax.rem(klass + seq, 2) < lengths_by(seq)

    def live_column(klass):
        at = iota((half, HEAD), 0)
        return jnp.where(is_live(at // slots, lax.rem(at, slots), klass), 1.0, 0.0)

    def live_row(klass):
        at = iota((1, HEAD), 1)
        live = is_live(at // slots, lax.rem(at, slots), klass) & (at < half)
        return jnp.where(live, 1.0, 0.0)

    def place_lanes(seq, slot, column):
        target = seq * slots + slot
        before = jnp.sum(
            jnp.where(iota((half, HEAD), 0) < target, column, 0.0), axis=0, keepdims=True
        )
        count = jnp.sum(column, axis=0, keepdims=True)
        rest = count + target.astype(F32) - before
        return jnp.where(is_live(seq, slot, cls), before, rest).astype(jnp.int32)

    def place_rows(seq, slot, klass, flags):
        target = seq * slots + slot
        before = jnp.sum(
            jnp.where(iota(seq.shape, 1) < target, flags, 0.0), axis=1, keepdims=True
        )
        count = jnp.sum(flags, axis=1, keepdims=True)
        rest = count + target.astype(F32) - before
        return jnp.where(is_live(seq, slot, klass), before, rest).astype(jnp.int32)

    def chip_tokens(chip):
        return jnp.concatenate([entered[chip * 2], entered[chip * 2 + 1]], axis=1)

    loaded("gains1")
    squares = jnp.zeros((half, 1), F32)
    for index, off in enumerate([0] + near_first):
        chip = swapped(off)
        with jax.named_scope(f"tokens_wait{index}"):
            if index:
                arrived("tokens", entered.at[pl.ds(chip * 2, 2)], off)
            else:
                arrived("tokens", entered.at[kv * 2 + 1 - tp], off)
            loaded(f"units1{index}", units1.at[chip_rows(chip), :])
            if index == kv_size - 1:
                arrived("lens", lens_all.at[pl.ds(0, devices - 1)])
        with jax.named_scope(f"units_slot{index}"):
            if index == kv_size - 1:
                column = live_column(cls)
                lane = iota((1, HEAD), 1)
                place = place_lanes(
                    jnp.minimum(lane // slots, devices - 1), lax.rem(lane, slots), column
                )
                reorder = one_hot(iota((half, HEAD), 0) == place)[:, :half]
            squares = squares + ffn_slot(
                unit_acc, units1, gains1_ref, chip, chip_tokens(chip), index == 0
            )
        if index == kv_size - 2:
            with jax.named_scope("exchange"):
                loaded("proj", proj.at[:, 0 : 4 * cols])
                for kind in range(4):
                    at = kind_cols(kind)
                    to_partner("proj", proj.at[:, at], proj.at[:, at])
    with jax.named_scope("finish0"):
        hidden = dot(reorder, finish(unit_acc, squares)).astype(BF16)
    with jax.named_scope("down_wait"):
        loaded("down1")
    with jax.named_scope("down0"):
        for off in far_first:
            chip = swapped(off)
            term = dot(hidden, down1[:, chip_rows(chip)])
            red_send[0, off] = term[:pack].astype(BF16)
            red_send[1, off] = term[pack:].astype(BF16)
            remote("red0", red_send.at[0, off], red_recv.at[0, off], chip, core_of(chip, 0))
        own_term = dot(hidden, down1[:, chip_rows(kv)])
        for off in far_first:
            chip = swapped(off)
            remote("red1", red_send.at[1, off], red_recv.at[1, off], chip, core_of(chip, 0))
    with jax.named_scope("exchange_out"):
        loaded("out")
        to_partner("out", out_w.at[:, own_cols], out_w.at[:, own_cols])
    with jax.named_scope("tables"):
        residual = dot(reorder, chip_tokens(kv))
        flags = live_row(cls)
        other_flags = live_row(1 - cls)
        at = iota((rows, HEAD), 0)
        slot = lax.rem(at, slots)
        place = place_rows(at // BLK, slot, cls, flags)
        kind = lax.rem(at // slots + cls, 2)
        lane = iota((rows, HEAD), 1)
        spread = one_hot(
            (lane // pack == kind) & (lax.rem(lane, pack) == place) & (lane < 2 * pack)
        )[:, : 2 * pack]
        lane = iota((1, devices * 2 * BLK), 1)
        place = place_lanes(lane // (2 * BLK), lax.rem(lane, slots), column)
        at = iota((kv_size * pack, devices * 2 * BLK), 0)
        chip_at = lax.rem(iota((kv_size * pack, devices * 2 * BLK), 1) // slots, kv_size)
        gather_heads = one_hot((at // pack == chip_at) & (lax.rem(at, pack) == place))
        at = iota((BLK, HEAD), 0)
        klass = at // slots
        place = place_rows(
            jnp.zeros((BLK, HEAD), jnp.int32) + me,
            lax.rem(at, slots),
            klass,
            jnp.where(klass == cls, flags, other_flags),
        )
        lane = iota((BLK, HEAD), 1)
        pick_small = jnp.where(
            (lax.rem(lane // pack + cls, 2) == klass)
            & (lax.rem(lane, pack) == place)
            & (lane < 2 * pack),
            1.0,
            0.0,
        )[:, : 2 * pack]
        at = iota((rows, HEAD), 0)
        seq, token = at // BLK, lax.rem(at, BLK)
        klass = lax.rem(seq + token, 2)
        place = place_rows(seq, token // 2, klass, jnp.where(klass == cls, flags, other_flags))
        lane = iota((rows, HEAD), 1)
        restore = one_hot(
            (lax.rem(lane // half + cls, 2) == klass)
            & (lax.rem(lane, half) == place)
            & (lane < rows)
        )[:, :rows]
    with jax.named_scope("statecut"):
        loaded("state")
        for head in range(HEADS):
            high = state[head].astype(BF16)
            state_high[head] = high
            state_low[head] = (state[head] - high.astype(F32)).astype(BF16)
    for group in range(2):
        with jax.named_scope(f"red0_{group}"):
            at = slice(group * pack, (group + 1) * pack)
            arrived(f"red{group}", red_recv.at[group, pl.ds(1, kv_size - 1)])
            total = own_term[at]
            for off in range(1, kv_size):
                total = total + red_recv[group, off].astype(F32)
            middle[group, kv] = (residual[at] + 0.5 * total).astype(BF16)
            to_class(
                f"middle{group}",
                lambda off: middle.at[group, kv],
                lambda off: middle.at[group, kv],
                1 if group else kv_size,
            )

    with jax.named_scope("proj_wait"):
        arrived("proj", proj.at[:, 0 : 4 * cols])
        loaded("small", small_w.at[0 : 2 * HEADS])
        loaded("gains_mix")
        loaded("rates")
    squares = jnp.zeros((pack, 1), F32)
    for index, off in enumerate([0] + near_first):
        chip = swapped(off)
        at = chip_rows(chip)
        with jax.named_scope(f"middle_wait{index}"):
            if index:
                arrived("middle0", middle.at[0, chip], off)
        with jax.named_scope(f"proj_slot{index}"):
            values = middle[0, chip].astype(F32)
            squares = squares + jnp.sum(values * values, axis=1, keepdims=True)
            scaled = (values * gains_mix_ref[:, at]).astype(BF16)
            small_term = lax.dot_general(
                scaled, small_w[:, at], (((1,), (1,)), ((), ())), preferred_element_type=F32
            )
            if index == 0:
                proj_acc[...] = dot(scaled, proj[at, :])
                small_acc[0] = small_term
            elif index < kv_size - 1:
                proj_acc[...] += dot(scaled, proj[at, :])
                small_acc[0] += small_term
    with jax.named_scope("partsend"):
        mix_scale = lax.rsqrt(squares / channels + EPSILON)
        for pair in range(2):
            lanes = slice(pair * 2 * wide, (pair + 1) * 2 * wide)
            projected = proj_acc[:, lanes] + dot(scaled, proj[at, lanes])
            projected = (projected * mix_scale).astype(BF16)
            stacked = jnp.concatenate([projected[:, :wide], projected[:, wide:]], axis=0)
            part = dot(spread, stacked).astype(BF16)
            part_send[pair] = part.reshape(devices, BLK, wide)
            to_all(
                f"part{pair}",
                lambda other, peer: part_send.at[pair, peer],
                lambda other: part_recv.at[pair, kv, cls],
            )
            if pair == 0:
                small_acc[0] = (small_acc[0] + small_term) * mix_scale
                to_partner("small", small_acc.at[0], small_recv.at[0])
        for pair in range(2):
            part_recv[pair, kv, cls] = part_send[pair, me]

    with jax.named_scope("dead_units"):
        loaded("gains2")
        loaded("units2", units2)
        arrived("middle1", middle.at[1, pl.ds(0, kv_size - 1)])
        values = jnp.concatenate([middle[1, chip] for chip in range(kv_size)], axis=1).astype(F32)
        squares = jnp.sum(values * values, axis=1, keepdims=True)
        dead_acc[...] = dot((values * gains2_ref[...]).astype(BF16), units2[...])
        dead_hidden = finish(dead_acc, squares)

    def cut_terms(a):
        high = a.astype(BF16).astype(F32)
        return high, a - high

    def dot_fine(a, b, across=False):
        high_a, low_a = cut_terms(a)
        high_b, low_b = cut_terms(b)
        axis = 1 if across else 0
        left = jnp.concatenate([high_a, high_a, low_a], axis=1).astype(BF16)
        right = jnp.concatenate([high_b, low_b, high_b], axis=axis).astype(BF16)
        return lax.dot_general(
            left, right, (((1,), (axis,)), ((), ())), preferred_element_type=F32
        )

    with jax.named_scope("premix"):
        arrived("small", small_recv.at[0])
        small_all = jnp.concatenate([small_acc[0], small_recv[0]], axis=0)
        high, low = cut_terms(small_all)
        picked_small = dot(pick_small.astype(BF16), high.astype(BF16)) + dot(
            pick_small.astype(BF16), low.astype(BF16)
        )
        write_pre = picked_small[:, 0:HEADS]
        forget_pre = picked_small[:, HEADS : 2 * HEADS]

        size = HEADS * BLK

        def token_of(at):
            at = lax.rem(at, BLK)
            return 2 * lax.rem(at, slots) + lax.rem(at // slots + me, 2)

        row = iota((size, size), 0)
        col = iota((size, size), 1)
        same = (row // BLK) == (col // BLK)
        causal = same & (token_of(row) >= token_of(col))
        strict = same & (token_of(row) > token_of(col))
        diagonal = row == col
        identity = jnp.where(diagonal, 1.0, 0.0)
        pick = iota((size, HEADS), 0) // BLK == iota((size, HEADS), 1)

        def as_column(block):
            return jnp.sum(jnp.where(pick, block, 0.0), axis=1, keepdims=True)

        def to_row(column):
            return jnp.sum(jnp.where(diagonal, column, 0.0), axis=0, keepdims=True)

        live = jnp.where(token_of(iota((size, 1), 0)) < length_ref[...], 1.0, 0.0)
        write_col = as_column(jnp.concatenate([write_pre] * HEADS, axis=0))
        forget_col = as_column(jnp.concatenate([forget_pre] * HEADS, axis=0))
        rate_col = as_column(jnp.broadcast_to(rates_ref[...], (size, HEADS)))
        write_gate = jax.nn.sigmoid(write_col) * live
        softplus = jnp.maximum(forget_col, 0.0) + jnp.log1p(jnp.exp(-jnp.abs(forget_col)))
        forget = -jnp.exp(rate_col) * softplus * live
        forget_row = to_row(forget)
        cumulative = jnp.sum(jnp.where(causal, forget_row, 0.0), axis=1, keepdims=True)
        final = jnp.sum(jnp.where(same, forget_row, 0.0), axis=1, keepdims=True)
        decay = jnp.where(
            causal, jnp.exp(jnp.minimum(cumulative - to_row(cumulative), 0.0)), 0.0
        )
        growth = jnp.exp(cumulative)
        fading = jnp.exp(final - cumulative)
        shrink = jnp.exp(final)

    with jax.named_scope("partwait0"):
        arrived("part0", part_send.at[0, pl.ds(0, devices - 1)])
    scope = jax.named_scope("mix0")
    scope.__enter__()
    upper = iota((BLK, wide), 0) < slots

    def by_head(pair):
        ahead, behind = [], []
        for chip in range(kv_size):
            mine = part_recv[pair, chip, 0].astype(F32)
            theirs = part_recv[pair, chip, 1].astype(F32)
            front = jnp.where(upper, mine, theirs)
            back = pltpu.roll(jnp.where(upper, theirs, mine), slots, 0)
            for start in range(0, wide, HEAD):
                ahead.append(front[:, start : start + HEAD])
                behind.append(back[:, start : start + HEAD])
        return jnp.concatenate(ahead, axis=0), jnp.concatenate(behind, axis=0)

    query, key_in = by_head(0)
    query_unit = (
        query
        * lax.rsqrt(jnp.sum(query * query, axis=1, keepdims=True) + EPSILON)
        * (1.0 / math.sqrt(HEAD))
    )
    key_unit = key_in * lax.rsqrt(jnp.sum(key_in * key_in, axis=1, keepdims=True) + EPSILON)
    products = dot_fine(jnp.concatenate([key_unit, query_unit], axis=0), key_unit, True)
    lower = products[:size]
    lower = jnp.where(strict, write_gate * decay * lower, 0.0)
    squared = dot_fine(lower, lower)
    fourth = dot_fine(squared, squared)
    inverse = dot_fine(identity - lower, identity + squared)
    inverse = dot_fine(inverse, identity + fourth)
    key_grown = (write_gate * growth) * key_unit
    query_grown = query_unit * growth
    scores = products[size:] * decay

    key_terms, query_terms = [], []
    for head in range(HEADS):
        at = slice(head * BLK, (head + 1) * BLK)
        high, low = cut_terms(jnp.concatenate([key_grown[at], query_grown[at]], axis=0))
        both = jnp.concatenate([high, low], axis=0).astype(BF16)
        result = dot(both, state_high[head])
        result = result[: 2 * BLK] + result[2 * BLK :]
        result = result + dot(both[: 2 * BLK], state_low[head])
        key_terms.append(result[:BLK])
        query_terms.append(result[BLK:])
    scope.__exit__(None, None, None)
    with jax.named_scope("partwait1"):
        arrived("part1", part_send.at[1, pl.ds(0, devices - 1)])
    scope = jax.named_scope("mix1")
    scope.__enter__()
    value, gating = by_head(1)
    update = dot_fine(inverse, write_gate * value - jnp.concatenate(key_terms, axis=0))
    attend = jnp.concatenate(query_terms, axis=0) + dot_fine(scores, update)
    normed = attend * lax.rsqrt(jnp.mean(attend * attend, axis=1, keepdims=True) + EPSILON)
    normed = normed * jax.nn.silu(gating) * live

    per_chip = wide // HEAD

    def lanes_of(chip):
        first = chip * per_chip
        return jnp.concatenate(
            [normed[(first + at) * BLK : (first + at + 1) * BLK] for at in range(per_chip)], axis=1
        )

    fronts, backs = [], []
    for chip in range(0, kv_size, 2):
        even, odd = lanes_of(chip), lanes_of(chip + 1)
        fronts.append(jnp.where(upper, even, pltpu.roll(odd, slots, 0)))
        backs.append(jnp.where(upper, pltpu.roll(even, slots, 0), odd))
    heads_send[0] = jnp.concatenate(fronts, axis=0).astype(BF16)
    heads_send[1] = jnp.concatenate(backs, axis=0).astype(BF16)
    to_all(
        "heads",
        lambda other, peer: heads_send.at[lax.rem(cls + other, 2)],
        lambda other: heads_recv.at[me],
    )
    heads_recv[me] = heads_send[cls]
    scope.__exit__(None, None, None)

    with jax.named_scope("newstate"):
        faded = key_unit * fading
        for head in range(HEADS):
            at = slice(head * BLK, (head + 1) * BLK)
            key_high, key_low = cut_terms(faded[at])
            value_high, value_low = cut_terms(update[at])
            outer = lax.dot_general(
                jnp.concatenate([key_high, key_high, key_low], axis=0).astype(BF16),
                jnp.concatenate([value_high, value_low, value_high], axis=0).astype(BF16),
                (((0,), (0,)), ((), ())),
                preferred_element_type=F32,
            )
            state_out[0, head] = shrink[head * BLK : head * BLK + 1] * state[head] + outer

    def hand_over(group, hidden, source):
        for off in far_first:
            chip = swapped(off)
            term = dot(hidden, down2[:, chip_rows(chip)]).astype(BF16)
            fin_send[group, off, 0] = term[:, :cols]
            fin_send[group, off, 1] = term[:, cols:]
            for other in (0, 1):
                core = core_of(chip, other)
                remote(
                    f"fin{group}", fin_send.at[group, off, core],
                    fin_recv.at[group, off, other], chip, core,
                )
        term = source.astype(F32) + 0.5 * dot(hidden, down2[:, chip_rows(kv)])
        own_send[group, 0] = term[:, :cols]
        own_send[group, 1] = term[:, cols:]
        to_partner(f"own{group}", own_send.at[group, 1 - tp], own_recv.at[group])

    def take_in(group):
        arrived(f"own{group}", own_recv.at[group])
        arrived(f"fin{group}", fin_recv.at[group, pl.ds(1, kv_size - 1)])
        sums = [own_send[group, tp], own_recv[group]]
        for other in (0, 1):
            total = fin_recv[group, 1, other].astype(F32)
            for off in range(2, kv_size):
                total = total + fin_recv[group, off, other].astype(F32)
            sums[other] = sums[other] + 0.5 * total
        return [total.astype(BF16) for total in sums]

    with jax.named_scope("dead_down"):
        loaded("down2")
        hand_over(1, dead_hidden, middle[1, kv])

    with jax.named_scope("gather2"):
        arrived("heads", heads_recv.at[pl.ds(0, devices - 1)])
        arrived("out", out_w.at[:, own_cols])
    with jax.named_scope("outproj"):
        blocks = heads_recv[...].reshape(devices * 2 * BLK, wide)
        mixed = dot(gather_heads, blocks).astype(BF16)
        terms = []
        for part in range(2):
            chips = range(part * kv_size // 2, (part + 1) * kv_size // 2)
            left = jnp.concatenate([mixed[chip * pack : (chip + 1) * pack] for chip in chips], axis=1)
            right = out_w[chips[0] * wide : (chips[-1] + 1) * wide, :]
            terms.append(dot(left, right).astype(BF16).astype(F32))
        second_in[kv] = (middle[0, kv].astype(F32) + (terms[0] + terms[1])).astype(BF16)
        to_class("second", lambda off: second_in.at[kv], lambda off: second_in.at[kv], kv_size)

    squares = jnp.zeros((pack, 1), F32)
    for index, off in enumerate([0] + near_first):
        chip = swapped(off)
        with jax.named_scope(f"second_wait{index}"):
            if index:
                arrived("second", second_in.at[chip], off)
        with jax.named_scope(f"live_slot{index}"):
            squares = squares + ffn_slot(
                live_acc, units2, gains2_ref, chip, second_in[chip], index == 0
            )
    with jax.named_scope("finish1"):
        hidden = finish(live_acc, squares)
    with jax.named_scope("down1"):
        hand_over(0, hidden, second_in[kv])
    with jax.named_scope("dead_in"):
        dead_sums = take_in(1)
    with jax.named_scope("live_in"):
        live_sums = take_in(0)
    with jax.named_scope("last"):
        packed = jnp.concatenate(
            [live_sums[0], dead_sums[0], live_sums[1], dead_sums[1]], axis=0
        )
        mixed_out_ref[...] = dot(restore, packed).astype(BF16)
    with jax.named_scope("tail"):
        totals = {
            "tokens": entered.at[pl.ds(0, devices - 1)],
            "lens": lens_all.at[pl.ds(0, devices - 1)],
            "proj": proj.at[:, 0 : 4 * cols],
            "out": out_w.at[:, own_cols],
            "small": small_acc.at[0],
            "heads": heads_recv.at[pl.ds(0, devices - 1)],
            "second": second_in.at[pl.ds(0, kv_size - 1)],
        }
        for index in range(2):
            totals[f"red{index}"] = red_send.at[index, pl.ds(1, kv_size - 1)]
            totals[f"middle{index}"] = middle.at[index, pl.ds(0, kv_size - 1)]
            totals[f"part{index}"] = part_send.at[index, pl.ds(0, devices - 1)]
            totals[f"fin{index}"] = fin_send.at[index, pl.ds(1, kv_size - 1)]
            totals[f"own{index}"] = own_send.at[index, 0]
        for name in sends:
            of_phase(name, totals[name]).wait_send()


def fused_call(mesh, *args):
    (
        tokens, lengths, state, gain_first, first_gate, first_up, first_down, gain_mix,
        query_weight, key_weight, value_weight, gating_weight, write_weight, forget_weight,
        forget_rate, out_weight, gain_second, second_gate, second_up, second_down,
    ) = args
    kv_size = mesh.shape["kv"]
    devices = kv_size * mesh.shape["tp"]
    rows, cols = tokens.shape
    wide = 2 * cols
    channels = gain_first.shape[0]
    hidden_local = first_gate.shape[1]
    half, pack = rows // 2, rows // 4
    in_hbm = pl.BlockSpec(memory_space=pltpu.HBM)
    in_vmem = pl.BlockSpec(memory_space=pltpu.VMEM)
    dma = pltpu.SemaphoreType.DMA
    operands = (
        tokens, lengths.reshape(1, 1), gain_first.reshape(1, -1), gain_mix.reshape(1, -1),
        gain_second.reshape(1, -1), forget_rate.reshape(1, -1), state,
        first_gate, first_up, first_down, query_weight, key_weight, value_weight,
        gating_weight, write_weight.T, forget_weight.T, out_weight, second_gate, second_up,
        second_down,
    )
    operands = [
        array if array.dtype == jnp.int32 else pltpu.with_memory_space_constraint(array, pltpu.HBM)
        for array in operands
    ]
    mixed_out, new_state = pl.pallas_call(
        functools.partial(fused_kernel, kv_size, channels),
        out_shape=(
            pltpu.VMEM(tokens.shape, tokens.dtype),
            pltpu.VMEM(state.shape, state.dtype),
        ),
        in_specs=[in_hbm] * len(operands),
        out_specs=(in_vmem, in_vmem),
        scratch_shapes=[
            pltpu.VMEM((channels, 2 * hidden_local), BF16),
            pltpu.VMEM((hidden_local, channels), BF16),
            pltpu.VMEM((channels, 2 * hidden_local), BF16),
            pltpu.VMEM((hidden_local, channels), BF16),
            pltpu.VMEM((channels, 4 * wide), BF16),
            pltpu.VMEM((channels, wide), BF16),
            pltpu.VMEM((HEAD, channels), BF16),
            pltpu.VMEM(state.shape[1:], F32),
            pltpu.VMEM(state.shape[1:], BF16),
            pltpu.VMEM(state.shape[1:], BF16),
            pltpu.VMEM((1, channels), F32),
            pltpu.VMEM((1, channels), F32),
            pltpu.VMEM((1, channels), F32),
            pltpu.VMEM((1, HEADS), F32),
            pltpu.VMEM((rows, cols), BF16),
            pltpu.VMEM((1, 1), jnp.int32),
            pltpu.VMEM((devices, 1, HEAD), jnp.int32),
            pltpu.VMEM((2, half, cols), BF16),
            pltpu.VMEM((devices, half, cols), BF16),
            pltpu.VMEM((half, 2 * hidden_local), F32),
            pltpu.VMEM((pack, 2 * hidden_local), F32),
            pltpu.VMEM((pack, 2 * hidden_local), F32),
            pltpu.VMEM((pack, 4 * wide), F32),
            pltpu.VMEM((1, pack, HEAD), F32),
            pltpu.VMEM((2, kv_size, pack, wide), BF16),
            pltpu.VMEM((kv_size, pack, wide), BF16),
            pltpu.VMEM((2, 2 * BLK, wide), BF16),
            pltpu.VMEM((devices, 2 * BLK, wide), BF16),
            pltpu.VMEM((2, kv_size, pack, wide), BF16),
            pltpu.VMEM((2, kv_size, pack, wide), BF16),
            pltpu.VMEM((2, devices, BLK, wide), BF16),
            pltpu.VMEM((2, kv_size, 2, BLK, wide), BF16),
            pltpu.VMEM((1, pack, HEAD), F32),
            pltpu.VMEM((2, kv_size, 2, pack, cols), BF16),
            pltpu.VMEM((2, kv_size, 2, pack, cols), BF16),
            pltpu.VMEM((2, 2, pack, cols), F32),
            pltpu.VMEM((2, pack, cols), F32),
            dma((kv_size + 13,)),
            dma((17,)),
            dma((3 * kv_size + 14,)),
        ],
        compiler_params=pltpu.CompilerParams(
            collective_id=0, has_side_effects=True, vmem_limit_bytes=VMEM_LIMIT
        ),
    )(*operands)
    return hand_out(mixed_out, new_state)


def hand_out_kernel(mixed, state, mixed_out_hbm, state_out_hbm, sems):
    puts = [
        pltpu.make_async_copy(mixed, mixed_out_hbm, sems.at[0]),
        pltpu.make_async_copy(state, state_out_hbm, sems.at[1]),
    ]
    for put in puts:
        put.start()
    for put in puts:
        put.wait()


def hand_out(mixed_out, new_state):
    in_hbm = pl.BlockSpec(memory_space=pltpu.HBM)
    in_vmem = pl.BlockSpec(memory_space=pltpu.VMEM)
    arrays = [
        pltpu.with_memory_space_constraint(array, pltpu.VMEM) for array in (mixed_out, new_state)
    ]
    return pl.pallas_call(
        hand_out_kernel,
        out_shape=tuple(jax.ShapeDtypeStruct(array.shape, array.dtype) for array in arrays),
        in_specs=[in_vmem, in_vmem],
        out_specs=(in_hbm, in_hbm),
        scratch_shapes=[pltpu.SemaphoreType.DMA((2,))],
        compiler_params=pltpu.CompilerParams(vmem_limit_bytes=8 * 1024 * 1024),
    )(*arrays)


def fits_fused(mesh, args):
    tokens, lengths, state, first_gate = args[0], args[1], args[2], args[4]
    rows, cols = tokens.shape
    kv_size = mesh.shape["kv"]
    devices = kv_size * mesh.shape["tp"]
    return (
        mesh.shape["tp"] == 2
        and mesh.shape["kv"] & (mesh.shape["kv"] - 1) == 0
        and lengths.shape[0] == 1
        and rows == devices * BLK
        and devices * 2 * BLK == HEAD
        and kv_size * BLK // 2 == 2 * BLK
        and devices * cols == HEADS * HEAD
        and cols % 256 == 0
        and first_gate.shape[1] % 128 == 0
        and state.shape[1:] == (HEADS, HEAD, HEAD)
    )


def solution(mesh):
    in_specs = (
        P("dp", ("kv", "tp")),
        P(("dp", "kv", "tp")),
        P(("dp", "kv", "tp"), None, None, None),
        P(),
        P(None, "kv"),
        P(None, "kv"),
        P("kv", None),
        P(),
        P(None, ("kv", "tp")),
        P(None, ("kv", "tp")),
        P(None, ("kv", "tp")),
        P(None, ("kv", "tp")),
        P(),
        P(),
        P(),
        P(None, ("kv", "tp")),
        P(),
        P(None, "kv"),
        P(None, "kv"),
        P("kv", None),
    )
    out_specs = (P("dp", ("kv", "tp")), P(("dp", "kv", "tp"), None, None, None))

    def body(*args):
        if fits_fused(mesh, args):
            return fused_call(mesh, *args)
        return per_device(*args)

    return jax.shard_map(
        body, mesh=mesh, in_specs=in_specs, out_specs=out_specs, check_vma=False
    )
```

```python
import functools
import math

import jax
import jax.numpy as jnp
from jax import lax
from jax.experimental import pallas as pl
from jax.experimental.pallas import tpu as pltpu
from jax.sharding import PartitionSpec as P

HEADS = 16
HEAD = 128
BLK = 8


EPSILON = 1e-06


def fold_step(gain, gate_cols, up_cols, portion):
    values = portion.astype(jnp.float32)
    scaled = (values * gain).astype(jnp.bfloat16)
    gate_acc = jnp.dot(scaled, gate_cols, preferred_element_type=jnp.float32)
    up_acc = jnp.dot(scaled, up_cols, preferred_element_type=jnp.float32)
    squares = jnp.sum(values * values, axis=1)
    return (gate_acc, up_acc, squares)


def finish_units(gate_acc, up_acc, squares, channels, down_rows):
    row_scale = lax.rsqrt(squares / channels + EPSILON)[:, None]
    hidden = (jax.nn.silu(gate_acc * row_scale) * (up_acc * row_scale)).astype(jnp.bfloat16)
    return jnp.dot(hidden, down_rows, preferred_element_type=jnp.float32)


def feed_forward(hidden_in, gain, w_gate, w_up, w_down):
    channels = gain.shape[0]
    paired = lax.all_to_all(hidden_in, "tp", split_axis=0, concat_axis=1, tiled=True)
    gate_acc, up_acc, squares = fold_step(
        gain, w_gate, w_up, lax.all_gather(paired, "kv", axis=1, tiled=True)
    )
    ffn_term = finish_units(gate_acc, up_acc, squares, channels, w_down)
    partial_value = lax.psum_scatter(ffn_term, "kv", scatter_dimension=1, tiled=True)
    summed = lax.all_to_all(partial_value, "tp", split_axis=1, concat_axis=0, tiled=True)
    return (hidden_in.astype(jnp.float32) + 0.5 * summed).astype(jnp.bfloat16)


def delta_block(query, key_in, value, gating, write_pre, forget_pre, rates, live, state):
    seq_count, block_len, head_count, head_size = query.shape
    precise = lax.Precision.HIGHEST
    query_unit = (
        query
        * lax.rsqrt(jnp.sum(query * query, axis=-1, keepdims=True) + EPSILON)
        / math.sqrt(head_size)
    )
    key_unit = key_in * lax.rsqrt(jnp.sum(key_in * key_in, axis=-1, keepdims=True) + EPSILON)
    live_rows = live[:, :, None]
    write_gate = jax.nn.sigmoid(write_pre) * live_rows
    forget = -jnp.exp(rates)[None, None, :] * jax.nn.softplus(forget_pre) * live_rows
    cumulative = jnp.cumsum(forget, axis=1)
    cum_heads = jnp.transpose(cumulative, (0, 2, 1))
    positions = jnp.arange(block_len)
    causal = positions[:, None] >= positions[None, :]
    strict = positions[:, None] > positions[None, :]
    differ = jnp.minimum(cum_heads[:, :, :, None] - cum_heads[:, :, None, :], 0.0)
    decay_mat = jnp.where(causal, jnp.exp(differ), 0.0)
    key_dots = jnp.einsum("sthd,suhd->shtu", key_unit, key_unit, precision=precise)
    write_heads = jnp.transpose(write_gate, (0, 2, 1))
    strict_part = jnp.where(strict, write_heads[:, :, :, None] * decay_mat * key_dots, 0.0)
    identity = jnp.eye(block_len, dtype=jnp.float32)
    squared = jnp.einsum("shtu,shuv->shtv", strict_part, strict_part, precision=precise)
    fourth = jnp.einsum("shtu,shuv->shtv", squared, squared, precision=precise)
    inverse = jnp.einsum(
        "shtu,shuv->shtv", identity - strict_part, identity + squared, precision=precise
    )
    inverse = jnp.einsum("shtu,shuv->shtv", inverse, identity + fourth, precision=precise)
    growth = jnp.exp(cumulative)
    target = jnp.einsum(
        "shtu,suhv->sthv", inverse, write_gate[..., None] * value, precision=precise
    )
    key_mix = jnp.einsum(
        "shtu,suhk->sthk", inverse, (write_gate * growth)[..., None] * key_unit, precision=precise
    )
    update = target - jnp.einsum("sthk,shkv->sthv", key_mix, state, precision=precise)
    scores = jnp.einsum("sthd,suhd->shtu", query_unit, key_unit, precision=precise) * decay_mat
    attend = jnp.einsum("sthk,shkv->sthv", query_unit * growth[..., None], state, precision=precise)
    attend = attend + jnp.einsum("shtu,suhv->sthv", scores, update, precision=precise)
    final_cum = cumulative[:, -1:, :]
    fading = jnp.exp(final_cum - cumulative)
    new_state = jnp.exp(final_cum[:, 0, :])[:, :, None, None] * state
    new_state = new_state + jnp.einsum(
        "sthk,sthv->shkv", key_unit * fading[..., None], update, precision=precise
    )
    normed = attend * lax.rsqrt(jnp.mean(attend * attend, axis=-1, keepdims=True) + EPSILON)
    normed = normed * jax.nn.silu(gating) * live[:, :, None, None]
    mixed_heads = normed.reshape(seq_count * block_len, head_count * head_size).astype(jnp.bfloat16)
    return (mixed_heads, new_state)


def per_device(
    tokens,
    lengths,
    state,
    gain_first,
    first_gate,
    first_up,
    first_down,
    gain_mix,
    query_weight,
    key_weight,
    value_weight,
    gating_weight,
    write_weight,
    forget_weight,
    forget_rate,
    out_weight,
    gain_second,
    second_gate,
    second_up,
    second_down,
):
    after_first = feed_forward(tokens, gain_first, first_gate, first_up, first_down)
    seq_count = lengths.shape[0]
    own_count = seq_count * BLK
    whole_rows = lax.all_gather(after_first, ("kv", "tp"), axis=1, tiled=True)
    scaled_all = (whole_rows.astype(jnp.float32) * gain_mix).astype(jnp.bfloat16)
    stacked = jnp.stack(
        [
            jnp.dot(scaled_all, matrix, preferred_element_type=jnp.float32)
            for matrix in (query_weight, key_weight, value_weight, gating_weight)
        ]
    )
    owned = lax.all_to_all(
        stacked.astype(jnp.bfloat16), ("kv", "tp"), split_axis=1, concat_axis=2, tiled=True
    ).astype(stacked.dtype)
    row_start = lax.axis_index(("kv", "tp")) * own_count
    own_values = lax.dynamic_slice_in_dim(whole_rows, row_start, own_count, 0).astype(jnp.float32)
    own_scaled = lax.dynamic_slice_in_dim(scaled_all, row_start, own_count, 0)
    mix_scale = lax.rsqrt(jnp.mean(own_values * own_values, axis=1, keepdims=True) + EPSILON)
    query = (owned[0] * mix_scale).reshape(seq_count, BLK, HEADS, HEAD)
    key_in = (owned[1] * mix_scale).reshape(seq_count, BLK, HEADS, HEAD)
    value = (owned[2] * mix_scale).reshape(seq_count, BLK, HEADS, HEAD)
    gating = (owned[3] * mix_scale).reshape(seq_count, BLK, HEADS, HEAD)
    write_pre = (
        jnp.dot(own_scaled, write_weight, preferred_element_type=jnp.float32) * mix_scale
    ).reshape(seq_count, BLK, HEADS)
    forget_pre = (
        jnp.dot(own_scaled, forget_weight, preferred_element_type=jnp.float32) * mix_scale
    ).reshape(seq_count, BLK, HEADS)
    positions = jnp.arange(BLK, dtype=jnp.int32)
    live = (positions[None, :] < lengths[:, None]).astype(jnp.float32)
    mixed_heads, new_state = delta_block(
        query, key_in, value, gating, write_pre, forget_pre, forget_rate, live, state
    )
    half_cols = mixed_heads.shape[1] // 2
    portion = lax.all_gather(mixed_heads, ("kv", "tp"), axis=0, tiled=True)
    first_half = jnp.dot(
        portion[:, :half_cols], out_weight[:half_cols], preferred_element_type=jnp.float32
    ).astype(jnp.bfloat16)
    second_half = jnp.dot(
        portion[:, half_cols:], out_weight[half_cols:], preferred_element_type=jnp.float32
    ).astype(jnp.bfloat16)
    first_half, second_half = lax.optimization_barrier((first_half, second_half))
    mixed_sum = first_half.astype(jnp.float32) + second_half.astype(jnp.float32)
    after_mix = (after_first.astype(jnp.float32) + mixed_sum).astype(jnp.bfloat16)
    mixed_out = feed_forward(after_mix, gain_second, second_gate, second_up, second_down)
    return (mixed_out, new_state)


F32 = jnp.float32
BF16 = jnp.bfloat16
MESH = pl.DeviceIdType.MESH
VMEM_LIMIT = 58 * 1024 * 1024


def fused_kernel(
    kv_size,
    channels,
    tokens_hbm,
    lengths_hbm,
    gains1_hbm,
    gains_mix_hbm,
    gains2_hbm,
    rates_hbm,
    state_hbm,
    gate1_hbm,
    up1_hbm,
    down1_hbm,
    query_hbm,
    key_hbm,
    value_hbm,
    gating_hbm,
    write_hbm,
    forget_hbm,
    out_hbm,
    gate2_hbm,
    up2_hbm,
    down2_hbm,
    packed_out,
    order_out,
    state_out,
    units1,
    down1,
    units2,
    down2,
    proj,
    out_w,
    small_w,
    state,
    state_high,
    state_low,
    gains1_ref,
    gains_mix_ref,
    gains2_ref,
    rates_ref,
    tokens_ref,
    length_ref,
    lens_all,
    picked,
    entered,
    unit_acc,
    live_acc,
    dead_acc,
    proj_acc,
    small_acc,
    middle,
    second_in,
    heads_send,
    heads_recv,
    red_send,
    red_recv,
    part_send,
    part_recv,
    small_recv,
    fin_send,
    fin_recv,
    own_send,
    own_recv,
    load_sems,
    send_sems,
    recv_sems,
):
    kv = lax.axis_index("kv")
    tp = lax.axis_index("tp")
    devices = 2 * kv_size
    me = kv * 2 + tp
    cls = lax.rem(kv + tp, 2)
    rows, cols = tokens_ref.shape
    wide = 2 * cols
    slots = BLK // 2
    half = rows // 2
    pack = rows // 4
    hidden_local = gate1_hbm.shape[1]
    own_cols = pl.ds(pl.multiple_of(tp * cols, cols), cols)
    inner = lax.rem((kv + 1) // 2, 2)
    near_first = [1, 2 + inner, 3 - inner]
    far_first = near_first[::-1]

    loads = {}

    def load(name, *pairs):
        sem = load_sems.at[len(loads)]
        loads[name] = [pltpu.make_async_copy(src, dst, sem) for src, dst in pairs]

    def start(name):
        for copy in loads[name]:
            copy.start()

    def loaded(name, ref=None):
        if ref is None:
            loads[name][0].wait()
        else:
            sem = load_sems.at[list(loads).index(name)]
            pltpu.make_async_copy(ref, ref, sem).wait()

    def swapped(off):
        chip, bit = 0, 1
        while bit < kv_size:
            chip = chip + bit * lax.rem(kv // bit + off // bit, 2)
            bit *= 2
        return chip

    def core_of(chip, other):
        return lax.rem(chip + cls + other, 2)

    def chip_rows(chip):
        return pl.ds(pl.multiple_of(chip * wide, wide), wide)

    def kind_cols(kind):
        return pl.ds(pl.multiple_of(kind * wide + tp * cols, cols), cols)

    load("length", (lengths_hbm, length_ref))
    load("tokens", (tokens_hbm, tokens_ref))
    load("gains1", (gains1_hbm, gains1_ref))
    for index, off in enumerate([0] + near_first):
        at = chip_rows(swapped(off))
        load(
            f"units1{index}",
            (gate1_hbm.at[at, :], units1.at[at, 0:hidden_local]),
            (up1_hbm.at[at, :], units1.at[at, hidden_local : 2 * hidden_local]),
        )
    early = list(loads)
    kinds = (query_hbm, key_hbm, value_hbm, gating_hbm)
    load("proj", *[(ref, proj.at[:, kind_cols(kind)]) for kind, ref in enumerate(kinds)])
    load("down1", (down1_hbm, down1))
    load(
        "small",
        (write_hbm, small_w.at[0:HEADS]),
        (forget_hbm, small_w.at[HEADS : 2 * HEADS]),
    )
    load("gains_mix", (gains_mix_hbm, gains_mix_ref))
    load("rates", (rates_hbm, rates_ref))
    load("out", (out_hbm, out_w.at[:, own_cols]))
    load("state", (state_hbm.at[0], state))
    load("gains2", (gains2_hbm, gains2_ref))
    load(
        "units2",
        (gate2_hbm, units2.at[:, 0:hidden_local]),
        (up2_hbm, units2.at[:, hidden_local : 2 * hidden_local]),
    )
    load("down2", (down2_hbm, down2))
    late = [name for name in loads if name not in early]
    for name in early[:2]:
        start(name)
    barrier = pltpu.get_barrier_semaphore()
    here = 0
    for off in far_first + [here]:
        for core in (tp, 1 - tp) if off is not here else (1 - tp,):
            pl.semaphore_signal(
                barrier, inc=1, device_id={"kv": swapped(off), "tp": core}, device_id_type=MESH
            )
    for name in early[2:]:
        start(name)

    sends, receives, width = {}, {}, [0]

    def remote(name, src, dst, chip, core, at=0, spread=1):
        sends.setdefault(name.rstrip("01"), len(sends))
        if name not in receives:
            receives[name] = width[0]
            width[0] += spread
        copy = pltpu.make_async_remote_copy(
            src_ref=src,
            dst_ref=dst,
            send_sem=send_sems.at[sends[name.rstrip("01")]],
            recv_sem=recv_sems.at[receives[name] + at],
            device_id={"kv": chip, "tp": core},
            device_id_type=MESH,
        )
        copy.start()

    def arrived(name, ref, at=0):
        sem = recv_sems.at[receives[name] + at]
        pltpu.make_async_remote_copy(
            src_ref=ref,
            dst_ref=ref,
            send_sem=sem,
            recv_sem=sem,
            device_id={"kv": kv, "tp": 1 - tp},
            device_id_type=MESH,
        ).wait_recv()

    def to_class(name, src, dst, spread=1):
        for off in far_first:
            chip = swapped(off)
            remote(name, src(off), dst(off), chip, core_of(chip, 0), off if spread > 1 else 0, spread)

    def to_all(name, src, dst, spread=1):
        for off in far_first:
            chip = swapped(off)
            same = lax.rem(off, 2)
            for other in (same, 1 - same):
                core = core_of(chip, other)
                remote(
                    name, src(other, chip * 2 + core), dst(other), chip, core,
                    off if spread > 1 else 0, spread,
                )
        to_partner(name, src(1, kv * 2 + 1 - tp), dst(1))

    def to_partner(name, src, dst):
        remote(name, src, dst, kv, 1 - tp)

    def columns_of(hidden, down, chips):
        right = jnp.concatenate([down[:, chip_rows(chip)] for chip in chips], axis=1)
        both = jnp.dot(hidden, right, preferred_element_type=F32)
        return [both[:, at * wide : (at + 1) * wide] for at in range(len(chips))]

    pairs = [(far_first[0], far_first[1]), (far_first[2], 0)]

    def iota(shape, axis):
        return lax.broadcasted_iota(jnp.int32, shape, axis)

    def dot(a, b):
        return jnp.dot(a, b, preferred_element_type=F32)

    def one_hot(mask):
        return jnp.where(mask, 1.0, 0.0).astype(BF16)

    row = iota((rows, rows), 0)
    col = iota((rows, rows), 1)
    at_class = lax.rem(row, half)
    at_seq = at_class // slots
    which = lax.rem(cls + row // half + at_seq, 2)
    picks = one_hot(col == at_seq * BLK + 2 * lax.rem(at_class, slots) + which)
    with jax.named_scope("small_wait"):
        loaded("length")
        loaded("tokens")
    lens_all[me] = jnp.broadcast_to(length_ref[...], (1, HEAD))
    chosen = dot(picks, tokens_ref[...]).astype(BF16)
    picked[...] = chosen.reshape(2, half, cols)
    entered[me] = chosen[:half]
    with jax.named_scope("barrier"):
        pl.semaphore_wait(barrier, devices - 1)
    to_all("tokens", lambda other, peer: picked.at[other], lambda other: entered.at[me], kv_size)
    to_all("lens", lambda other, peer: lens_all.at[me], lambda other: lens_all.at[me])
    for name in late:
        start(name)
    small_w[2 * HEADS :] = jnp.zeros((HEAD - 2 * HEADS, channels), BF16)

    def ffn_slot(acc, units, gain_ref, chip, portion, first):
        at = chip_rows(chip)
        values = portion.astype(F32)
        scaled = (values * gain_ref[:, at]).astype(BF16)
        term = dot(scaled, units[at, :])
        if first:
            acc[...] = term
        else:
            acc[...] += term
        return jnp.sum(values * values, axis=1, keepdims=True)

    def finish(acc, squares):
        row_scale = lax.rsqrt(squares / channels + EPSILON)
        gate = acc[:, 0:hidden_local] * row_scale
        up = acc[:, hidden_local : 2 * hidden_local] * row_scale
        return (jax.nn.silu(gate) * up).astype(BF16)

    def lengths_by(seq):
        found = jnp.zeros(seq.shape, jnp.int32)
        for index in range(devices):
            found = jnp.where(seq == index, lens_all[index], found)
        return found

    def is_live(seq, slot, klass):
        return 2 * slot + lax.rem(klass + seq, 2) < lengths_by(seq)

    def live_column(klass):
        at = iota((half, HEAD), 0)
        return jnp.where(is_live(at // slots, lax.rem(at, slots), klass), 1.0, 0.0)

    def live_row(klass):
        at = iota((1, HEAD), 1)
        live = is_live(at // slots, lax.rem(at, slots), klass) & (at < half)
        return jnp.where(live, 1.0, 0.0)

    def place_lanes(seq, slot, column):
        target = seq * slots + slot
        before = jnp.sum(
            jnp.where(iota((half, HEAD), 0) < target, column, 0.0), axis=0, keepdims=True
        )
        count = jnp.sum(column, axis=0, keepdims=True)
        rest = count + target.astype(F32) - before
        return jnp.where(is_live(seq, slot, cls), before, rest).astype(jnp.int32)

    def place_rows(seq, slot, klass, flags):
        target = seq * slots + slot
        before = jnp.sum(
            jnp.where(iota(seq.shape, 1) < target, flags, 0.0), axis=1, keepdims=True
        )
        count = jnp.sum(flags, axis=1, keepdims=True)
        rest = count + target.astype(F32) - before
        return jnp.where(is_live(seq, slot, klass), before, rest).astype(jnp.int32)

    def chip_tokens(chip):
        return jnp.concatenate([entered[chip * 2], entered[chip * 2 + 1]], axis=1)

    loaded("gains1")
    squares = jnp.zeros((half, 1), F32)
    for index, off in enumerate([0] + near_first):
        chip = swapped(off)
        with jax.named_scope(f"tokens_wait{index}"):
            if index:
                arrived("tokens", entered.at[pl.ds(chip * 2, 2)], off)
            else:
                arrived("tokens", entered.at[kv * 2 + 1 - tp], off)
            loaded(f"units1{index}", units1.at[chip_rows(chip), :])
            if index == kv_size - 1:
                arrived("lens", lens_all.at[pl.ds(0, devices - 1)])
        with jax.named_scope(f"units_slot{index}"):
            if index == kv_size - 1:
                column = live_column(cls)
                lane = iota((1, HEAD), 1)
                place = place_lanes(
                    jnp.minimum(lane // slots, devices - 1), lax.rem(lane, slots), column
                )
                reorder = one_hot(iota((half, HEAD), 0) == place)[:, :half]
            squares = squares + ffn_slot(
                unit_acc, units1, gains1_ref, chip, chip_tokens(chip), index == 0
            )
        if index == kv_size - 2:
            with jax.named_scope("exchange"):
                loaded("proj", proj.at[:, 0 : 4 * cols])
                for kind in range(4):
                    at = kind_cols(kind)
                    to_partner("proj", proj.at[:, at], proj.at[:, at])
    with jax.named_scope("finish0"):
        hidden = dot(reorder, finish(unit_acc, squares)).astype(BF16)
    with jax.named_scope("down_wait"):
        loaded("down1")
    with jax.named_scope("down0"):
        for pair in pairs:
            chips = [swapped(off) for off in pair]
            for off, chip, term in zip(pair, chips, columns_of(hidden, down1, chips)):
                if off is pairs[1][1]:
                    own_term = term
                    continue
                red_send[0, off] = term[:pack].astype(BF16)
                red_send[1, off] = term[pack:].astype(BF16)
                remote("red0", red_send.at[0, off], red_recv.at[0, off], chip, core_of(chip, 0))
    with jax.named_scope("exchange_out"):
        loaded("out")
        to_partner("out", out_w.at[:, own_cols], out_w.at[:, own_cols])
    with jax.named_scope("tables"):
        residual = dot(reorder, chip_tokens(kv))
        flags = live_row(cls)
        other_flags = live_row(1 - cls)
        at = iota((rows, HEAD), 0)
        slot = lax.rem(at, slots)
        place = place_rows(at // BLK, slot, cls, flags)
        kind = lax.rem(at // slots + cls, 2)
        lane = iota((rows, HEAD), 1)
        spread = one_hot(
            (lane // pack == kind) & (lax.rem(lane, pack) == place) & (lane < 2 * pack)
        )[:, : 2 * pack]
        lane = iota((1, devices * 2 * BLK), 1)
        place = place_lanes(lane // (2 * BLK), lax.rem(lane, slots), column)
        at = iota((kv_size * pack, devices * 2 * BLK), 0)
        chip_at = lax.rem(iota((kv_size * pack, devices * 2 * BLK), 1) // slots, kv_size)
        gather_heads = one_hot((at // pack == chip_at) & (lax.rem(at, pack) == place))
        at = iota((BLK, HEAD), 0)
        klass = at // slots
        place = place_rows(
            jnp.zeros((BLK, HEAD), jnp.int32) + me,
            lax.rem(at, slots),
            klass,
            jnp.where(klass == cls, flags, other_flags),
        )
        lane = iota((BLK, HEAD), 1)
        pick_small = jnp.where(
            (lax.rem(lane // pack + cls, 2) == klass)
            & (lax.rem(lane, pack) == place)
            & (lane < 2 * pack),
            1.0,
            0.0,
        )[:, : 2 * pack]
        at = iota((rows, HEAD), 0)
        seq, token = at // BLK, lax.rem(at, BLK)
        klass = lax.rem(seq + token, 2)
        place = place_rows(seq, token // 2, klass, jnp.where(klass == cls, flags, other_flags))
        lane = iota((rows, HEAD), 1)
        order_out[...] = one_hot(
            (lax.rem(lane // half + cls, 2) == klass)
            & (lax.rem(lane, half) == place)
            & (lane < rows)
        )[:, :rows]
    with jax.named_scope("statecut"):
        loaded("state")
        for head in range(HEADS):
            high = state[head].astype(BF16)
            state_high[head] = high
            state_low[head] = (state[head] - high.astype(F32)).astype(BF16)
    for off in far_first:
        chip = swapped(off)
        remote("red1", red_send.at[1, off], red_recv.at[1, off], chip, core_of(chip, 0))

    def first_done(group):
        at = slice(group * pack, (group + 1) * pack)
        arrived(f"red{group}", red_recv.at[group, pl.ds(1, kv_size - 1)])
        total = own_term[at]
        for off in range(1, kv_size):
            total = total + red_recv[group, off].astype(F32)
        middle[group, kv] = (residual[at] + 0.5 * total).astype(BF16)
        to_class(
            f"middle{group}",
            lambda off: middle.at[group, kv],
            lambda off: middle.at[group, kv],
            1 if group else kv_size,
        )

    with jax.named_scope("red0"):
        first_done(0)
    with jax.named_scope("proj_wait"):
        arrived("proj", proj.at[:, 0 : 4 * cols])
        loaded("small", small_w.at[0 : 2 * HEADS])
        loaded("gains_mix")
        loaded("rates")
    squares = jnp.zeros((pack, 1), F32)
    for index, off in enumerate([0] + near_first):
        chip = swapped(off)
        at = chip_rows(chip)
        with jax.named_scope(f"middle_wait{index}"):
            if index:
                arrived("middle0", middle.at[0, chip], off)
        with jax.named_scope(f"proj_slot{index}"):
            values = middle[0, chip].astype(F32)
            squares = squares + jnp.sum(values * values, axis=1, keepdims=True)
            scaled = (values * gains_mix_ref[:, at]).astype(BF16)
            small_term = lax.dot_general(
                scaled, small_w[:, at], (((1,), (1,)), ((), ())), preferred_element_type=F32
            )
            if index == 0:
                proj_acc[...] = dot(scaled, proj[at, :])
                small_acc[0] = small_term
                with jax.named_scope("red1"):
                    first_done(1)
            elif index < kv_size - 1:
                proj_acc[...] += dot(scaled, proj[at, :])
                small_acc[0] += small_term
    with jax.named_scope("partsend"):
        mix_scale = lax.rsqrt(squares / channels + EPSILON)
        for pair in range(2):
            lanes = slice(pair * 2 * wide, (pair + 1) * 2 * wide)
            projected = proj_acc[:, lanes] + dot(scaled, proj[at, lanes])
            projected = (projected * mix_scale).astype(BF16)
            stacked = jnp.concatenate([projected[:, :wide], projected[:, wide:]], axis=0)
            part = dot(spread, stacked).astype(BF16)
            part_send[pair] = part.reshape(devices, BLK, wide)
            to_all(
                f"part{pair}",
                lambda other, peer: part_send.at[pair, peer],
                lambda other: part_recv.at[pair, kv, cls],
            )
            if pair == 0:
                small_acc[0] = (small_acc[0] + small_term) * mix_scale
                to_partner("small", small_acc.at[0], small_recv.at[0])
        for pair in range(2):
            part_recv[pair, kv, cls] = part_send[pair, me]

    def cut_terms(a):
        high = a.astype(BF16).astype(F32)
        return high, a - high

    def dot_fine(a, b, across=False):
        high_a, low_a = cut_terms(a)
        high_b, low_b = cut_terms(b)
        axis = 1 if across else 0
        left = jnp.concatenate([high_a, high_a, low_a], axis=1).astype(BF16)
        right = jnp.concatenate([high_b, low_b, high_b], axis=axis).astype(BF16)
        return lax.dot_general(
            left, right, (((1,), (axis,)), ((), ())), preferred_element_type=F32
        )

    with jax.named_scope("premix"):
        arrived("small", small_recv.at[0])
        small_all = jnp.concatenate([small_acc[0], small_recv[0]], axis=0)
        high, low = cut_terms(small_all)
        picked_small = dot(pick_small.astype(BF16), high.astype(BF16)) + dot(
            pick_small.astype(BF16), low.astype(BF16)
        )
        write_pre = picked_small[:, 0:HEADS]
        forget_pre = picked_small[:, HEADS : 2 * HEADS]

        size = HEADS * BLK

        def token_of(at):
            at = lax.rem(at, BLK)
            return 2 * lax.rem(at, slots) + lax.rem(at // slots + me, 2)

        row = iota((size, size), 0)
        col = iota((size, size), 1)
        same = (row // BLK) == (col // BLK)
        causal = same & (token_of(row) >= token_of(col))
        strict = same & (token_of(row) > token_of(col))
        diagonal = row == col
        identity = jnp.where(diagonal, 1.0, 0.0)
        pick = iota((size, HEADS), 0) // BLK == iota((size, HEADS), 1)

        def as_column(block):
            return jnp.sum(jnp.where(pick, block, 0.0), axis=1, keepdims=True)

        def to_row(column):
            return jnp.sum(jnp.where(diagonal, column, 0.0), axis=0, keepdims=True)

        live = jnp.where(token_of(iota((size, 1), 0)) < length_ref[...], 1.0, 0.0)
        write_col = as_column(jnp.concatenate([write_pre] * HEADS, axis=0))
        forget_col = as_column(jnp.concatenate([forget_pre] * HEADS, axis=0))
        rate_col = as_column(jnp.broadcast_to(rates_ref[...], (size, HEADS)))
        write_gate = jax.nn.sigmoid(write_col) * live
        softplus = jnp.maximum(forget_col, 0.0) + jnp.log1p(jnp.exp(-jnp.abs(forget_col)))
        forget = -jnp.exp(rate_col) * softplus * live
        forget_row = to_row(forget)
        cumulative = jnp.sum(jnp.where(causal, forget_row, 0.0), axis=1, keepdims=True)
        final = jnp.sum(jnp.where(same, forget_row, 0.0), axis=1, keepdims=True)
        decay = jnp.where(
            causal, jnp.exp(jnp.minimum(cumulative - to_row(cumulative), 0.0)), 0.0
        )
        growth = jnp.exp(cumulative)
        fading = jnp.exp(final - cumulative)
        shrink = jnp.exp(final)

    with jax.named_scope("dead_units"):
        loaded("gains2")
        loaded("units2", units2)
        arrived("middle1", middle.at[1, pl.ds(0, kv_size - 1)])
        values = jnp.concatenate([middle[1, chip] for chip in range(kv_size)], axis=1).astype(F32)
        squares = jnp.sum(values * values, axis=1, keepdims=True)
        dead_acc[...] = dot((values * gains2_ref[...]).astype(BF16), units2[...])
        dead_hidden = finish(dead_acc, squares)

    with jax.named_scope("partwait0"):
        arrived("part0", part_send.at[0, pl.ds(0, devices - 1)])
    scope = jax.named_scope("mix0")
    scope.__enter__()
    upper = iota((BLK, wide), 0) < slots

    def by_head(pair):
        ahead, behind = [], []
        for chip in range(kv_size):
            mine = part_recv[pair, chip, 0].astype(F32)
            theirs = part_recv[pair, chip, 1].astype(F32)
            front = jnp.where(upper, mine, theirs)
            back = pltpu.roll(jnp.where(upper, theirs, mine), slots, 0)
            for start in range(0, wide, HEAD):
                ahead.append(front[:, start : start + HEAD])
                behind.append(back[:, start : start + HEAD])
        return jnp.concatenate(ahead, axis=0), jnp.concatenate(behind, axis=0)

    query, key_in = by_head(0)
    query_unit = (
        query
        * lax.rsqrt(jnp.sum(query * query, axis=1, keepdims=True) + EPSILON)
        * (1.0 / math.sqrt(HEAD))
    )
    key_unit = key_in * lax.rsqrt(jnp.sum(key_in * key_in, axis=1, keepdims=True) + EPSILON)
    products = dot_fine(jnp.concatenate([key_unit, query_unit], axis=0), key_unit, True)
    lower = products[:size]
    lower = jnp.where(strict, write_gate * decay * lower, 0.0)
    squared = dot_fine(lower, lower)
    fourth = dot_fine(squared, squared)
    inverse = dot_fine(identity - lower, identity + squared)
    inverse = dot_fine(inverse, identity + fourth)
    key_grown = (write_gate * growth) * key_unit
    query_grown = query_unit * growth
    scores = products[size:] * decay

    key_terms, query_terms = [], []
    for head in range(HEADS):
        at = slice(head * BLK, (head + 1) * BLK)
        high, low = cut_terms(jnp.concatenate([key_grown[at], query_grown[at]], axis=0))
        both = jnp.concatenate([high, low], axis=0).astype(BF16)
        result = dot(both, state_high[head])
        result = result[: 2 * BLK] + result[2 * BLK :]
        result = result + dot(both[: 2 * BLK], state_low[head])
        key_terms.append(result[:BLK])
        query_terms.append(result[BLK:])
    scope.__exit__(None, None, None)
    with jax.named_scope("partwait1"):
        arrived("part1", part_send.at[1, pl.ds(0, devices - 1)])
    scope = jax.named_scope("mix1")
    scope.__enter__()
    value, gating = by_head(1)
    update = dot_fine(inverse, write_gate * value - jnp.concatenate(key_terms, axis=0))
    attend = jnp.concatenate(query_terms, axis=0) + dot_fine(scores, update)
    normed = attend * lax.rsqrt(jnp.mean(attend * attend, axis=1, keepdims=True) + EPSILON)
    normed = normed * jax.nn.silu(gating) * live

    per_chip = wide // HEAD

    def lanes_of(chip):
        first = chip * per_chip
        return jnp.concatenate(
            [normed[(first + at) * BLK : (first + at + 1) * BLK] for at in range(per_chip)], axis=1
        )

    fronts, backs = [], []
    for chip in range(0, kv_size, 2):
        even, odd = lanes_of(chip), lanes_of(chip + 1)
        fronts.append(jnp.where(upper, even, pltpu.roll(odd, slots, 0)))
        backs.append(jnp.where(upper, pltpu.roll(even, slots, 0), odd))
    heads_send[0] = jnp.concatenate(fronts, axis=0).astype(BF16)
    heads_send[1] = jnp.concatenate(backs, axis=0).astype(BF16)
    to_all(
        "heads",
        lambda other, peer: heads_send.at[lax.rem(cls + other, 2)],
        lambda other: heads_recv.at[me],
    )
    heads_recv[me] = heads_send[cls]
    scope.__exit__(None, None, None)

    with jax.named_scope("newstate"):
        faded = key_unit * fading
        for head in range(HEADS):
            at = slice(head * BLK, (head + 1) * BLK)
            key_high, key_low = cut_terms(faded[at])
            value_high, value_low = cut_terms(update[at])
            outer = lax.dot_general(
                jnp.concatenate([key_high, key_high, key_low], axis=0).astype(BF16),
                jnp.concatenate([value_high, value_low, value_high], axis=0).astype(BF16),
                (((0,), (0,)), ((), ())),
                preferred_element_type=F32,
            )
            state_out[0, head] = shrink[head * BLK : head * BLK + 1] * state[head] + outer

    def hand_off(group, off):
        chip = swapped(off)
        for other in (0, 1):
            core = core_of(chip, other)
            remote(
                f"fin{group}", fin_send.at[group, off, core],
                fin_recv.at[group, off, other], chip, core,
            )

    def hand_own(group):
        to_partner(f"own{group}", own_send.at[group, 1 - tp], own_recv.at[group])

    def second_down(group, hidden, source, at_once):
        for pair in pairs:
            chips = [swapped(off) for off in pair]
            for off, chip, term in zip(pair, chips, columns_of(hidden, down2, chips)):
                if off is pairs[1][1]:
                    term = source.astype(F32) + 0.5 * term
                    own_send[group, 0] = term[:, :cols]
                    own_send[group, 1] = term[:, cols:]
                    continue
                fin_send[group, off, 0] = term[:, :cols].astype(BF16)
                fin_send[group, off, 1] = term[:, cols:].astype(BF16)
                if at_once:
                    hand_off(group, off)
        if at_once:
            hand_own(group)

    def take_in(group):
        arrived(f"own{group}", own_recv.at[group])
        arrived(f"fin{group}", fin_recv.at[group, pl.ds(1, kv_size - 1)])
        sums = [own_send[group, tp], own_recv[group]]
        for other in (0, 1):
            total = fin_recv[group, 1, other].astype(F32)
            for off in range(2, kv_size):
                total = total + fin_recv[group, off, other].astype(F32)
            sums[other] = sums[other] + 0.5 * total
        return [total.astype(BF16) for total in sums]

    with jax.named_scope("dead_down"):
        loaded("down2")
        second_down(1, dead_hidden, middle[1, kv], False)
    with jax.named_scope("gather2"):
        arrived("heads", heads_recv.at[pl.ds(0, devices - 1)])
        arrived("out", out_w.at[:, own_cols])
    with jax.named_scope("outproj"):
        blocks = heads_recv[...].reshape(devices * 2 * BLK, wide)
        mixed = dot(gather_heads, blocks).astype(BF16)
        terms = []
        for part in range(2):
            chips = range(part * kv_size // 2, (part + 1) * kv_size // 2)
            left = jnp.concatenate([mixed[chip * pack : (chip + 1) * pack] for chip in chips], axis=1)
            right = out_w[chips[0] * wide : (chips[-1] + 1) * wide, :]
            terms.append(dot(left, right).astype(BF16).astype(F32))
        second_in[kv] = (middle[0, kv].astype(F32) + (terms[0] + terms[1])).astype(BF16)
        to_class("second", lambda off: second_in.at[kv], lambda off: second_in.at[kv], kv_size)

    squares = jnp.zeros((pack, 1), F32)
    for index, off in enumerate([0] + near_first):
        chip = swapped(off)
        with jax.named_scope(f"second_wait{index}"):
            if index:
                arrived("second", second_in.at[chip], off)
        with jax.named_scope(f"live_slot{index}"):
            squares = squares + ffn_slot(
                live_acc, units2, gains2_ref, chip, second_in[chip], index == 0
            )
        if index == 1:
            with jax.named_scope("dead_off"):
                for off in far_first:
                    hand_off(1, off)
                hand_own(1)
    with jax.named_scope("finish1"):
        hidden = finish(live_acc, squares)
    with jax.named_scope("down1"):
        second_down(0, hidden, second_in[kv], True)
    with jax.named_scope("dead_in"):
        dead_sums = take_in(1)
    with jax.named_scope("live_in"):
        live_sums = take_in(0)
    with jax.named_scope("last"):
        packed_out[...] = jnp.concatenate(
            [live_sums[0], dead_sums[0], live_sums[1], dead_sums[1]], axis=0
        )
    with jax.named_scope("tail"):
        totals = {
            "tokens": entered.at[pl.ds(0, devices - 1)],
            "lens": lens_all.at[pl.ds(0, devices - 1)],
            "proj": proj.at[:, 0 : 4 * cols],
            "out": out_w.at[:, own_cols],
            "small": small_acc.at[0],
            "heads": heads_recv.at[pl.ds(0, devices - 1)],
            "second": second_in.at[pl.ds(0, kv_size - 1)],
            "red": red_send.at[:, pl.ds(1, kv_size - 1)],
            "middle": middle.at[:, pl.ds(0, kv_size - 1)],
            "part": part_send.at[:, pl.ds(0, devices - 1)],
            "fin": fin_send.at[:, pl.ds(1, kv_size - 1)],
            "own": own_send.at[0],
        }
        for name, ref in totals.items():
            sem = send_sems.at[sends[name]]
            pltpu.make_async_remote_copy(
                src_ref=ref,
                dst_ref=ref,
                send_sem=sem,
                recv_sem=sem,
                device_id={"kv": kv, "tp": 1 - tp},
                device_id_type=MESH,
            ).wait_send()


def fused_call(mesh, *args):
    (
        tokens, lengths, state, gain_first, first_gate, first_up, first_down, gain_mix,
        query_weight, key_weight, value_weight, gating_weight, write_weight, forget_weight,
        forget_rate, out_weight, gain_second, second_gate, second_up, second_down,
    ) = args
    kv_size = mesh.shape["kv"]
    devices = kv_size * mesh.shape["tp"]
    rows, cols = tokens.shape
    wide = 2 * cols
    channels = gain_first.shape[0]
    hidden_local = first_gate.shape[1]
    half, pack = rows // 2, rows // 4
    in_hbm = pl.BlockSpec(memory_space=pltpu.HBM)
    in_vmem = pl.BlockSpec(memory_space=pltpu.VMEM)
    dma = pltpu.SemaphoreType.DMA
    operands = (
        tokens, lengths.reshape(1, 1), gain_first.reshape(1, -1), gain_mix.reshape(1, -1),
        gain_second.reshape(1, -1), forget_rate.reshape(1, -1), state,
        first_gate, first_up, first_down, query_weight, key_weight, value_weight,
        gating_weight, write_weight.T, forget_weight.T, out_weight, second_gate, second_up,
        second_down,
    )
    operands = [
        array if array.dtype == jnp.int32 else pltpu.with_memory_space_constraint(array, pltpu.HBM)
        for array in operands
    ]
    results = pl.pallas_call(
        functools.partial(fused_kernel, kv_size, channels),
        out_shape=(
            pltpu.VMEM(tokens.shape, tokens.dtype),
            pltpu.VMEM((rows, rows), BF16),
            pltpu.VMEM(state.shape, state.dtype),
        ),
        in_specs=[in_hbm] * len(operands),
        out_specs=(in_vmem, in_vmem, in_vmem),
        scratch_shapes=[
            pltpu.VMEM((channels, 2 * hidden_local), BF16),
            pltpu.VMEM((hidden_local, channels), BF16),
            pltpu.VMEM((channels, 2 * hidden_local), BF16),
            pltpu.VMEM((hidden_local, channels), BF16),
            pltpu.VMEM((channels, 4 * wide), BF16),
            pltpu.VMEM((channels, wide), BF16),
            pltpu.VMEM((HEAD, channels), BF16),
            pltpu.VMEM(state.shape[1:], F32),
            pltpu.VMEM(state.shape[1:], BF16),
            pltpu.VMEM(state.shape[1:], BF16),
            pltpu.VMEM((1, channels), F32),
            pltpu.VMEM((1, channels), F32),
            pltpu.VMEM((1, channels), F32),
            pltpu.VMEM((1, HEADS), F32),
            pltpu.VMEM((rows, cols), BF16),
            pltpu.VMEM((1, 1), jnp.int32),
            pltpu.VMEM((devices, 1, HEAD), jnp.int32),
            pltpu.VMEM((2, half, cols), BF16),
            pltpu.VMEM((devices, half, cols), BF16),
            pltpu.VMEM((half, 2 * hidden_local), F32),
            pltpu.VMEM((pack, 2 * hidden_local), F32),
            pltpu.VMEM((pack, 2 * hidden_local), F32),
            pltpu.VMEM((pack, 4 * wide), F32),
            pltpu.VMEM((1, pack, HEAD), F32),
            pltpu.VMEM((2, kv_size, pack, wide), BF16),
            pltpu.VMEM((kv_size, pack, wide), BF16),
            pltpu.VMEM((2, 2 * BLK, wide), BF16),
            pltpu.VMEM((devices, 2 * BLK, wide), BF16),
            pltpu.VMEM((2, kv_size, pack, wide), BF16),
            pltpu.VMEM((2, kv_size, pack, wide), BF16),
            pltpu.VMEM((2, devices, BLK, wide), BF16),
            pltpu.VMEM((2, kv_size, 2, BLK, wide), BF16),
            pltpu.VMEM((1, pack, HEAD), F32),
            pltpu.VMEM((2, kv_size, 2, pack, cols), BF16),
            pltpu.VMEM((2, kv_size, 2, pack, cols), BF16),
            pltpu.VMEM((2, 2, pack, cols), F32),
            pltpu.VMEM((2, pack, cols), F32),
            dma((kv_size + 13,)),
            dma((12,)),
            dma((3 * kv_size + 14,)),
        ],
        compiler_params=pltpu.CompilerParams(
            collective_id=0, has_side_effects=True, vmem_limit_bytes=VMEM_LIMIT
        ),
    )(*operands)
    return hand_out(*results)


def hand_out_kernel(packed, order, state, mixed_hbm, state_hbm, mixed, sems):
    put_state = pltpu.make_async_copy(state, state_hbm, sems.at[0])
    put_state.start()
    restored = jnp.dot(order[...], packed[...], preferred_element_type=F32)
    mixed[...] = restored.astype(BF16)
    put_mixed = pltpu.make_async_copy(mixed, mixed_hbm, sems.at[1])
    put_mixed.start()
    put_mixed.wait()
    put_state.wait()


def hand_out(packed, order, new_state):
    in_hbm = pl.BlockSpec(memory_space=pltpu.HBM)
    in_vmem = pl.BlockSpec(memory_space=pltpu.VMEM)
    arrays = [
        pltpu.with_memory_space_constraint(array, pltpu.VMEM)
        for array in (packed, order, new_state)
    ]
    return pl.pallas_call(
        hand_out_kernel,
        out_shape=(
            jax.ShapeDtypeStruct(packed.shape, packed.dtype),
            jax.ShapeDtypeStruct(new_state.shape, new_state.dtype),
        ),
        in_specs=[in_vmem] * 3,
        out_specs=(in_hbm, in_hbm),
        scratch_shapes=[
            pltpu.VMEM(packed.shape, packed.dtype),
            pltpu.SemaphoreType.DMA((2,)),
        ],
        compiler_params=pltpu.CompilerParams(vmem_limit_bytes=8 * 1024 * 1024),
    )(*arrays)


def fits_fused(mesh, args):
    tokens, lengths, state, first_gate = args[0], args[1], args[2], args[4]
    rows, cols = tokens.shape
    kv_size = mesh.shape["kv"]
    devices = kv_size * mesh.shape["tp"]
    return (
        mesh.shape["tp"] == 2
        and mesh.shape["kv"] & (mesh.shape["kv"] - 1) == 0
        and lengths.shape[0] == 1
        and rows == devices * BLK
        and devices * 2 * BLK == HEAD
        and kv_size * BLK // 2 == 2 * BLK
        and devices * cols == HEADS * HEAD
        and cols % 256 == 0
        and first_gate.shape[1] % 128 == 0
        and state.shape[1:] == (HEADS, HEAD, HEAD)
    )


def solution(mesh):
    in_specs = (
        P("dp", ("kv", "tp")),
        P(("dp", "kv", "tp")),
        P(("dp", "kv", "tp"), None, None, None),
        P(),
        P(None, "kv"),
        P(None, "kv"),
        P("kv", None),
        P(),
        P(None, ("kv", "tp")),
        P(None, ("kv", "tp")),
        P(None, ("kv", "tp")),
        P(None, ("kv", "tp")),
        P(),
        P(),
        P(),
        P(None, ("kv", "tp")),
        P(),
        P(None, "kv"),
        P(None, "kv"),
        P("kv", None),
    )
    out_specs = (P("dp", ("kv", "tp")), P(("dp", "kv", "tp"), None, None, None))

    def body(*args):
        if fits_fused(mesh, args):
            return fused_call(mesh, *args)
        return per_device(*args)

    return jax.shard_map(
        body, mesh=mesh, in_specs=in_specs, out_specs=out_specs, check_vma=False
    )
```

```python
import functools
import math

import jax
import jax.numpy as jnp
from jax import lax
from jax.experimental import pallas as pl
from jax.experimental.pallas import tpu as pltpu
from jax.sharding import PartitionSpec as P

HEADS = 16
HEAD = 128
BLK = 8


EPSILON = 1e-06


def fold_step(gain, gate_cols, up_cols, portion):
    values = portion.astype(jnp.float32)
    scaled = (values * gain).astype(jnp.bfloat16)
    gate_acc = jnp.dot(scaled, gate_cols, preferred_element_type=jnp.float32)
    up_acc = jnp.dot(scaled, up_cols, preferred_element_type=jnp.float32)
    squares = jnp.sum(values * values, axis=1)
    return (gate_acc, up_acc, squares)


def finish_units(gate_acc, up_acc, squares, channels, down_rows):
    row_scale = lax.rsqrt(squares / channels + EPSILON)[:, None]
    hidden = (jax.nn.silu(gate_acc * row_scale) * (up_acc * row_scale)).astype(jnp.bfloat16)
    return jnp.dot(hidden, down_rows, preferred_element_type=jnp.float32)


def feed_forward(hidden_in, gain, w_gate, w_up, w_down):
    channels = gain.shape[0]
    paired = lax.all_to_all(hidden_in, "tp", split_axis=0, concat_axis=1, tiled=True)
    gate_acc, up_acc, squares = fold_step(
        gain, w_gate, w_up, lax.all_gather(paired, "kv", axis=1, tiled=True)
    )
    ffn_term = finish_units(gate_acc, up_acc, squares, channels, w_down)
    partial_value = lax.psum_scatter(ffn_term, "kv", scatter_dimension=1, tiled=True)
    summed = lax.all_to_all(partial_value, "tp", split_axis=1, concat_axis=0, tiled=True)
    return (hidden_in.astype(jnp.float32) + 0.5 * summed).astype(jnp.bfloat16)


def delta_block(query, key_in, value, gating, write_pre, forget_pre, rates, live, state):
    seq_count, block_len, head_count, head_size = query.shape
    precise = lax.Precision.HIGHEST
    query_unit = (
        query
        * lax.rsqrt(jnp.sum(query * query, axis=-1, keepdims=True) + EPSILON)
        / math.sqrt(head_size)
    )
    key_unit = key_in * lax.rsqrt(jnp.sum(key_in * key_in, axis=-1, keepdims=True) + EPSILON)
    live_rows = live[:, :, None]
    write_gate = jax.nn.sigmoid(write_pre) * live_rows
    forget = -jnp.exp(rates)[None, None, :] * jax.nn.softplus(forget_pre) * live_rows
    cumulative = jnp.cumsum(forget, axis=1)
    cum_heads = jnp.transpose(cumulative, (0, 2, 1))
    positions = jnp.arange(block_len)
    causal = positions[:, None] >= positions[None, :]
    strict = positions[:, None] > positions[None, :]
    differ = jnp.minimum(cum_heads[:, :, :, None] - cum_heads[:, :, None, :], 0.0)
    decay_mat = jnp.where(causal, jnp.exp(differ), 0.0)
    key_dots = jnp.einsum("sthd,suhd->shtu", key_unit, key_unit, precision=precise)
    write_heads = jnp.transpose(write_gate, (0, 2, 1))
    strict_part = jnp.where(strict, write_heads[:, :, :, None] * decay_mat * key_dots, 0.0)
    identity = jnp.eye(block_len, dtype=jnp.float32)
    squared = jnp.einsum("shtu,shuv->shtv", strict_part, strict_part, precision=precise)
    fourth = jnp.einsum("shtu,shuv->shtv", squared, squared, precision=precise)
    inverse = jnp.einsum(
        "shtu,shuv->shtv", identity - strict_part, identity + squared, precision=precise
    )
    inverse = jnp.einsum("shtu,shuv->shtv", inverse, identity + fourth, precision=precise)
    growth = jnp.exp(cumulative)
    target = jnp.einsum(
        "shtu,suhv->sthv", inverse, write_gate[..., None] * value, precision=precise
    )
    key_mix = jnp.einsum(
        "shtu,suhk->sthk", inverse, (write_gate * growth)[..., None] * key_unit, precision=precise
    )
    update = target - jnp.einsum("sthk,shkv->sthv", key_mix, state, precision=precise)
    scores = jnp.einsum("sthd,suhd->shtu", query_unit, key_unit, precision=precise) * decay_mat
    attend = jnp.einsum("sthk,shkv->sthv", query_unit * growth[..., None], state, precision=precise)
    attend = attend + jnp.einsum("shtu,suhv->sthv", scores, update, precision=precise)
    final_cum = cumulative[:, -1:, :]
    fading = jnp.exp(final_cum - cumulative)
    new_state = jnp.exp(final_cum[:, 0, :])[:, :, None, None] * state
    new_state = new_state + jnp.einsum(
        "sthk,sthv->shkv", key_unit * fading[..., None], update, precision=precise
    )
    normed = attend * lax.rsqrt(jnp.mean(attend * attend, axis=-1, keepdims=True) + EPSILON)
    normed = normed * jax.nn.silu(gating) * live[:, :, None, None]
    mixed_heads = normed.reshape(seq_count * block_len, head_count * head_size).astype(jnp.bfloat16)
    return (mixed_heads, new_state)


def per_device(
    tokens,
    lengths,
    state,
    gain_first,
    first_gate,
    first_up,
    first_down,
    gain_mix,
    query_weight,
    key_weight,
    value_weight,
    gating_weight,
    write_weight,
    forget_weight,
    forget_rate,
    out_weight,
    gain_second,
    second_gate,
    second_up,
    second_down,
):
    after_first = feed_forward(tokens, gain_first, first_gate, first_up, first_down)
    seq_count = lengths.shape[0]
    own_count = seq_count * BLK
    whole_rows = lax.all_gather(after_first, ("kv", "tp"), axis=1, tiled=True)
    scaled_all = (whole_rows.astype(jnp.float32) * gain_mix).astype(jnp.bfloat16)
    stacked = jnp.stack(
        [
            jnp.dot(scaled_all, matrix, preferred_element_type=jnp.float32)
            for matrix in (query_weight, key_weight, value_weight, gating_weight)
        ]
    )
    owned = lax.all_to_all(
        stacked.astype(jnp.bfloat16), ("kv", "tp"), split_axis=1, concat_axis=2, tiled=True
    ).astype(stacked.dtype)
    row_start = lax.axis_index(("kv", "tp")) * own_count
    own_values = lax.dynamic_slice_in_dim(whole_rows, row_start, own_count, 0).astype(jnp.float32)
    own_scaled = lax.dynamic_slice_in_dim(scaled_all, row_start, own_count, 0)
    mix_scale = lax.rsqrt(jnp.mean(own_values * own_values, axis=1, keepdims=True) + EPSILON)
    query = (owned[0] * mix_scale).reshape(seq_count, BLK, HEADS, HEAD)
    key_in = (owned[1] * mix_scale).reshape(seq_count, BLK, HEADS, HEAD)
    value = (owned[2] * mix_scale).reshape(seq_count, BLK, HEADS, HEAD)
    gating = (owned[3] * mix_scale).reshape(seq_count, BLK, HEADS, HEAD)
    write_pre = (
        jnp.dot(own_scaled, write_weight, preferred_element_type=jnp.float32) * mix_scale
    ).reshape(seq_count, BLK, HEADS)
    forget_pre = (
        jnp.dot(own_scaled, forget_weight, preferred_element_type=jnp.float32) * mix_scale
    ).reshape(seq_count, BLK, HEADS)
    positions = jnp.arange(BLK, dtype=jnp.int32)
    live = (positions[None, :] < lengths[:, None]).astype(jnp.float32)
    mixed_heads, new_state = delta_block(
        query, key_in, value, gating, write_pre, forget_pre, forget_rate, live, state
    )
    half_cols = mixed_heads.shape[1] // 2
    portion = lax.all_gather(mixed_heads, ("kv", "tp"), axis=0, tiled=True)
    first_half = jnp.dot(
        portion[:, :half_cols], out_weight[:half_cols], preferred_element_type=jnp.float32
    ).astype(jnp.bfloat16)
    second_half = jnp.dot(
        portion[:, half_cols:], out_weight[half_cols:], preferred_element_type=jnp.float32
    ).astype(jnp.bfloat16)
    first_half, second_half = lax.optimization_barrier((first_half, second_half))
    mixed_sum = first_half.astype(jnp.float32) + second_half.astype(jnp.float32)
    after_mix = (after_first.astype(jnp.float32) + mixed_sum).astype(jnp.bfloat16)
    mixed_out = feed_forward(after_mix, gain_second, second_gate, second_up, second_down)
    return (mixed_out, new_state)


F32 = jnp.float32
BF16 = jnp.bfloat16
MESH = pl.DeviceIdType.MESH
VMEM_LIMIT = 58 * 1024 * 1024


def fused_kernel(
    kv_size,
    channels,
    tokens_hbm,
    lengths_hbm,
    gains1_hbm,
    gains_mix_hbm,
    gains2_hbm,
    rates_hbm,
    state_hbm,
    gate1_hbm,
    up1_hbm,
    down1_hbm,
    query_hbm,
    key_hbm,
    value_hbm,
    gating_hbm,
    write_hbm,
    forget_hbm,
    out_hbm,
    gate2_hbm,
    up2_hbm,
    down2_hbm,
    packed_out,
    order_out,
    state_out,
    units1,
    down1,
    units2,
    down2,
    proj,
    out_w,
    small_w,
    state,
    state_high,
    state_low,
    gains1_ref,
    gains_mix_ref,
    gains2_ref,
    rates_ref,
    tokens_ref,
    length_ref,
    lens_all,
    picked,
    entered,
    unit_acc,
    live_acc,
    proj_acc,
    small_acc,
    middle,
    second_in,
    heads_send,
    heads_recv,
    red_send,
    red_recv,
    part_send,
    part_recv,
    small_recv,
    fin_send,
    fin_recv,
    own_send,
    own_recv,
    spread_cols,
    load_sems,
    send_sems,
    recv_sems,
):
    kv = lax.axis_index("kv")
    tp = lax.axis_index("tp")
    devices = 2 * kv_size
    me = kv * 2 + tp
    cls = lax.rem(kv + tp, 2)
    rows, cols = tokens_ref.shape
    wide = 2 * cols
    slots = BLK // 2
    half = rows // 2
    pack = rows // 4
    hidden_local = gate1_hbm.shape[1]
    own_cols = pl.ds(pl.multiple_of(tp * cols, cols), cols)
    inner = lax.rem((kv + 1) // 2, 2)
    near_first = [1, 2 + inner, 3 - inner]
    far_first = near_first[::-1]

    loads, load_at = {}, {}

    def load(name, *pairs, after=None):
        load_at[name] = load_at[after] if after else len(set(load_at.values()))
        sem = load_sems.at[load_at[name]]
        loads[name] = [pltpu.make_async_copy(src, dst, sem) for src, dst in pairs]

    def start(name):
        for copy in loads[name]:
            copy.start()

    def loaded(name, ref=None):
        if ref is None:
            loads[name][0].wait()
        else:
            sem = load_sems.at[load_at[name]]
            pltpu.make_async_copy(ref, ref, sem).wait()

    def swapped(off):
        chip, bit = 0, 1
        while bit < kv_size:
            chip = chip + bit * lax.rem(kv // bit + off // bit, 2)
            bit *= 2
        return chip

    def core_of(chip, other):
        return lax.rem(chip + cls + other, 2)

    def chip_rows(chip):
        return pl.ds(pl.multiple_of(chip * wide, wide), wide)

    def kind_cols(kind):
        return pl.ds(pl.multiple_of(kind * wide + tp * cols, cols), cols)

    load("length", (lengths_hbm, length_ref))
    load("tokens", (tokens_hbm, tokens_ref))
    load("gains1", (gains1_hbm, gains1_ref))
    for index, off in enumerate([0] + near_first):
        at = chip_rows(swapped(off))
        load(
            f"units1{index}",
            (gate1_hbm.at[at, :], units1.at[at, 0:hidden_local]),
            (up1_hbm.at[at, :], units1.at[at, hidden_local : 2 * hidden_local]),
        )
    early = list(loads)
    kinds = (query_hbm, key_hbm, value_hbm, gating_hbm)
    load("proj", *[(ref, proj.at[:, kind_cols(kind)]) for kind, ref in enumerate(kinds)])
    load("down1", (down1_hbm, down1))
    load(
        "small",
        (write_hbm, small_w.at[0:HEADS]),
        (forget_hbm, small_w.at[HEADS : 2 * HEADS]),
    )
    load("gains_mix", (gains_mix_hbm, gains_mix_ref), after="length")
    load("rates", (rates_hbm, rates_ref), after="tokens")
    load("out", (out_hbm, out_w.at[:, own_cols]))
    load("state", (state_hbm.at[0], state), after="units10")
    load("gains2", (gains2_hbm, gains2_ref), after="gains1")
    load(
        "units2",
        (gate2_hbm, units2.at[:, 0:hidden_local]),
        (up2_hbm, units2.at[:, hidden_local : 2 * hidden_local]),
        after="units11",
    )
    load("down2", (down2_hbm, down2), after="units12")
    last = ("state", "gains2", "units2", "down2")
    late = [name for name in loads if name not in early and name not in last]
    for name in early[:2]:
        start(name)
    barrier = pltpu.get_barrier_semaphore()
    here = 0
    for off in far_first + [here]:
        for core in (tp, 1 - tp) if off is not here else (1 - tp,):
            pl.semaphore_signal(
                barrier, inc=1, device_id={"kv": swapped(off), "tp": core}, device_id_type=MESH
            )
    for name in early[2:]:
        start(name)

    sends, receives, width = {}, {}, [0]
    send_after = {"heads": "tokens", "second": "lens", "fin": "red", "own": "out"}
    receive_after = {
        "heads": "tokens",
        "second": "tokens",
        "fin0": "red0",
        "fin1": "red1",
        "own0": "small",
        "own1": "proj",
    }

    def remote(name, src, dst, chip, core, at=0, spread=1):
        base = name.rstrip("01")
        if base not in sends:
            sends[base] = sends[send_after[base]] if base in send_after else len(set(sends.values()))
        if name not in receives:
            if name in receive_after:
                receives[name] = receives[receive_after[name]]
            else:
                receives[name] = width[0]
                width[0] += spread
        copy = pltpu.make_async_remote_copy(
            src_ref=src,
            dst_ref=dst,
            send_sem=send_sems.at[sends[name.rstrip("01")]],
            recv_sem=recv_sems.at[receives[name] + at],
            device_id={"kv": chip, "tp": core},
            device_id_type=MESH,
        )
        copy.start()

    def arrived(name, ref, at=0):
        sem = recv_sems.at[receives[name] + at]
        pltpu.make_async_remote_copy(
            src_ref=ref,
            dst_ref=ref,
            send_sem=sem,
            recv_sem=sem,
            device_id={"kv": kv, "tp": 1 - tp},
            device_id_type=MESH,
        ).wait_recv()

    def all_sent(name, ref):
        sem = send_sems.at[sends[name]]
        pltpu.make_async_remote_copy(
            src_ref=ref,
            dst_ref=ref,
            send_sem=sem,
            recv_sem=sem,
            device_id={"kv": kv, "tp": 1 - tp},
            device_id_type=MESH,
        ).wait_send()

    def to_class(name, src, dst, spread=1):
        for off in far_first:
            chip = swapped(off)
            remote(name, src(off), dst(off), chip, core_of(chip, 0), off if spread > 1 else 0, spread)

    def to_all(name, src, dst, spread=1):
        for off in far_first:
            chip = swapped(off)
            first = lax.rem(chip + cls, 2)
            for other in (first, 1 - first):
                core = core_of(chip, other)
                remote(
                    name, src(other, chip * 2 + core), dst(other), chip, core,
                    off if spread > 1 else 0, spread,
                )
        to_partner(name, src(1, kv * 2 + 1 - tp), dst(1))

    def to_partner(name, src, dst):
        remote(name, src, dst, kv, 1 - tp)

    def columns_of(hidden, down, chips):
        right = jnp.concatenate([down[:, chip_rows(chip)] for chip in chips], axis=1)
        both = jnp.dot(hidden, right, preferred_element_type=F32)
        return [both[:, at * wide : (at + 1) * wide] for at in range(len(chips))]

    pairs = [(far_first[0], far_first[1]), (far_first[2], 0)]

    def iota(shape, axis):
        return lax.broadcasted_iota(jnp.int32, shape, axis)

    def dot(a, b):
        return jnp.dot(a, b, preferred_element_type=F32)

    def one_hot(mask):
        return jnp.where(mask, 1.0, 0.0).astype(BF16)

    row = iota((rows, rows), 0)
    col = iota((rows, rows), 1)
    at_class = lax.rem(row, half)
    at_seq = at_class // slots
    which = lax.rem(cls + row // half + at_seq, 2)
    picks = one_hot(col == at_seq * BLK + 2 * lax.rem(at_class, slots) + which)
    with jax.named_scope("small_wait"):
        loaded("length")
        loaded("tokens")
    lens_all[me] = jnp.broadcast_to(length_ref[...], (1, HEAD))
    chosen = dot(picks, tokens_ref[...]).astype(BF16)
    picked[...] = chosen.reshape(2, half, cols)
    entered[me] = chosen[:half]
    with jax.named_scope("barrier"):
        pl.semaphore_wait(barrier, devices - 1)
    to_all("tokens", lambda other, peer: picked.at[other], lambda other: entered.at[me], kv_size)
    to_all("lens", lambda other, peer: lens_all.at[me], lambda other: lens_all.at[me])
    for name in late:
        start(name)
    small_w[2 * HEADS :] = jnp.zeros((HEAD - 2 * HEADS, channels), BF16)

    def ffn_slot(acc, units, gain_ref, chip, portion, index):
        at = chip_rows(chip)
        values = portion.astype(F32)
        scaled = (values * gain_ref[:, at]).astype(BF16)
        term = dot(scaled, units[at, :])
        if index == 0:
            acc[...] = term
        elif index < kv_size - 1:
            acc[...] += term
        else:
            term = acc[...] + term
        return jnp.sum(values * values, axis=1, keepdims=True), term

    def finish(acc, squares):
        row_scale = lax.rsqrt(squares / channels + EPSILON)
        gate = acc[:, 0:hidden_local] * row_scale
        up = acc[:, hidden_local : 2 * hidden_local] * row_scale
        return (jax.nn.silu(gate) * up).astype(BF16)

    def lengths_by(seq):
        found = jnp.zeros(seq.shape, jnp.int32)
        for index in range(devices):
            found = jnp.where(seq == index, lens_all[index], found)
        return found

    def is_live(seq, slot, klass):
        return 2 * slot + lax.rem(klass + seq, 2) < lengths_by(seq)

    def live_column(klass):
        at = iota((half, HEAD), 0)
        return jnp.where(is_live(at // slots, lax.rem(at, slots), klass), 1.0, 0.0)

    def live_row(klass):
        at = iota((1, HEAD), 1)
        live = is_live(at // slots, lax.rem(at, slots), klass) & (at < half)
        return jnp.where(live, 1.0, 0.0)

    def place_lanes(seq, slot, column):
        target = seq * slots + slot
        before = jnp.sum(
            jnp.where(iota((half, HEAD), 0) < target, column, 0.0), axis=0, keepdims=True
        )
        count = jnp.sum(column, axis=0, keepdims=True)
        rest = count + target.astype(F32) - before
        return jnp.where(is_live(seq, slot, cls), before, rest).astype(jnp.int32)

    def place_rows(seq, slot, klass, flags):
        target = seq * slots + slot
        before = jnp.sum(
            jnp.where(iota(seq.shape, 1) < target, flags, 0.0), axis=1, keepdims=True
        )
        count = jnp.sum(flags, axis=1, keepdims=True)
        rest = count + target.astype(F32) - before
        return jnp.where(is_live(seq, slot, klass), before, rest).astype(jnp.int32)

    def chip_tokens(chip):
        return jnp.concatenate([entered[chip * 2], entered[chip * 2 + 1]], axis=1)

    loaded("gains1")
    squares = jnp.zeros((half, 1), F32)
    for index, off in enumerate([0] + near_first):
        chip = swapped(off)
        with jax.named_scope(f"tokens_wait{index}"):
            if index:
                arrived("tokens", entered.at[pl.ds(chip * 2, 2)], off)
            else:
                arrived("tokens", entered.at[kv * 2 + 1 - tp], off)
            loaded(f"units1{index}", units1.at[chip_rows(chip), :])
            if index == kv_size - 1:
                arrived("lens", lens_all.at[pl.ds(0, devices - 1)])
        with jax.named_scope(f"units_slot{index}"):
            if index == kv_size - 1:
                column = live_column(cls)
                lane = iota((1, HEAD), 1)
                place = place_lanes(
                    jnp.minimum(lane // slots, devices - 1), lax.rem(lane, slots), column
                )
                reorder = one_hot(iota((half, HEAD), 0) == place)[:, :half]
            square, total = ffn_slot(
                unit_acc, units1, gains1_ref, chip, chip_tokens(chip), index
            )
            squares = squares + square
        if index == kv_size - 2:
            with jax.named_scope("exchange"):
                loaded("proj", proj.at[:, 0 : 4 * cols])
                for kind in range(4):
                    at = kind_cols(kind)
                    to_partner("proj", proj.at[:, at], proj.at[:, at])
    with jax.named_scope("finish0"):
        hidden = dot(reorder, finish(total, squares)).astype(BF16)
    with jax.named_scope("down_wait"):
        loaded("down1")
    with jax.named_scope("down0"):
        for pair in pairs:
            chips = [swapped(off) for off in pair]
            for off, chip, term in zip(pair, chips, columns_of(hidden, down1, chips)):
                if off is pairs[1][1]:
                    own_term = term
                    continue
                red_send[0, off] = term[:pack].astype(BF16)
                red_send[1, off] = term[pack:].astype(BF16)
                remote("red0", red_send.at[0, off], red_recv.at[0, off], chip, core_of(chip, 0))
    with jax.named_scope("exchange_out"):
        loaded("out")
        to_partner("out", out_w.at[:, own_cols], out_w.at[:, own_cols])
        for name in last:
            start(name)
    with jax.named_scope("tables"):
        residual = dot(reorder, chip_tokens(kv))
        flags = live_row(cls)
        other_flags = live_row(1 - cls)
        at = iota((rows, HEAD), 0)
        slot = lax.rem(at, slots)
        place = place_rows(at // BLK, slot, cls, flags)
        kind = lax.rem(at // slots + at // BLK + cls, 2)
        lane = iota((rows, HEAD), 1)
        spread = one_hot(
            (lane // pack == kind) & (lax.rem(lane, pack) == place) & (lane < 2 * pack)
        )[:, : 2 * pack]
        lane = iota((1, devices * 2 * BLK), 1)
        place = place_lanes(lane // (2 * BLK), lax.rem(lane, slots), column)
        at = iota((kv_size * pack, devices * 2 * BLK), 0)
        chip_at = lax.rem(iota((kv_size * pack, devices * 2 * BLK), 1) // slots, kv_size)
        gather_heads = one_hot((at // pack == chip_at) & (lax.rem(at, pack) == place))
        at = iota((BLK, HEAD), 0)
        klass = lax.rem(at // slots + me, 2)
        place = place_rows(
            jnp.zeros((BLK, HEAD), jnp.int32) + me,
            lax.rem(at, slots),
            klass,
            jnp.where(klass == cls, flags, other_flags),
        )
        lane = iota((BLK, HEAD), 1)
        pick_small = jnp.where(
            (lax.rem(lane // pack + cls, 2) == klass)
            & (lax.rem(lane, pack) == place)
            & (lane < 2 * pack),
            1.0,
            0.0,
        )[:, : 2 * pack]
        at = iota((rows, HEAD), 0)
        seq, token = at // BLK, lax.rem(at, BLK)
        klass = lax.rem(seq + token, 2)
        place = place_rows(seq, token // 2, klass, jnp.where(klass == cls, flags, other_flags))
        lane = iota((rows, HEAD), 1)
        order_out[...] = one_hot(
            (lax.rem(lane // half + cls, 2) == klass)
            & (lax.rem(lane, half) == place)
            & (lane < rows)
        )[:, :rows]
    for off in far_first:
        chip = swapped(off)
        remote("red1", red_send.at[1, off], red_recv.at[1, off], chip, core_of(chip, 0))

    def first_done(group):
        at = slice(group * pack, (group + 1) * pack)
        arrived(f"red{group}", red_recv.at[group, pl.ds(1, kv_size - 1)])
        total = own_term[at]
        for off in range(1, kv_size):
            total = total + red_recv[group, off].astype(F32)
        middle[group, kv] = (residual[at] + 0.5 * total).astype(BF16)
        to_class(
            f"middle{group}",
            lambda off: middle.at[group, kv],
            lambda off: middle.at[group, kv],
            1 if group else kv_size,
        )

    with jax.named_scope("red0"):
        first_done(0)
    with jax.named_scope("statecut"):
        loaded("state")
        for head in range(HEADS):
            high = state[head].astype(BF16)
            state_high[head] = high
            state_low[head] = (state[head] - high.astype(F32)).astype(BF16)
    with jax.named_scope("proj_wait"):
        arrived("proj", proj.at[:, 0 : 4 * cols])
        loaded("small", small_w.at[0 : 2 * HEADS])
        loaded("gains_mix")
        loaded("rates")
    squares = jnp.zeros((pack, 1), F32)
    for index, off in enumerate([0] + near_first):
        chip = swapped(off)
        at = chip_rows(chip)
        with jax.named_scope(f"middle_wait{index}"):
            if index:
                arrived("middle0", middle.at[0, chip], off)
        with jax.named_scope(f"proj_slot{index}"):
            values = middle[0, chip].astype(F32)
            squares = squares + jnp.sum(values * values, axis=1, keepdims=True)
            scaled = (values * gains_mix_ref[:, at]).astype(BF16)
            small_term = lax.dot_general(
                scaled, small_w[:, at], (((1,), (1,)), ((), ())), preferred_element_type=F32
            )
            if index == 0:
                proj_acc[...] = dot(scaled, proj[at, :])
                small_acc[0] = small_term
                with jax.named_scope("red1"):
                    first_done(1)
            elif index < kv_size - 1:
                proj_acc[...] += dot(scaled, proj[at, :])
                small_acc[0] += small_term
    with jax.named_scope("partsend"):
        mix_scale = lax.rsqrt(squares / channels + EPSILON)
        for pair in range(2):
            lanes = slice(pair * 2 * wide, (pair + 1) * 2 * wide)
            projected = proj_acc[:, lanes] + dot(scaled, proj[at, lanes])
            projected = (projected * mix_scale).astype(BF16)
            stacked = jnp.concatenate([projected[:, :wide], projected[:, wide:]], axis=0)
            part = dot(spread, stacked).astype(BF16)
            part_send[pair] = part.reshape(devices, BLK, wide)
            to_all(
                f"part{pair}",
                lambda other, peer: part_send.at[pair, peer],
                lambda other: part_recv.at[pair, kv, cls],
            )
            if pair == 0:
                small_acc[0] = (small_acc[0] + small_term) * mix_scale
                to_partner("small", small_acc.at[0], small_recv.at[0])
        for pair in range(2):
            part_recv[pair, kv, cls] = part_send[pair, me]

    def cut_terms(a):
        high = a.astype(BF16).astype(F32)
        return high, a - high

    def dot_fine(a, b, across=False):
        high_a, low_a = cut_terms(a)
        high_b, low_b = cut_terms(b)
        axis = 1 if across else 0
        left = jnp.concatenate([high_a, high_a, low_a], axis=1).astype(BF16)
        right = jnp.concatenate([high_b, low_b, high_b], axis=axis).astype(BF16)
        return lax.dot_general(
            left, right, (((1,), (axis,)), ((), ())), preferred_element_type=F32
        )

    with jax.named_scope("premix_a"):
        size = HEADS * BLK

        def token_of(at):
            at = lax.rem(at, BLK)
            return 2 * lax.rem(at, slots) + at // slots

        row = iota((size, size), 0)
        col = iota((size, size), 1)
        same = (row // BLK) == (col // BLK)
        causal = same & (token_of(row) >= token_of(col))
        strict = same & (token_of(row) > token_of(col))
        diagonal = row == col
        pick = iota((size, HEADS), 0) // BLK == iota((size, HEADS), 1)

        def as_column(block):
            return jnp.sum(jnp.where(pick, block, 0.0), axis=1, keepdims=True)

        def to_row(column):
            return jnp.sum(jnp.where(diagonal, column, 0.0), axis=0, keepdims=True)

    with jax.named_scope("dead_units"):
        all_sent("tokens", entered.at[pl.ds(0, devices - 1)])
        all_sent("lens", lens_all.at[pl.ds(0, devices - 1)])
        all_sent("red", red_send.at[:, pl.ds(1, kv_size - 1)])
        all_sent("out", out_w.at[:, own_cols])
        loaded("gains2")
        loaded("units2", units2)
        arrived("middle1", middle.at[1, pl.ds(0, kv_size - 1)])
        values = jnp.concatenate([middle[1, chip] for chip in range(kv_size)], axis=1).astype(F32)
        squares = jnp.sum(values * values, axis=1, keepdims=True)
        dead_hidden = finish(dot((values * gains2_ref[...]).astype(BF16), units2[...]), squares)

    with jax.named_scope("premix"):
        arrived("small", small_recv.at[0])
        small_all = jnp.concatenate([small_acc[0], small_recv[0]], axis=0)
        high, low = cut_terms(small_all)
        picked_small = dot(pick_small.astype(BF16), high.astype(BF16)) + dot(
            pick_small.astype(BF16), low.astype(BF16)
        )
        write_pre = picked_small[:, 0:HEADS]
        forget_pre = picked_small[:, HEADS : 2 * HEADS]

        live = jnp.where(token_of(iota((size, 1), 0)) < length_ref[...], 1.0, 0.0)
        write_col = as_column(jnp.concatenate([write_pre] * HEADS, axis=0))
        forget_col = as_column(jnp.concatenate([forget_pre] * HEADS, axis=0))
        rate_col = as_column(jnp.broadcast_to(rates_ref[...], (size, HEADS)))
        write_gate = jax.nn.sigmoid(write_col) * live
        softplus = jnp.maximum(forget_col, 0.0) + jnp.log1p(jnp.exp(-jnp.abs(forget_col)))
        forget = -jnp.exp(rate_col) * softplus * live
        forget_row = to_row(forget)
        cumulative = jnp.sum(jnp.where(causal, forget_row, 0.0), axis=1, keepdims=True)
        final = jnp.sum(jnp.where(same, forget_row, 0.0), axis=1, keepdims=True)
        decay = jnp.where(
            causal, jnp.exp(jnp.minimum(cumulative - to_row(cumulative), 0.0)), 0.0
        )
        growth = jnp.exp(cumulative)
        fading = jnp.exp(final - cumulative)
        shrink = jnp.exp(final)

    with jax.named_scope("partwait0"):
        arrived("part0", part_send.at[0, pl.ds(0, devices - 1)])
    scope = jax.named_scope("mix0")
    scope.__enter__()
    upper = iota((BLK, wide), 0) < slots

    def by_head(pair):
        ahead, behind = [], []
        for chip in range(kv_size):
            even = part_recv[pair, chip, lax.rem(me, 2)].astype(F32)
            odd = part_recv[pair, chip, lax.rem(me + 1, 2)].astype(F32)
            front = jnp.where(upper, even, odd)
            back = pltpu.roll(jnp.where(upper, odd, even), slots, 0)
            for start in range(0, wide, HEAD):
                ahead.append(front[:, start : start + HEAD])
                behind.append(back[:, start : start + HEAD])
        return jnp.concatenate(ahead, axis=0), jnp.concatenate(behind, axis=0)

    query, key_in = by_head(0)
    query_unit = (
        query
        * lax.rsqrt(jnp.sum(query * query, axis=1, keepdims=True) + EPSILON)
        * (1.0 / math.sqrt(HEAD))
    )
    key_unit = key_in * lax.rsqrt(jnp.sum(key_in * key_in, axis=1, keepdims=True) + EPSILON)
    products = dot_fine(jnp.concatenate([key_unit, query_unit], axis=0), key_unit, True)
    lower = jnp.where(strict, write_gate * decay * products[:size], 0.0)
    scores = products[size:] * decay
    key_grown = (write_gate * growth) * key_unit
    query_grown = query_unit * growth

    key_terms, query_terms = [], []
    for head in range(HEADS):
        at = slice(head * BLK, (head + 1) * BLK)
        high, low = cut_terms(jnp.concatenate([key_grown[at], query_grown[at]], axis=0))
        both = jnp.concatenate([high, low], axis=0).astype(BF16)
        result = dot(both, state_high[head])
        result = result[: 2 * BLK] + result[2 * BLK :]
        result = result + dot(both[: 2 * BLK], state_low[head])
        key_terms.append(result[:BLK])
        query_terms.append(result[BLK:])
    for head in range(HEADS):
        at = slice(head * BLK, (head + 1) * BLK)
        for token in range(BLK):
            place = head * BLK + slots * (token % 2) + token // 2
            spread_cols[1, head, token] = jnp.broadcast_to(scores[at, place : place + 1], (BLK, HEAD))
            if token < BLK - 1:
                spread_cols[0, head, token] = jnp.broadcast_to(
                    lower[at, place : place + 1], (BLK, HEAD)
                )
    scope.__exit__(None, None, None)
    with jax.named_scope("partwait1"):
        arrived("part1", part_send.at[1, pl.ds(0, devices - 1)])
    scope = jax.named_scope("mix1")
    scope.__enter__()
    value, gating = by_head(1)
    updates, attends = [], []
    for head in range(HEADS):
        at = slice(head * BLK, (head + 1) * BLK)
        solved = (write_gate * value)[at] - key_terms[head]
        attend = query_terms[head]
        for token in range(BLK):
            place = slots * (token % 2) + token // 2
            known = jnp.broadcast_to(solved[place : place + 1], (BLK, HEAD))
            attend = attend + spread_cols[1, head, token] * known
            if token < BLK - 1:
                solved = solved - spread_cols[0, head, token] * known
        updates.append(solved)
        attends.append(attend)
    update = jnp.concatenate(updates, axis=0)
    attend = jnp.concatenate(attends, axis=0)
    normed = attend * lax.rsqrt(jnp.mean(attend * attend, axis=1, keepdims=True) + EPSILON)
    normed = normed * jax.nn.silu(gating) * live

    per_chip = wide // HEAD

    def lanes_of(chip):
        first = chip * per_chip
        return jnp.concatenate(
            [normed[(first + at) * BLK : (first + at + 1) * BLK] for at in range(per_chip)], axis=1
        )

    fronts, backs = [], []
    for chip in range(0, kv_size, 2):
        even, odd = lanes_of(chip), lanes_of(chip + 1)
        fronts.append(jnp.where(upper, even, pltpu.roll(odd, slots, 0)))
        backs.append(jnp.where(upper, pltpu.roll(even, slots, 0), odd))
    heads_send[0] = jnp.concatenate(fronts, axis=0).astype(BF16)
    heads_send[1] = jnp.concatenate(backs, axis=0).astype(BF16)
    to_all(
        "heads",
        lambda other, peer: heads_send.at[lax.rem(cls + other + me, 2)],
        lambda other: heads_recv.at[me],
    )
    heads_recv[me] = heads_send[lax.rem(cls + me, 2)]
    scope.__exit__(None, None, None)

    with jax.named_scope("newstate"):
        faded = key_unit * fading
        for head in range(HEADS):
            at = slice(head * BLK, (head + 1) * BLK)
            key_high, key_low = cut_terms(faded[at])
            value_high, value_low = cut_terms(update[at])
            outer = lax.dot_general(
                jnp.concatenate([key_high, key_high, key_low], axis=0).astype(BF16),
                jnp.concatenate([value_high, value_low, value_high], axis=0).astype(BF16),
                (((0,), (0,)), ((), ())),
                preferred_element_type=F32,
            )
            state_out[0, head] = shrink[head * BLK : head * BLK + 1] * state[head] + outer

    def hand_off(group, off):
        chip = swapped(off)
        for other in (0, 1):
            core = core_of(chip, other)
            remote(
                f"fin{group}", fin_send.at[group, off, core],
                fin_recv.at[group, off, other], chip, core,
            )

    def hand_own(group):
        to_partner(f"own{group}", own_send.at[group, 1 - tp], own_recv.at[group])

    def second_down(group, hidden, source, at_once):
        for pair in pairs:
            chips = [swapped(off) for off in pair]
            for off, chip, term in zip(pair, chips, columns_of(hidden, down2, chips)):
                if off is pairs[1][1]:
                    term = source.astype(F32) + 0.5 * term
                    own_send[group, 0] = term[:, :cols]
                    own_send[group, 1] = term[:, cols:]
                    continue
                fin_send[group, off, 0] = term[:, :cols].astype(BF16)
                fin_send[group, off, 1] = term[:, cols:].astype(BF16)
                if at_once:
                    hand_off(group, off)
        if at_once:
            hand_own(group)

    def take_in(group):
        arrived(f"own{group}", own_recv.at[group])
        arrived(f"fin{group}", fin_recv.at[group, pl.ds(1, kv_size - 1)])
        sums = [own_send[group, tp], own_recv[group]]
        for other in (0, 1):
            total = fin_recv[group, 1, other].astype(F32)
            for off in range(2, kv_size):
                total = total + fin_recv[group, off, other].astype(F32)
            sums[other] = sums[other] + 0.5 * total
        return [total.astype(BF16) for total in sums]

    with jax.named_scope("dead_down"):
        loaded("down2")
        second_down(1, dead_hidden, middle[1, kv], False)
    with jax.named_scope("gather2"):
        arrived("heads", heads_recv.at[pl.ds(0, devices - 1)])
        arrived("out", out_w.at[:, own_cols])
    with jax.named_scope("outproj"):
        blocks = heads_recv[...].reshape(devices * 2 * BLK, wide)
        mixed = dot(gather_heads, blocks).astype(BF16)
        terms = []
        for part in range(2):
            chips = range(part * kv_size // 2, (part + 1) * kv_size // 2)
            left = jnp.concatenate([mixed[chip * pack : (chip + 1) * pack] for chip in chips], axis=1)
            right = out_w[chips[0] * wide : (chips[-1] + 1) * wide, :]
            terms.append(dot(left, right).astype(BF16).astype(F32))
        second_in[kv] = (middle[0, kv].astype(F32) + (terms[0] + terms[1])).astype(BF16)
        to_class("second", lambda off: second_in.at[kv], lambda off: second_in.at[kv], kv_size)

    squares = jnp.zeros((pack, 1), F32)
    for index, off in enumerate([0] + near_first):
        chip = swapped(off)
        with jax.named_scope(f"second_wait{index}"):
            if index:
                arrived("second", second_in.at[chip], off)
        with jax.named_scope(f"live_slot{index}"):
            square, total = ffn_slot(
                live_acc, units2, gains2_ref, chip, second_in[chip], index
            )
            squares = squares + square
        if index == 1:
            with jax.named_scope("dead_off"):
                for off in far_first:
                    hand_off(1, off)
                hand_own(1)
    with jax.named_scope("finish1"):
        hidden = finish(total, squares)
    with jax.named_scope("down1"):
        second_down(0, hidden, second_in[kv], True)
    with jax.named_scope("dead_in"):
        dead_sums = take_in(1)
    with jax.named_scope("live_in"):
        live_sums = take_in(0)
    with jax.named_scope("last"):
        packed_out[...] = jnp.concatenate(
            [live_sums[0], dead_sums[0], live_sums[1], dead_sums[1]], axis=0
        )
    with jax.named_scope("tail"):
        all_sent("proj", proj.at[:, 0 : 4 * cols])
        all_sent("small", small_acc.at[0])
        all_sent("heads", heads_recv.at[pl.ds(0, devices - 1)])
        all_sent("second", second_in.at[pl.ds(0, kv_size - 1)])
        all_sent("middle", middle.at[:, pl.ds(0, kv_size - 1)])
        all_sent("part", part_send.at[:, pl.ds(0, devices - 1)])
        all_sent("fin", fin_send.at[:, pl.ds(1, kv_size - 1)])
        all_sent("own", own_send.at[0])


def fused_call(mesh, *args):
    (
        tokens, lengths, state, gain_first, first_gate, first_up, first_down, gain_mix,
        query_weight, key_weight, value_weight, gating_weight, write_weight, forget_weight,
        forget_rate, out_weight, gain_second, second_gate, second_up, second_down,
    ) = args
    kv_size = mesh.shape["kv"]
    devices = kv_size * mesh.shape["tp"]
    rows, cols = tokens.shape
    wide = 2 * cols
    channels = gain_first.shape[0]
    hidden_local = first_gate.shape[1]
    half, pack = rows // 2, rows // 4
    in_hbm = pl.BlockSpec(memory_space=pltpu.HBM)
    in_vmem = pl.BlockSpec(memory_space=pltpu.VMEM)
    dma = pltpu.SemaphoreType.DMA
    operands = (
        tokens, lengths.reshape(1, 1), gain_first.reshape(1, -1), gain_mix.reshape(1, -1),
        gain_second.reshape(1, -1), forget_rate.reshape(1, -1), state,
        first_gate, first_up, first_down, query_weight, key_weight, value_weight,
        gating_weight, write_weight.T, forget_weight.T, out_weight, second_gate, second_up,
        second_down,
    )
    operands = [
        array if array.dtype == jnp.int32 else pltpu.with_memory_space_constraint(array, pltpu.HBM)
        for array in operands
    ]
    results = pl.pallas_call(
        functools.partial(fused_kernel, kv_size, channels),
        out_shape=(
            pltpu.VMEM(tokens.shape, tokens.dtype),
            pltpu.VMEM((rows, rows), BF16),
            pltpu.VMEM(state.shape, state.dtype),
        ),
        in_specs=[in_hbm] * len(operands),
        out_specs=(in_vmem, in_vmem, in_vmem),
        scratch_shapes=[
            pltpu.VMEM((channels, 2 * hidden_local), BF16),
            pltpu.VMEM((hidden_local, channels), BF16),
            pltpu.VMEM((channels, 2 * hidden_local), BF16),
            pltpu.VMEM((hidden_local, channels), BF16),
            pltpu.VMEM((channels, 4 * wide), BF16),
            pltpu.VMEM((channels, wide), BF16),
            pltpu.VMEM((HEAD, channels), BF16),
            pltpu.VMEM(state.shape[1:], F32),
            pltpu.VMEM(state.shape[1:], BF16),
            pltpu.VMEM(state.shape[1:], BF16),
            pltpu.VMEM((1, channels), F32),
            pltpu.VMEM((1, channels), F32),
            pltpu.VMEM((1, channels), F32),
            pltpu.VMEM((1, HEADS), F32),
            pltpu.VMEM((rows, cols), BF16),
            pltpu.VMEM((1, 1), jnp.int32),
            pltpu.VMEM((devices, 1, HEAD), jnp.int32),
            pltpu.VMEM((2, half, cols), BF16),
            pltpu.VMEM((devices, half, cols), BF16),
            pltpu.VMEM((half, 2 * hidden_local), F32),
            pltpu.VMEM((pack, 2 * hidden_local), F32),
            pltpu.VMEM((pack, 4 * wide), F32),
            pltpu.VMEM((1, pack, HEAD), F32),
            pltpu.VMEM((2, kv_size, pack, wide), BF16),
            pltpu.VMEM((kv_size, pack, wide), BF16),
            pltpu.VMEM((2, 2 * BLK, wide), BF16),
            pltpu.VMEM((devices, 2 * BLK, wide), BF16),
            pltpu.VMEM((2, kv_size, pack, wide), BF16),
            pltpu.VMEM((2, kv_size, pack, wide), BF16),
            pltpu.VMEM((2, devices, BLK, wide), BF16),
            pltpu.VMEM((2, kv_size, 2, BLK, wide), BF16),
            pltpu.VMEM((1, pack, HEAD), F32),
            pltpu.VMEM((2, kv_size, 2, pack, cols), BF16),
            pltpu.VMEM((2, kv_size, 2, pack, cols), BF16),
            pltpu.VMEM((2, 2, pack, cols), F32),
            pltpu.VMEM((2, pack, cols), F32),
            pltpu.VMEM((2, HEADS, BLK, BLK, HEAD), F32),
            dma((kv_size + 7,)),
            dma((8,)),
            dma((2 * kv_size + 9,)),
        ],
        compiler_params=pltpu.CompilerParams(
            collective_id=0, has_side_effects=True, vmem_limit_bytes=VMEM_LIMIT
        ),
    )(*operands)
    return hand_out(*results)


def hand_out_kernel(packed, order, state, mixed_hbm, state_hbm, mixed, sems):
    puts = [pltpu.make_async_copy(state, state_hbm, sems.at[0])]
    puts[0].start()
    restored = jnp.dot(order[...], packed[...], preferred_element_type=F32)
    mixed[...] = restored.astype(BF16)
    puts.append(pltpu.make_async_copy(mixed, mixed_hbm, sems.at[1]))
    puts[-1].start()
    for put in puts:
        put.wait()


def hand_out(packed, order, new_state):
    in_hbm = pl.BlockSpec(memory_space=pltpu.HBM)
    in_vmem = pl.BlockSpec(memory_space=pltpu.VMEM)
    arrays = [
        pltpu.with_memory_space_constraint(array, pltpu.VMEM)
        for array in (packed, order, new_state)
    ]
    return pl.pallas_call(
        hand_out_kernel,
        out_shape=(
            jax.ShapeDtypeStruct(packed.shape, packed.dtype),
            jax.ShapeDtypeStruct(new_state.shape, new_state.dtype),
        ),
        in_specs=[in_vmem] * 3,
        out_specs=(in_hbm, in_hbm),
        scratch_shapes=[
            pltpu.VMEM(packed.shape, packed.dtype),
            pltpu.SemaphoreType.DMA((2,)),
        ],
        compiler_params=pltpu.CompilerParams(vmem_limit_bytes=8 * 1024 * 1024),
    )(*arrays)


def fits_fused(mesh, args):
    tokens, lengths, state, first_gate = args[0], args[1], args[2], args[4]
    rows, cols = tokens.shape
    kv_size = mesh.shape["kv"]
    devices = kv_size * mesh.shape["tp"]
    return (
        mesh.shape["tp"] == 2
        and mesh.shape["kv"] & (mesh.shape["kv"] - 1) == 0
        and lengths.shape[0] == 1
        and rows == devices * BLK
        and devices * 2 * BLK == HEAD
        and kv_size * BLK // 2 == 2 * BLK
        and devices * cols == HEADS * HEAD
        and cols % 256 == 0
        and first_gate.shape[1] % 128 == 0
        and state.shape[1:] == (HEADS, HEAD, HEAD)
    )


def solution(mesh):
    in_specs = (
        P("dp", ("kv", "tp")),
        P(("dp", "kv", "tp")),
        P(("dp", "kv", "tp"), None, None, None),
        P(),
        P(None, "kv"),
        P(None, "kv"),
        P("kv", None),
        P(),
        P(None, ("kv", "tp")),
        P(None, ("kv", "tp")),
        P(None, ("kv", "tp")),
        P(None, ("kv", "tp")),
        P(),
        P(),
        P(),
        P(None, ("kv", "tp")),
        P(),
        P(None, "kv"),
        P(None, "kv"),
        P("kv", None),
    )
    out_specs = (P("dp", ("kv", "tp")), P(("dp", "kv", "tp"), None, None, None))

    def body(*args):
        if fits_fused(mesh, args):
            return fused_call(mesh, *args)
        return per_device(*args)

    return jax.shard_map(
        body, mesh=mesh, in_specs=in_specs, out_specs=out_specs, check_vma=False
    )
```

```python
import functools
import math

import jax
import jax.numpy as jnp
from jax import lax
from jax.experimental import pallas as pl
from jax.experimental.pallas import tpu as pltpu
from jax.sharding import PartitionSpec as P

HEADS = 16
HEAD = 128
BLK = 8


EPSILON = 1e-06


def fold_step(gain, gate_cols, up_cols, portion):
    values = portion.astype(jnp.float32)
    scaled = (values * gain).astype(jnp.bfloat16)
    gate_acc = jnp.dot(scaled, gate_cols, preferred_element_type=jnp.float32)
    up_acc = jnp.dot(scaled, up_cols, preferred_element_type=jnp.float32)
    squares = jnp.sum(values * values, axis=1)
    return (gate_acc, up_acc, squares)


def finish_units(gate_acc, up_acc, squares, channels, down_rows):
    row_scale = lax.rsqrt(squares / channels + EPSILON)[:, None]
    hidden = (jax.nn.silu(gate_acc * row_scale) * (up_acc * row_scale)).astype(jnp.bfloat16)
    return jnp.dot(hidden, down_rows, preferred_element_type=jnp.float32)


def feed_forward(hidden_in, gain, w_gate, w_up, w_down):
    channels = gain.shape[0]
    paired = lax.all_to_all(hidden_in, "tp", split_axis=0, concat_axis=1, tiled=True)
    gate_acc, up_acc, squares = fold_step(
        gain, w_gate, w_up, lax.all_gather(paired, "kv", axis=1, tiled=True)
    )
    ffn_term = finish_units(gate_acc, up_acc, squares, channels, w_down)
    partial_value = lax.psum_scatter(ffn_term, "kv", scatter_dimension=1, tiled=True)
    summed = lax.all_to_all(partial_value, "tp", split_axis=1, concat_axis=0, tiled=True)
    return (hidden_in.astype(jnp.float32) + 0.5 * summed).astype(jnp.bfloat16)


def delta_block(query, key_in, value, gating, write_pre, forget_pre, rates, live, state):
    seq_count, block_len, head_count, head_size = query.shape
    precise = lax.Precision.HIGHEST
    query_unit = (
        query
        * lax.rsqrt(jnp.sum(query * query, axis=-1, keepdims=True) + EPSILON)
        / math.sqrt(head_size)
    )
    key_unit = key_in * lax.rsqrt(jnp.sum(key_in * key_in, axis=-1, keepdims=True) + EPSILON)
    live_rows = live[:, :, None]
    write_gate = jax.nn.sigmoid(write_pre) * live_rows
    forget = -jnp.exp(rates)[None, None, :] * jax.nn.softplus(forget_pre) * live_rows
    cumulative = jnp.cumsum(forget, axis=1)
    cum_heads = jnp.transpose(cumulative, (0, 2, 1))
    positions = jnp.arange(block_len)
    causal = positions[:, None] >= positions[None, :]
    strict = positions[:, None] > positions[None, :]
    differ = jnp.minimum(cum_heads[:, :, :, None] - cum_heads[:, :, None, :], 0.0)
    decay_mat = jnp.where(causal, jnp.exp(differ), 0.0)
    key_dots = jnp.einsum("sthd,suhd->shtu", key_unit, key_unit, precision=precise)
    write_heads = jnp.transpose(write_gate, (0, 2, 1))
    strict_part = jnp.where(strict, write_heads[:, :, :, None] * decay_mat * key_dots, 0.0)
    identity = jnp.eye(block_len, dtype=jnp.float32)
    squared = jnp.einsum("shtu,shuv->shtv", strict_part, strict_part, precision=precise)
    fourth = jnp.einsum("shtu,shuv->shtv", squared, squared, precision=precise)
    inverse = jnp.einsum(
        "shtu,shuv->shtv", identity - strict_part, identity + squared, precision=precise
    )
    inverse = jnp.einsum("shtu,shuv->shtv", inverse, identity + fourth, precision=precise)
    growth = jnp.exp(cumulative)
    target = jnp.einsum(
        "shtu,suhv->sthv", inverse, write_gate[..., None] * value, precision=precise
    )
    key_mix = jnp.einsum(
        "shtu,suhk->sthk", inverse, (write_gate * growth)[..., None] * key_unit, precision=precise
    )
    update = target - jnp.einsum("sthk,shkv->sthv", key_mix, state, precision=precise)
    scores = jnp.einsum("sthd,suhd->shtu", query_unit, key_unit, precision=precise) * decay_mat
    attend = jnp.einsum("sthk,shkv->sthv", query_unit * growth[..., None], state, precision=precise)
    attend = attend + jnp.einsum("shtu,suhv->sthv", scores, update, precision=precise)
    final_cum = cumulative[:, -1:, :]
    fading = jnp.exp(final_cum - cumulative)
    new_state = jnp.exp(final_cum[:, 0, :])[:, :, None, None] * state
    new_state = new_state + jnp.einsum(
        "sthk,sthv->shkv", key_unit * fading[..., None], update, precision=precise
    )
    normed = attend * lax.rsqrt(jnp.mean(attend * attend, axis=-1, keepdims=True) + EPSILON)
    normed = normed * jax.nn.silu(gating) * live[:, :, None, None]
    mixed_heads = normed.reshape(seq_count * block_len, head_count * head_size).astype(jnp.bfloat16)
    return (mixed_heads, new_state)


def per_device(
    tokens,
    lengths,
    state,
    gain_first,
    first_gate,
    first_up,
    first_down,
    gain_mix,
    query_weight,
    key_weight,
    value_weight,
    gating_weight,
    write_weight,
    forget_weight,
    forget_rate,
    out_weight,
    gain_second,
    second_gate,
    second_up,
    second_down,
):
    after_first = feed_forward(tokens, gain_first, first_gate, first_up, first_down)
    seq_count = lengths.shape[0]
    own_count = seq_count * BLK
    whole_rows = lax.all_gather(after_first, ("kv", "tp"), axis=1, tiled=True)
    scaled_all = (whole_rows.astype(jnp.float32) * gain_mix).astype(jnp.bfloat16)
    stacked = jnp.stack(
        [
            jnp.dot(scaled_all, matrix, preferred_element_type=jnp.float32)
            for matrix in (query_weight, key_weight, value_weight, gating_weight)
        ]
    )
    owned = lax.all_to_all(
        stacked.astype(jnp.bfloat16), ("kv", "tp"), split_axis=1, concat_axis=2, tiled=True
    ).astype(stacked.dtype)
    row_start = lax.axis_index(("kv", "tp")) * own_count
    own_values = lax.dynamic_slice_in_dim(whole_rows, row_start, own_count, 0).astype(jnp.float32)
    own_scaled = lax.dynamic_slice_in_dim(scaled_all, row_start, own_count, 0)
    mix_scale = lax.rsqrt(jnp.mean(own_values * own_values, axis=1, keepdims=True) + EPSILON)
    query = (owned[0] * mix_scale).reshape(seq_count, BLK, HEADS, HEAD)
    key_in = (owned[1] * mix_scale).reshape(seq_count, BLK, HEADS, HEAD)
    value = (owned[2] * mix_scale).reshape(seq_count, BLK, HEADS, HEAD)
    gating = (owned[3] * mix_scale).reshape(seq_count, BLK, HEADS, HEAD)
    write_pre = (
        jnp.dot(own_scaled, write_weight, preferred_element_type=jnp.float32) * mix_scale
    ).reshape(seq_count, BLK, HEADS)
    forget_pre = (
        jnp.dot(own_scaled, forget_weight, preferred_element_type=jnp.float32) * mix_scale
    ).reshape(seq_count, BLK, HEADS)
    positions = jnp.arange(BLK, dtype=jnp.int32)
    live = (positions[None, :] < lengths[:, None]).astype(jnp.float32)
    mixed_heads, new_state = delta_block(
        query, key_in, value, gating, write_pre, forget_pre, forget_rate, live, state
    )
    half_cols = mixed_heads.shape[1] // 2
    portion = lax.all_gather(mixed_heads, ("kv", "tp"), axis=0, tiled=True)
    first_half = jnp.dot(
        portion[:, :half_cols], out_weight[:half_cols], preferred_element_type=jnp.float32
    ).astype(jnp.bfloat16)
    second_half = jnp.dot(
        portion[:, half_cols:], out_weight[half_cols:], preferred_element_type=jnp.float32
    ).astype(jnp.bfloat16)
    first_half, second_half = lax.optimization_barrier((first_half, second_half))
    mixed_sum = first_half.astype(jnp.float32) + second_half.astype(jnp.float32)
    after_mix = (after_first.astype(jnp.float32) + mixed_sum).astype(jnp.bfloat16)
    mixed_out = feed_forward(after_mix, gain_second, second_gate, second_up, second_down)
    return (mixed_out, new_state)


F32 = jnp.float32
BF16 = jnp.bfloat16
MESH = pl.DeviceIdType.MESH
VMEM_LIMIT = 58 * 1024 * 1024


def fused_kernel(
    kv_size,
    channels,
    tokens_hbm,
    lengths_hbm,
    gains1_hbm,
    gains_mix_hbm,
    gains2_hbm,
    rates_hbm,
    state_hbm,
    gate1_hbm,
    up1_hbm,
    down1_hbm,
    query_hbm,
    key_hbm,
    value_hbm,
    gating_hbm,
    write_hbm,
    forget_hbm,
    out_hbm,
    gate2_hbm,
    up2_hbm,
    down2_hbm,
    packed_out,
    order_out,
    state_out,
    units1,
    down1,
    units2,
    down2,
    proj,
    out_w,
    small_w,
    state,
    state_high,
    state_low,
    gains1_ref,
    gains_mix_ref,
    gains2_ref,
    rates_ref,
    tokens_ref,
    length_ref,
    lens_all,
    picked,
    entered,
    unit_acc,
    live_acc,
    proj_acc,
    small_acc,
    middle,
    second_in,
    heads_send,
    heads_recv,
    red_send,
    red_recv,
    part_send,
    part_recv,
    small_recv,
    fin_send,
    fin_recv,
    own_send,
    own_recv,
    spread_cols,
    load_sems,
    send_sems,
    recv_sems,
):
    kv = lax.axis_index("kv")
    tp = lax.axis_index("tp")
    devices = 2 * kv_size
    me = kv * 2 + tp
    cls = lax.rem(kv + tp, 2)
    rows, cols = tokens_ref.shape
    wide = 2 * cols
    slots = BLK // 2
    half = rows // 2
    pack = rows // 4
    hidden_local = gate1_hbm.shape[1]
    own_cols = pl.ds(pl.multiple_of(tp * cols, cols), cols)
    inner = lax.rem((kv + 1) // 2, 2)
    near_first = [1, 2 + inner, 3 - inner]
    far_first = near_first[::-1]

    loads, load_at = {}, {}

    def load(name, *pairs, after=None):
        load_at[name] = load_at[after] if after else len(set(load_at.values()))
        sem = load_sems.at[load_at[name]]
        loads[name] = [pltpu.make_async_copy(src, dst, sem) for src, dst in pairs]

    def start(name):
        for copy in loads[name]:
            copy.start()

    def loaded(name, ref=None):
        if ref is None:
            loads[name][0].wait()
        else:
            sem = load_sems.at[load_at[name]]
            pltpu.make_async_copy(ref, ref, sem).wait()

    def swapped(off):
        chip, bit = 0, 1
        while bit < kv_size:
            chip = chip + bit * lax.rem(kv // bit + off // bit, 2)
            bit *= 2
        return chip

    def core_of(chip, other):
        return lax.rem(chip + cls + other, 2)

    def chip_rows(chip):
        return pl.ds(pl.multiple_of(chip * wide, wide), wide)

    def kind_cols(kind):
        return pl.ds(pl.multiple_of(kind * wide + tp * cols, cols), cols)

    load("length", (lengths_hbm, length_ref))
    load("tokens", (tokens_hbm, tokens_ref))
    load("gains1", (gains1_hbm, gains1_ref))
    for index, off in enumerate([0] + near_first):
        at = chip_rows(swapped(off))
        load(
            f"units1{index}",
            (gate1_hbm.at[at, :], units1.at[at, 0:hidden_local]),
            (up1_hbm.at[at, :], units1.at[at, hidden_local : 2 * hidden_local]),
        )
    early = list(loads)
    kinds = (query_hbm, key_hbm, value_hbm, gating_hbm)
    load("proj", *[(ref, proj.at[:, kind_cols(kind)]) for kind, ref in enumerate(kinds)])
    load("down1", (down1_hbm, down1))
    load(
        "small",
        (write_hbm, small_w.at[0:HEADS]),
        (forget_hbm, small_w.at[HEADS : 2 * HEADS]),
    )
    load("gains_mix", (gains_mix_hbm, gains_mix_ref), after="length")
    load("rates", (rates_hbm, rates_ref), after="tokens")
    load("out", (out_hbm, out_w.at[:, own_cols]))
    load("state", (state_hbm.at[0], state), after="units10")
    load("gains2", (gains2_hbm, gains2_ref), after="gains1")
    load(
        "units2",
        (gate2_hbm, units2.at[:, 0:hidden_local]),
        (up2_hbm, units2.at[:, hidden_local : 2 * hidden_local]),
        after="units11",
    )
    load("down2", (down2_hbm, down2), after="units12")
    last = ("state", "gains2", "units2", "down2")
    late = [name for name in loads if name not in early and name not in last]
    for name in early[:2]:
        start(name)
    barrier = pltpu.get_barrier_semaphore()
    here = 0
    for off in far_first + [here]:
        for core in (tp, 1 - tp) if off is not here else (1 - tp,):
            pl.semaphore_signal(
                barrier, inc=1, device_id={"kv": swapped(off), "tp": core}, device_id_type=MESH
            )
    for name in early[2:]:
        start(name)

    sends, receives, width = {}, {}, [0]
    send_after = {"heads": "tokens", "second": "lens", "fin": "red", "own": "out"}
    receive_after = {
        "heads0": "tokens",
        "heads1": "lens",
        "second": "tokens",
        "fin0": "red0",
        "fin1": "red1",
        "own0": "small",
        "own1": "proj",
    }

    def remote(name, src, dst, chip, core, at=0, spread=1):
        base = name.rstrip("01")
        if base not in sends:
            sends[base] = sends[send_after[base]] if base in send_after else len(set(sends.values()))
        if name not in receives:
            if name in receive_after:
                receives[name] = receives[receive_after[name]]
            else:
                receives[name] = width[0]
                width[0] += spread
        copy = pltpu.make_async_remote_copy(
            src_ref=src,
            dst_ref=dst,
            send_sem=send_sems.at[sends[name.rstrip("01")]],
            recv_sem=recv_sems.at[receives[name] + at],
            device_id={"kv": chip, "tp": core},
            device_id_type=MESH,
        )
        copy.start()

    def arrived(name, ref, at=0):
        sem = recv_sems.at[receives[name] + at]
        pltpu.make_async_remote_copy(
            src_ref=ref,
            dst_ref=ref,
            send_sem=sem,
            recv_sem=sem,
            device_id={"kv": kv, "tp": 1 - tp},
            device_id_type=MESH,
        ).wait_recv()

    def all_sent(name, ref):
        sem = send_sems.at[sends[name]]
        pltpu.make_async_remote_copy(
            src_ref=ref,
            dst_ref=ref,
            send_sem=sem,
            recv_sem=sem,
            device_id={"kv": kv, "tp": 1 - tp},
            device_id_type=MESH,
        ).wait_send()

    def to_class(name, src, dst, spread=1):
        for off in far_first:
            chip = swapped(off)
            remote(name, src(off), dst(off), chip, core_of(chip, 0), off if spread > 1 else 0, spread)

    def to_all(name, src, dst, spread=1, near="", far="", order=far_first):
        for off in order:
            chip = swapped(off)
            first = lax.rem(chip + cls, 2)
            for other in (first, 1 - first):
                core = core_of(chip, other)
                remote(
                    name + (near if off is far_first[2] else far),
                    src(other, chip * 2 + core), dst(other), chip, core,
                    off if spread > 1 else 0, spread,
                )
        to_partner(name + near, src(1, kv * 2 + 1 - tp), dst(1))

    def to_partner(name, src, dst):
        remote(name, src, dst, kv, 1 - tp)

    def columns_of(hidden, down, chips):
        right = jnp.concatenate([down[:, chip_rows(chip)] for chip in chips], axis=1)
        both = jnp.dot(hidden, right, preferred_element_type=F32)
        return [both[:, at * wide : (at + 1) * wide] for at in range(len(chips))]

    pairs = [(far_first[0], far_first[1]), (far_first[2], 0)]

    def iota(shape, axis):
        return lax.broadcasted_iota(jnp.int32, shape, axis)

    def dot(a, b):
        return jnp.dot(a, b, preferred_element_type=F32)

    def one_hot(mask):
        return jnp.where(mask, 1.0, 0.0).astype(BF16)

    row = iota((rows, rows), 0)
    col = iota((rows, rows), 1)
    at_class = lax.rem(row, half)
    at_seq = at_class // slots
    which = lax.rem(cls + row // half + at_seq, 2)
    picks = one_hot(col == at_seq * BLK + 2 * lax.rem(at_class, slots) + which)
    loaded("length")
    loaded("tokens")
    lens_all[me] = jnp.broadcast_to(length_ref[...], (1, HEAD))
    chosen = dot(picks, tokens_ref[...]).astype(BF16)
    picked[...] = chosen.reshape(2, half, cols)
    entered[me] = chosen[:half]
    pl.semaphore_wait(barrier, devices - 1)
    to_all("tokens", lambda other, peer: picked.at[other], lambda other: entered.at[me], kv_size)
    to_all("lens", lambda other, peer: lens_all.at[me], lambda other: lens_all.at[me])
    for name in late:
        start(name)
    small_w[2 * HEADS :] = jnp.zeros((HEAD - 2 * HEADS, channels), BF16)

    def ffn_slot(acc, units, gain_ref, chip, portion, index):
        at = chip_rows(chip)
        values = portion.astype(F32)
        scaled = (values * gain_ref[:, at]).astype(BF16)
        term = dot(scaled, units[at, :])
        if index == 0:
            acc[...] = term
        elif index < kv_size - 1:
            acc[...] += term
        else:
            term = acc[...] + term
        return jnp.sum(values * values, axis=1, keepdims=True), term

    def finish(acc, squares):
        row_scale = lax.rsqrt(squares / channels + EPSILON)
        gate = acc[:, 0:hidden_local] * row_scale
        up = acc[:, hidden_local : 2 * hidden_local] * row_scale
        return (jax.nn.silu(gate) * up).astype(BF16)

    def lengths_by(seq):
        found = jnp.zeros(seq.shape, jnp.int32)
        for index in range(devices):
            found = jnp.where(seq == index, lens_all[index], found)
        return found

    def is_live(seq, slot, klass):
        return 2 * slot + lax.rem(klass + seq, 2) < lengths_by(seq)

    def live_column(klass):
        at = iota((half, HEAD), 0)
        return jnp.where(is_live(at // slots, lax.rem(at, slots), klass), 1.0, 0.0)

    def live_row(klass):
        at = iota((1, HEAD), 1)
        live = is_live(at // slots, lax.rem(at, slots), klass) & (at < half)
        return jnp.where(live, 1.0, 0.0)

    def place_lanes(seq, slot, column):
        target = seq * slots + slot
        before = jnp.sum(
            jnp.where(iota((half, HEAD), 0) < target, column, 0.0), axis=0, keepdims=True
        )
        count = jnp.sum(column, axis=0, keepdims=True)
        rest = count + target.astype(F32) - before
        return jnp.where(is_live(seq, slot, cls), before, rest).astype(jnp.int32)

    def place_rows(seq, slot, klass, flags):
        target = seq * slots + slot
        before = jnp.sum(
            jnp.where(iota(seq.shape, 1) < target, flags, 0.0), axis=1, keepdims=True
        )
        count = jnp.sum(flags, axis=1, keepdims=True)
        rest = count + target.astype(F32) - before
        return jnp.where(is_live(seq, slot, klass), before, rest).astype(jnp.int32)

    def chip_tokens(chip):
        return jnp.concatenate([entered[chip * 2], entered[chip * 2 + 1]], axis=1)

    loaded("gains1")
    squares = jnp.zeros((half, 1), F32)
    for index, off in enumerate([0] + near_first):
        chip = swapped(off)
        if index:
            arrived("tokens", entered.at[pl.ds(chip * 2, 2)], off)
        else:
            arrived("tokens", entered.at[kv * 2 + 1 - tp], off)
        loaded(f"units1{index}", units1.at[chip_rows(chip), :])
        if index == kv_size - 1:
            arrived("lens", lens_all.at[pl.ds(0, devices - 1)])
        if index == kv_size - 1:
            column = live_column(cls)
            lane = iota((1, HEAD), 1)
            place = place_lanes(
                jnp.minimum(lane // slots, devices - 1), lax.rem(lane, slots), column
            )
            reorder = one_hot(iota((half, HEAD), 0) == place)[:, :half]
        square, total = ffn_slot(
            unit_acc, units1, gains1_ref, chip, chip_tokens(chip), index
        )
        squares = squares + square
        if index == kv_size - 2:
            loaded("proj", proj.at[:, 0 : 4 * cols])
            for kind in range(4):
                at = kind_cols(kind)
                to_partner("proj", proj.at[:, at], proj.at[:, at])
    hidden = dot(reorder, finish(total, squares)).astype(BF16)
    loaded("down1")
    for pair in pairs:
        chips = [swapped(off) for off in pair]
        for off, chip, term in zip(pair, chips, columns_of(hidden, down1, chips)):
            if off is pairs[1][1]:
                own_term = term
                continue
            red_send[0, off] = term[:pack].astype(BF16)
            red_send[1, off] = term[pack:].astype(BF16)
            remote("red0", red_send.at[0, off], red_recv.at[0, off], chip, core_of(chip, 0))
    loaded("out")
    to_partner("out", out_w.at[:, own_cols], out_w.at[:, own_cols])
    for name in last:
        start(name)
    residual = dot(reorder, chip_tokens(kv))
    flags = live_row(cls)
    other_flags = live_row(1 - cls)
    at = iota((rows, HEAD), 0)
    slot = lax.rem(at, slots)
    place = place_rows(at // BLK, slot, cls, flags)
    kind = lax.rem(at // slots + at // BLK + cls, 2)
    lane = iota((rows, HEAD), 1)
    spread = one_hot(
        (lane // pack == kind) & (lax.rem(lane, pack) == place) & (lane < 2 * pack)
    )[:, : 2 * pack]
    lane = iota((1, devices * 2 * BLK), 1)
    place = place_lanes(lax.rem(lane, rows) // BLK, lax.rem(lane, slots), column)
    at = iota((kv_size * pack, devices * 2 * BLK), 0)
    lane = iota((kv_size * pack, devices * 2 * BLK), 1)
    chip_at = 2 * (lane // rows) + lax.rem(lane // slots, 2)
    gather_heads = one_hot((at // pack == chip_at) & (lax.rem(at, pack) == place))
    at = iota((BLK, HEAD), 0)
    klass = lax.rem(at // slots + me, 2)
    place = place_rows(
        jnp.zeros((BLK, HEAD), jnp.int32) + me,
        lax.rem(at, slots),
        klass,
        jnp.where(klass == cls, flags, other_flags),
    )
    lane = iota((BLK, HEAD), 1)
    pick_small = jnp.where(
        (lax.rem(lane // pack + cls, 2) == klass)
        & (lax.rem(lane, pack) == place)
        & (lane < 2 * pack),
        1.0,
        0.0,
    )[:, : 2 * pack]
    at = iota((rows, HEAD), 0)
    seq, token = at // BLK, lax.rem(at, BLK)
    klass = lax.rem(seq + token, 2)
    place = place_rows(seq, token // 2, klass, jnp.where(klass == cls, flags, other_flags))
    lane = iota((rows, HEAD), 1)
    order_out[...] = one_hot(
        (lax.rem(lane // half + cls, 2) == klass)
        & (lax.rem(lane, half) == place)
        & (lane < rows)
    )[:, :rows]
    for off in far_first:
        chip = swapped(off)
        remote("red1", red_send.at[1, off], red_recv.at[1, off], chip, core_of(chip, 0))

    def first_done(group):
        at = slice(group * pack, (group + 1) * pack)
        arrived(f"red{group}", red_recv.at[group, pl.ds(1, kv_size - 1)])
        total = own_term[at]
        for off in range(1, kv_size):
            total = total + red_recv[group, off].astype(F32)
        middle[group, kv] = (residual[at] + 0.5 * total).astype(BF16)
        to_class(
            f"middle{group}",
            lambda off: middle.at[group, kv],
            lambda off: middle.at[group, kv],
            1 if group else kv_size,
        )

    first_done(0)
    loaded("state")
    for head in range(HEADS):
        high = state[head].astype(BF16)
        state_high[head] = high
        state_low[head] = (state[head] - high.astype(F32)).astype(BF16)
    arrived("proj", proj.at[:, 0 : 4 * cols])
    loaded("small", small_w.at[0 : 2 * HEADS])
    loaded("gains_mix")
    loaded("rates")
    squares = jnp.zeros((pack, 1), F32)
    for index, off in enumerate([0] + near_first):
        chip = swapped(off)
        at = chip_rows(chip)
        if index:
            arrived("middle0", middle.at[0, chip], off)
        values = middle[0, chip].astype(F32)
        squares = squares + jnp.sum(values * values, axis=1, keepdims=True)
        scaled = (values * gains_mix_ref[:, at]).astype(BF16)
        small_term = lax.dot_general(
            scaled, small_w[:, at], (((1,), (1,)), ((), ())), preferred_element_type=F32
        )
        if index == 0:
            proj_acc[...] = dot(scaled, proj[at, :])
            small_acc[0] = small_term
            first_done(1)
        elif index < kv_size - 1:
            proj_acc[...] += dot(scaled, proj[at, :])
            small_acc[0] += small_term
    mix_scale = lax.rsqrt(squares / channels + EPSILON)
    for pair in range(2):
        lanes = slice(pair * 2 * wide, (pair + 1) * 2 * wide)
        projected = proj_acc[:, lanes] + dot(scaled, proj[at, lanes])
        projected = (projected * mix_scale).astype(BF16)
        stacked = jnp.concatenate([projected[:, :wide], projected[:, wide:]], axis=0)
        part = dot(spread, stacked).astype(BF16)
        part_send[pair] = part.reshape(devices, BLK, wide)
        to_all(
            f"part{pair}",
            lambda other, peer: part_send.at[pair, peer],
            lambda other: part_recv.at[pair, kv, cls],
            near="0",
            far="1",
            order=[far_first[2], far_first[0], far_first[1]],
        )
        if pair == 0:
            small_acc[0] = (small_acc[0] + small_term) * mix_scale
            to_partner("small", small_acc.at[0], small_recv.at[0])
    for pair in range(2):
        part_recv[pair, kv, cls] = part_send[pair, me]

    def cut_terms(a):
        high = a.astype(BF16).astype(F32)
        return high, a - high

    def dot_fine(a, b, across=False):
        high_a, low_a = cut_terms(a)
        high_b, low_b = cut_terms(b)
        axis = 1 if across else 0
        left = jnp.concatenate([high_a, high_a, low_a], axis=1).astype(BF16)
        right = jnp.concatenate([high_b, low_b, high_b], axis=axis).astype(BF16)
        return lax.dot_general(
            left, right, (((1,), (axis,)), ((), ())), preferred_element_type=F32
        )

    all_sent("tokens", entered.at[pl.ds(0, devices - 1)])
    all_sent("lens", lens_all.at[pl.ds(0, devices - 1)])
    all_sent("red", red_send.at[:, pl.ds(1, kv_size - 1)])
    all_sent("out", out_w.at[:, own_cols])
    arrived("small", small_recv.at[0])
    small_all = jnp.concatenate([small_acc[0], small_recv[0]], axis=0)
    high, low = cut_terms(small_all)
    picked_small = dot(pick_small.astype(BF16), high.astype(BF16)) + dot(
        pick_small.astype(BF16), low.astype(BF16)
    )
    write_pre = picked_small[:, 0:HEADS]
    forget_pre = picked_small[:, HEADS : 2 * HEADS]

    heads = HEADS // 2
    size = heads * BLK

    def token_of(at):
        at = lax.rem(at, BLK)
        return 2 * lax.rem(at, slots) + at // slots

    row = iota((size, size), 0)
    col = iota((size, size), 1)
    same = (row // BLK) == (col // BLK)
    causal = same & (token_of(row) >= token_of(col))
    strict = same & (token_of(row) > token_of(col))
    diagonal = row == col
    live = jnp.where(token_of(iota((size, 1), 0)) < length_ref[...], 1.0, 0.0)
    upper = iota((BLK, wide), 0) < slots
    even_class = lax.rem(me, 2)
    per_chip = wide // HEAD

    def to_row(column):
        return jnp.sum(jnp.where(diagonal, column, 0.0), axis=0, keepdims=True)

    def gates(side):
        pick = side * heads + iota((size, HEADS), 0) // BLK == iota((size, HEADS), 1)

        def as_column(block):
            return jnp.sum(jnp.where(pick, block, 0.0), axis=1, keepdims=True)

        write_col = as_column(jnp.concatenate([write_pre] * heads, axis=0))
        forget_col = as_column(jnp.concatenate([forget_pre] * heads, axis=0))
        rate_col = as_column(jnp.broadcast_to(rates_ref[...], (size, HEADS)))
        write_gate = jax.nn.sigmoid(write_col) * live
        softplus = jnp.maximum(forget_col, 0.0) + jnp.log1p(jnp.exp(-jnp.abs(forget_col)))
        forget = -jnp.exp(rate_col) * softplus * live
        forget_row = to_row(forget)
        cumulative = jnp.sum(jnp.where(causal, forget_row, 0.0), axis=1, keepdims=True)
        final = jnp.sum(jnp.where(same, forget_row, 0.0), axis=1, keepdims=True)
        decay = jnp.where(
            causal, jnp.exp(jnp.minimum(cumulative - to_row(cumulative), 0.0)), 0.0
        )
        return write_gate, decay, jnp.exp(cumulative), jnp.exp(final - cumulative), jnp.exp(final)

    def by_head(pair, side):
        ahead, behind = [], []
        for at in range(2):
            chip = 2 * side + at
            even = part_recv[pair, chip, even_class].astype(F32)
            odd = part_recv[pair, chip, 1 - even_class].astype(F32)
            front = jnp.where(upper, even, odd)
            back = pltpu.roll(jnp.where(upper, odd, even), slots, 0)
            for start_at in range(0, wide, HEAD):
                ahead.append(front[:, start_at : start_at + HEAD])
                behind.append(back[:, start_at : start_at + HEAD])
        return jnp.concatenate(ahead, axis=0), jnp.concatenate(behind, axis=0)

    kept = []
    sides = [kv // 2, 1 - kv // 2]
    all_gates = [gates(side) for side in sides]
    for group, side in enumerate(sides):
        write_gate, decay, growth, fading, shrink = all_gates[group]
        arrived(f"part0{group}", part_send.at[0, pl.ds(0, 3 + group)])
        query, key_in = by_head(0, side)
        query_unit = (
            query
            * lax.rsqrt(jnp.sum(query * query, axis=1, keepdims=True) + EPSILON)
            * (1.0 / math.sqrt(HEAD))
        )
        key_unit = key_in * lax.rsqrt(
            jnp.sum(key_in * key_in, axis=1, keepdims=True) + EPSILON
        )
        products = dot_fine(jnp.concatenate([key_unit, query_unit], axis=0), key_unit, True)
        lower = jnp.where(strict, write_gate * decay * products[:size], 0.0)
        scores = products[size:] * decay
        key_grown = (write_gate * growth) * key_unit
        query_grown = query_unit * growth
        key_terms, query_terms = [], []
        for head in range(heads):
            at = slice(head * BLK, (head + 1) * BLK)
            high, low = cut_terms(jnp.concatenate([key_grown[at], query_grown[at]], axis=0))
            both = jnp.concatenate([high, low], axis=0).astype(BF16)
            result = dot(both, state_high[side * heads + head])
            result = result[: 2 * BLK] + result[2 * BLK :]
            result = result + dot(both[: 2 * BLK], state_low[side * heads + head])
            key_terms.append(result[:BLK])
            query_terms.append(result[BLK:])
            for token in range(BLK):
                place = head * BLK + slots * (token % 2) + token // 2
                spread_cols[1, head, token] = jnp.broadcast_to(
                    scores[at, place : place + 1], (BLK, HEAD)
                )
                if token < BLK - 1:
                    spread_cols[0, head, token] = jnp.broadcast_to(
                        lower[at, place : place + 1], (BLK, HEAD)
                    )
        arrived(f"part1{group}", part_send.at[1, pl.ds(0, 3 + group)])
        value, gating = by_head(1, side)
        updates, attends = [], []
        for head in range(heads):
            at = slice(head * BLK, (head + 1) * BLK)
            solved = (write_gate * value)[at] - key_terms[head]
            attend = query_terms[head]
            for token in range(BLK):
                place = slots * (token % 2) + token // 2
                known = jnp.broadcast_to(solved[place : place + 1], (BLK, HEAD))
                attend = attend + spread_cols[1, head, token] * known
                if token < BLK - 1:
                    solved = solved - spread_cols[0, head, token] * known
            updates.append(solved)
            attends.append(attend)
        attend = jnp.concatenate(attends, axis=0)
        normed = attend * lax.rsqrt(jnp.mean(attend * attend, axis=1, keepdims=True) + EPSILON)
        normed = normed * jax.nn.silu(gating) * live
        even, odd = [
            jnp.concatenate(
                [
                    normed[(first + at) * BLK : (first + at + 1) * BLK]
                    for at in range(per_chip)
                ],
                axis=1,
            )
            for first in (0, per_chip)
        ]
        heads_send[group, 0] = jnp.where(upper, even, pltpu.roll(odd, slots, 0)).astype(BF16)
        heads_send[group, 1] = jnp.where(upper, pltpu.roll(even, slots, 0), odd).astype(BF16)
        to_all(
            f"heads{group}",
            lambda other, peer: heads_send.at[group, lax.rem(cls + other + me, 2)],
            lambda other: heads_recv.at[side, me],
        )
        heads_recv[side, me] = heads_send[group, lax.rem(cls + me, 2)]
        kept.append((key_unit * fading, updates, shrink))

    for side, (faded, updates, shrink) in zip(sides, kept):
        for head in range(heads):
            at = slice(head * BLK, (head + 1) * BLK)
            key_high, key_low = cut_terms(faded[at])
            value_high, value_low = cut_terms(updates[head])
            outer = lax.dot_general(
                jnp.concatenate([key_high, key_high, key_low], axis=0).astype(BF16),
                jnp.concatenate([value_high, value_low, value_high], axis=0).astype(BF16),
                (((0,), (0,)), ((), ())),
                preferred_element_type=F32,
            )
            index = side * heads + head
            state_out[0, index] = shrink[head * BLK : head * BLK + 1] * state[index] + outer

    def hand_off(group, off):
        chip = swapped(off)
        for other in (0, 1):
            core = core_of(chip, other)
            remote(
                f"fin{group}", fin_send.at[group, off, core],
                fin_recv.at[group, off, other], chip, core,
            )

    def hand_own(group):
        to_partner(f"own{group}", own_send.at[group, 1 - tp], own_recv.at[group])

    def second_down(group, hidden, source, at_once):
        for pair in pairs:
            chips = [swapped(off) for off in pair]
            for off, chip, term in zip(pair, chips, columns_of(hidden, down2, chips)):
                if off is pairs[1][1]:
                    term = source.astype(F32) + 0.5 * term
                    own_send[group, 0] = term[:, :cols]
                    own_send[group, 1] = term[:, cols:]
                    continue
                fin_send[group, off, 0] = term[:, :cols].astype(BF16)
                fin_send[group, off, 1] = term[:, cols:].astype(BF16)
                if at_once:
                    hand_off(group, off)
        if at_once:
            hand_own(group)

    def take_in(group):
        arrived(f"own{group}", own_recv.at[group])
        arrived(f"fin{group}", fin_recv.at[group, pl.ds(1, kv_size - 1)])
        sums = [own_send[group, tp], own_recv[group]]
        for other in (0, 1):
            total = fin_recv[group, 1, other].astype(F32)
            for off in range(2, kv_size):
                total = total + fin_recv[group, off, other].astype(F32)
            sums[other] = sums[other] + 0.5 * total
        return [total.astype(BF16) for total in sums]

    loaded("gains2")
    loaded("units2", units2)
    arrived("middle1", middle.at[1, pl.ds(0, kv_size - 1)])
    values = jnp.concatenate([middle[1, chip] for chip in range(kv_size)], axis=1).astype(F32)
    squares = jnp.sum(values * values, axis=1, keepdims=True)
    dead_hidden = finish(dot((values * gains2_ref[...]).astype(BF16), units2[...]), squares)

    loaded("down2")
    second_down(1, dead_hidden, middle[1, kv], False)
    for group in range(2):
        arrived(f"heads{group}", heads_recv.at[0, pl.ds(0, devices - 1)])
    arrived("out", out_w.at[:, own_cols])
    blocks = heads_recv[...].astype(F32).reshape(devices * 2 * BLK, wide).astype(BF16)
    mixed = dot(gather_heads, blocks).astype(BF16)
    terms = []
    for part in range(2):
        chips = range(part * kv_size // 2, (part + 1) * kv_size // 2)
        left = jnp.concatenate([mixed[chip * pack : (chip + 1) * pack] for chip in chips], axis=1)
        right = out_w[chips[0] * wide : (chips[-1] + 1) * wide, :]
        terms.append(dot(left, right).astype(BF16).astype(F32))
    second_in[kv] = (middle[0, kv].astype(F32) + (terms[0] + terms[1])).astype(BF16)
    to_class("second", lambda off: second_in.at[kv], lambda off: second_in.at[kv], kv_size)

    squares = jnp.zeros((pack, 1), F32)
    for index, off in enumerate([0] + near_first):
        chip = swapped(off)
        if index:
            arrived("second", second_in.at[chip], off)
        square, total = ffn_slot(
            live_acc, units2, gains2_ref, chip, second_in[chip], index
        )
        squares = squares + square
        if index == 1:
            for off in far_first:
                hand_off(1, off)
            hand_own(1)
    hidden = finish(total, squares)
    second_down(0, hidden, second_in[kv], True)
    dead_sums = take_in(1)
    live_sums = take_in(0)
    packed_out[...] = jnp.concatenate(
        [live_sums[0], dead_sums[0], live_sums[1], dead_sums[1]], axis=0
    )
    all_sent("proj", proj.at[:, 0 : 4 * cols])
    all_sent("small", small_acc.at[0])
    all_sent("heads", heads_recv.at[:, pl.ds(0, devices - 1)])
    all_sent("second", second_in.at[pl.ds(0, kv_size - 1)])
    all_sent("middle", middle.at[:, pl.ds(0, kv_size - 1)])
    all_sent("part", part_send.at[:, pl.ds(0, devices - 1)])
    all_sent("fin", fin_send.at[:, pl.ds(1, kv_size - 1)])
    all_sent("own", own_send.at[0])


def fused_call(mesh, *args):
    (
        tokens, lengths, state, gain_first, first_gate, first_up, first_down, gain_mix,
        query_weight, key_weight, value_weight, gating_weight, write_weight, forget_weight,
        forget_rate, out_weight, gain_second, second_gate, second_up, second_down,
    ) = args
    kv_size = mesh.shape["kv"]
    devices = kv_size * mesh.shape["tp"]
    rows, cols = tokens.shape
    wide = 2 * cols
    channels = gain_first.shape[0]
    hidden_local = first_gate.shape[1]
    half, pack = rows // 2, rows // 4
    in_hbm = pl.BlockSpec(memory_space=pltpu.HBM)
    in_vmem = pl.BlockSpec(memory_space=pltpu.VMEM)
    dma = pltpu.SemaphoreType.DMA
    operands = (
        tokens, lengths.reshape(1, 1), gain_first.reshape(1, -1), gain_mix.reshape(1, -1),
        gain_second.reshape(1, -1), forget_rate.reshape(1, -1), state,
        first_gate, first_up, first_down, query_weight, key_weight, value_weight,
        gating_weight, write_weight.T, forget_weight.T, out_weight, second_gate, second_up,
        second_down,
    )
    operands = [
        array if array.dtype == jnp.int32 else pltpu.with_memory_space_constraint(array, pltpu.HBM)
        for array in operands
    ]
    results = pl.pallas_call(
        functools.partial(fused_kernel, kv_size, channels),
        out_shape=(
            pltpu.VMEM(tokens.shape, tokens.dtype),
            pltpu.VMEM((rows, rows), BF16),
            pltpu.VMEM(state.shape, state.dtype),
        ),
        in_specs=[in_hbm] * len(operands),
        out_specs=(in_vmem, in_vmem, in_vmem),
        scratch_shapes=[
            pltpu.VMEM((channels, 2 * hidden_local), BF16),
            pltpu.VMEM((hidden_local, channels), BF16),
            pltpu.VMEM((channels, 2 * hidden_local), BF16),
            pltpu.VMEM((hidden_local, channels), BF16),
            pltpu.VMEM((channels, 4 * wide), BF16),
            pltpu.VMEM((channels, wide), BF16),
            pltpu.VMEM((HEAD, channels), BF16),
            pltpu.VMEM(state.shape[1:], F32),
            pltpu.VMEM(state.shape[1:], BF16),
            pltpu.VMEM(state.shape[1:], BF16),
            pltpu.VMEM((1, channels), F32),
            pltpu.VMEM((1, channels), F32),
            pltpu.VMEM((1, channels), F32),
            pltpu.VMEM((1, HEADS), F32),
            pltpu.VMEM((rows, cols), BF16),
            pltpu.VMEM((1, 1), jnp.int32),
            pltpu.VMEM((devices, 1, HEAD), jnp.int32),
            pltpu.VMEM((2, half, cols), BF16),
            pltpu.VMEM((devices, half, cols), BF16),
            pltpu.VMEM((half, 2 * hidden_local), F32),
            pltpu.VMEM((pack, 2 * hidden_local), F32),
            pltpu.VMEM((pack, 4 * wide), F32),
            pltpu.VMEM((1, pack, HEAD), F32),
            pltpu.VMEM((2, kv_size, pack, wide), BF16),
            pltpu.VMEM((kv_size, pack, wide), BF16),
            pltpu.VMEM((2, 2, BLK, wide), BF16),
            pltpu.VMEM((2, devices, BLK, wide), BF16),
            pltpu.VMEM((2, kv_size, pack, wide), BF16),
            pltpu.VMEM((2, kv_size, pack, wide), BF16),
            pltpu.VMEM((2, devices, BLK, wide), BF16),
            pltpu.VMEM((2, kv_size, 2, BLK, wide), BF16),
            pltpu.VMEM((1, pack, HEAD), F32),
            pltpu.VMEM((2, kv_size, 2, pack, cols), BF16),
            pltpu.VMEM((2, kv_size, 2, pack, cols), BF16),
            pltpu.VMEM((2, 2, pack, cols), F32),
            pltpu.VMEM((2, pack, cols), F32),
            pltpu.VMEM((2, HEADS // 2, BLK, BLK, HEAD), F32),
            dma((kv_size + 7,)),
            dma((8,)),
            dma((2 * kv_size + 11,)),
        ],
        compiler_params=pltpu.CompilerParams(
            collective_id=0, has_side_effects=True, vmem_limit_bytes=VMEM_LIMIT
        ),
    )(*operands)
    return hand_out(*results)


def hand_out_kernel(packed, order, state, mixed_hbm, state_hbm, mixed, sems):
    puts = [pltpu.make_async_copy(state, state_hbm, sems.at[0])]
    puts[0].start()
    restored = jnp.dot(order[...], packed[...], preferred_element_type=F32)
    mixed[...] = restored.astype(BF16)
    puts.append(pltpu.make_async_copy(mixed, mixed_hbm, sems.at[1]))
    puts[-1].start()
    for put in puts:
        put.wait()


def hand_out(packed, order, new_state):
    in_hbm = pl.BlockSpec(memory_space=pltpu.HBM)
    in_vmem = pl.BlockSpec(memory_space=pltpu.VMEM)
    arrays = [
        pltpu.with_memory_space_constraint(array, pltpu.VMEM)
        for array in (packed, order, new_state)
    ]
    return pl.pallas_call(
        hand_out_kernel,
        out_shape=(
            jax.ShapeDtypeStruct(packed.shape, packed.dtype),
            jax.ShapeDtypeStruct(new_state.shape, new_state.dtype),
        ),
        in_specs=[in_vmem] * 3,
        out_specs=(in_hbm, in_hbm),
        scratch_shapes=[
            pltpu.VMEM(packed.shape, packed.dtype),
            pltpu.SemaphoreType.DMA((2,)),
        ],
        compiler_params=pltpu.CompilerParams(vmem_limit_bytes=8 * 1024 * 1024),
    )(*arrays)


def fits_fused(mesh, args):
    tokens, lengths, state, first_gate = args[0], args[1], args[2], args[4]
    rows, cols = tokens.shape
    kv_size = mesh.shape["kv"]
    devices = kv_size * mesh.shape["tp"]
    return (
        mesh.shape["tp"] == 2
        and mesh.shape["kv"] & (mesh.shape["kv"] - 1) == 0
        and lengths.shape[0] == 1
        and rows == devices * BLK
        and devices * 2 * BLK == HEAD
        and kv_size * BLK // 2 == 2 * BLK
        and devices * cols == HEADS * HEAD
        and cols % 256 == 0
        and first_gate.shape[1] % 128 == 0
        and state.shape[1:] == (HEADS, HEAD, HEAD)
    )


def solution(mesh):
    in_specs = (
        P("dp", ("kv", "tp")),
        P(("dp", "kv", "tp")),
        P(("dp", "kv", "tp"), None, None, None),
        P(),
        P(None, "kv"),
        P(None, "kv"),
        P("kv", None),
        P(),
        P(None, ("kv", "tp")),
        P(None, ("kv", "tp")),
        P(None, ("kv", "tp")),
        P(None, ("kv", "tp")),
        P(),
        P(),
        P(),
        P(None, ("kv", "tp")),
        P(),
        P(None, "kv"),
        P(None, "kv"),
        P("kv", None),
    )
    out_specs = (P("dp", ("kv", "tp")), P(("dp", "kv", "tp"), None, None, None))

    def body(*args):
        if fits_fused(mesh, args):
            return fused_call(mesh, *args)
        return per_device(*args)

    return jax.shard_map(
        body, mesh=mesh, in_specs=in_specs, out_specs=out_specs, check_vma=False
    )
```

```python
import functools
import math

import jax
import jax.numpy as jnp
from jax import lax
from jax.experimental import pallas as pl
from jax.experimental.pallas import tpu as pltpu
from jax.sharding import PartitionSpec as P

HEADS = 16
HEAD = 128
BLK = 8


EPSILON = 1e-06


def fold_step(gain, gate_cols, up_cols, portion):
    values = portion.astype(jnp.float32)
    scaled = (values * gain).astype(jnp.bfloat16)
    gate_acc = jnp.dot(scaled, gate_cols, preferred_element_type=jnp.float32)
    up_acc = jnp.dot(scaled, up_cols, preferred_element_type=jnp.float32)
    squares = jnp.sum(values * values, axis=1)
    return (gate_acc, up_acc, squares)


def finish_units(gate_acc, up_acc, squares, channels, down_rows):
    row_scale = lax.rsqrt(squares / channels + EPSILON)[:, None]
    hidden = (jax.nn.silu(gate_acc * row_scale) * (up_acc * row_scale)).astype(jnp.bfloat16)
    return jnp.dot(hidden, down_rows, preferred_element_type=jnp.float32)


def feed_forward(hidden_in, gain, w_gate, w_up, w_down):
    channels = gain.shape[0]
    paired = lax.all_to_all(hidden_in, "tp", split_axis=0, concat_axis=1, tiled=True)
    gate_acc, up_acc, squares = fold_step(
        gain, w_gate, w_up, lax.all_gather(paired, "kv", axis=1, tiled=True)
    )
    ffn_term = finish_units(gate_acc, up_acc, squares, channels, w_down)
    partial_value = lax.psum_scatter(ffn_term, "kv", scatter_dimension=1, tiled=True)
    summed = lax.all_to_all(partial_value, "tp", split_axis=1, concat_axis=0, tiled=True)
    return (hidden_in.astype(jnp.float32) + 0.5 * summed).astype(jnp.bfloat16)


def delta_block(query, key_in, value, gating, write_pre, forget_pre, rates, live, state):
    seq_count, block_len, head_count, head_size = query.shape
    precise = lax.Precision.HIGHEST
    query_unit = (
        query
        * lax.rsqrt(jnp.sum(query * query, axis=-1, keepdims=True) + EPSILON)
        / math.sqrt(head_size)
    )
    key_unit = key_in * lax.rsqrt(jnp.sum(key_in * key_in, axis=-1, keepdims=True) + EPSILON)
    live_rows = live[:, :, None]
    write_gate = jax.nn.sigmoid(write_pre) * live_rows
    forget = -jnp.exp(rates)[None, None, :] * jax.nn.softplus(forget_pre) * live_rows
    cumulative = jnp.cumsum(forget, axis=1)
    cum_heads = jnp.transpose(cumulative, (0, 2, 1))
    positions = jnp.arange(block_len)
    causal = positions[:, None] >= positions[None, :]
    strict = positions[:, None] > positions[None, :]
    differ = jnp.minimum(cum_heads[:, :, :, None] - cum_heads[:, :, None, :], 0.0)
    decay_mat = jnp.where(causal, jnp.exp(differ), 0.0)
    key_dots = jnp.einsum("sthd,suhd->shtu", key_unit, key_unit, precision=precise)
    write_heads = jnp.transpose(write_gate, (0, 2, 1))
    strict_part = jnp.where(strict, write_heads[:, :, :, None] * decay_mat * key_dots, 0.0)
    identity = jnp.eye(block_len, dtype=jnp.float32)
    squared = jnp.einsum("shtu,shuv->shtv", strict_part, strict_part, precision=precise)
    fourth = jnp.einsum("shtu,shuv->shtv", squared, squared, precision=precise)
    inverse = jnp.einsum(
        "shtu,shuv->shtv", identity - strict_part, identity + squared, precision=precise
    )
    inverse = jnp.einsum("shtu,shuv->shtv", inverse, identity + fourth, precision=precise)
    growth = jnp.exp(cumulative)
    target = jnp.einsum(
        "shtu,suhv->sthv", inverse, write_gate[..., None] * value, precision=precise
    )
    key_mix = jnp.einsum(
        "shtu,suhk->sthk", inverse, (write_gate * growth)[..., None] * key_unit, precision=precise
    )
    update = target - jnp.einsum("sthk,shkv->sthv", key_mix, state, precision=precise)
    scores = jnp.einsum("sthd,suhd->shtu", query_unit, key_unit, precision=precise) * decay_mat
    attend = jnp.einsum("sthk,shkv->sthv", query_unit * growth[..., None], state, precision=precise)
    attend = attend + jnp.einsum("shtu,suhv->sthv", scores, update, precision=precise)
    final_cum = cumulative[:, -1:, :]
    fading = jnp.exp(final_cum - cumulative)
    new_state = jnp.exp(final_cum[:, 0, :])[:, :, None, None] * state
    new_state = new_state + jnp.einsum(
        "sthk,sthv->shkv", key_unit * fading[..., None], update, precision=precise
    )
    normed = attend * lax.rsqrt(jnp.mean(attend * attend, axis=-1, keepdims=True) + EPSILON)
    normed = normed * jax.nn.silu(gating) * live[:, :, None, None]
    mixed_heads = normed.reshape(seq_count * block_len, head_count * head_size).astype(jnp.bfloat16)
    return (mixed_heads, new_state)


def per_device(
    tokens,
    lengths,
    state,
    gain_first,
    first_gate,
    first_up,
    first_down,
    gain_mix,
    query_weight,
    key_weight,
    value_weight,
    gating_weight,
    write_weight,
    forget_weight,
    forget_rate,
    out_weight,
    gain_second,
    second_gate,
    second_up,
    second_down,
):
    after_first = feed_forward(tokens, gain_first, first_gate, first_up, first_down)
    seq_count = lengths.shape[0]
    own_count = seq_count * BLK
    whole_rows = lax.all_gather(after_first, ("kv", "tp"), axis=1, tiled=True)
    scaled_all = (whole_rows.astype(jnp.float32) * gain_mix).astype(jnp.bfloat16)
    stacked = jnp.stack(
        [
            jnp.dot(scaled_all, matrix, preferred_element_type=jnp.float32)
            for matrix in (query_weight, key_weight, value_weight, gating_weight)
        ]
    )
    owned = lax.all_to_all(
        stacked.astype(jnp.bfloat16), ("kv", "tp"), split_axis=1, concat_axis=2, tiled=True
    ).astype(stacked.dtype)
    row_start = lax.axis_index(("kv", "tp")) * own_count
    own_values = lax.dynamic_slice_in_dim(whole_rows, row_start, own_count, 0).astype(jnp.float32)
    own_scaled = lax.dynamic_slice_in_dim(scaled_all, row_start, own_count, 0)
    mix_scale = lax.rsqrt(jnp.mean(own_values * own_values, axis=1, keepdims=True) + EPSILON)
    query = (owned[0] * mix_scale).reshape(seq_count, BLK, HEADS, HEAD)
    key_in = (owned[1] * mix_scale).reshape(seq_count, BLK, HEADS, HEAD)
    value = (owned[2] * mix_scale).reshape(seq_count, BLK, HEADS, HEAD)
    gating = (owned[3] * mix_scale).reshape(seq_count, BLK, HEADS, HEAD)
    write_pre = (
        jnp.dot(own_scaled, write_weight, preferred_element_type=jnp.float32) * mix_scale
    ).reshape(seq_count, BLK, HEADS)
    forget_pre = (
        jnp.dot(own_scaled, forget_weight, preferred_element_type=jnp.float32) * mix_scale
    ).reshape(seq_count, BLK, HEADS)
    positions = jnp.arange(BLK, dtype=jnp.int32)
    live = (positions[None, :] < lengths[:, None]).astype(jnp.float32)
    mixed_heads, new_state = delta_block(
        query, key_in, value, gating, write_pre, forget_pre, forget_rate, live, state
    )
    half_cols = mixed_heads.shape[1] // 2
    portion = lax.all_gather(mixed_heads, ("kv", "tp"), axis=0, tiled=True)
    first_half = jnp.dot(
        portion[:, :half_cols], out_weight[:half_cols], preferred_element_type=jnp.float32
    ).astype(jnp.bfloat16)
    second_half = jnp.dot(
        portion[:, half_cols:], out_weight[half_cols:], preferred_element_type=jnp.float32
    ).astype(jnp.bfloat16)
    first_half, second_half = lax.optimization_barrier((first_half, second_half))
    mixed_sum = first_half.astype(jnp.float32) + second_half.astype(jnp.float32)
    after_mix = (after_first.astype(jnp.float32) + mixed_sum).astype(jnp.bfloat16)
    mixed_out = feed_forward(after_mix, gain_second, second_gate, second_up, second_down)
    return (mixed_out, new_state)


F32 = jnp.float32
BF16 = jnp.bfloat16
MESH = pl.DeviceIdType.MESH
VMEM_LIMIT = 58 * 1024 * 1024


def fused_kernel(
    kv_size,
    channels,
    tokens_hbm,
    lengths_hbm,
    gains1_hbm,
    gains_mix_hbm,
    gains2_hbm,
    rates_hbm,
    state_hbm,
    gate1_hbm,
    up1_hbm,
    down1_hbm,
    query_hbm,
    key_hbm,
    value_hbm,
    gating_hbm,
    write_hbm,
    forget_hbm,
    out_hbm,
    gate2_hbm,
    up2_hbm,
    down2_hbm,
    packed_out,
    order_out,
    state_out,
    units1,
    down1,
    units2,
    down2,
    proj,
    out_w,
    small_w,
    state,
    state_high,
    state_low,
    gains1_ref,
    gains_mix_ref,
    gains2_ref,
    rates_ref,
    tokens_ref,
    length_ref,
    lens_all,
    picked,
    entered,
    unit_acc,
    live_acc,
    proj_acc,
    small_acc,
    middle,
    second_in,
    heads_send,
    heads_recv,
    red_send,
    red_recv,
    part_send,
    part_recv,
    small_recv,
    fin_send,
    fin_recv,
    own_send,
    own_recv,
    spread_cols,
    load_sems,
    send_sems,
    recv_sems,
):
    kv = lax.axis_index("kv")
    tp = lax.axis_index("tp")
    devices = 2 * kv_size
    me = kv * 2 + tp
    cls = lax.rem(kv + tp, 2)
    rows, cols = tokens_ref.shape
    wide = 2 * cols
    slots = BLK // 2
    half = rows // 2
    pack = rows // 4
    hidden_local = gate1_hbm.shape[1]
    own_cols = pl.ds(pl.multiple_of(tp * cols, cols), cols)
    inner = lax.rem((kv + 1) // 2, 2)
    near_first = [1, 2 + inner, 3 - inner]
    far_first = near_first[::-1]

    loads, load_at = {}, {}

    def load(name, *pairs, after=None):
        load_at[name] = load_at[after] if after else len(set(load_at.values()))
        sem = load_sems.at[load_at[name]]
        loads[name] = [pltpu.make_async_copy(src, dst, sem) for src, dst in pairs]

    def start(name):
        for copy in loads[name]:
            copy.start()

    def loaded(name, ref=None):
        if ref is None:
            loads[name][0].wait()
        else:
            sem = load_sems.at[load_at[name]]
            pltpu.make_async_copy(ref, ref, sem).wait()

    def swapped(off):
        chip, bit = 0, 1
        while bit < kv_size:
            chip = chip + bit * lax.rem(kv // bit + off // bit, 2)
            bit *= 2
        return chip

    def core_of(chip, other):
        return lax.rem(chip + cls + other, 2)

    def chip_rows(chip):
        return pl.ds(pl.multiple_of(chip * wide, wide), wide)

    def kind_cols(kind):
        return pl.ds(pl.multiple_of(kind * wide + tp * cols, cols), cols)

    load("length", (lengths_hbm, length_ref))
    load("tokens", (tokens_hbm, tokens_ref))
    load("gains1", (gains1_hbm, gains1_ref))
    for index, off in enumerate([0] + near_first):
        at = chip_rows(swapped(off))
        load(
            f"units1{index}",
            (gate1_hbm.at[at, :], units1.at[at, 0:hidden_local]),
            (up1_hbm.at[at, :], units1.at[at, hidden_local : 2 * hidden_local]),
        )
    early = list(loads)
    kinds = (query_hbm, key_hbm, value_hbm, gating_hbm)
    load("proj", *[(ref, proj.at[:, kind_cols(kind)]) for kind, ref in enumerate(kinds)])
    load("down1", (down1_hbm, down1))
    load(
        "small",
        (write_hbm, small_w.at[0:HEADS]),
        (forget_hbm, small_w.at[HEADS : 2 * HEADS]),
    )
    load("gains_mix", (gains_mix_hbm, gains_mix_ref), after="length")
    load("rates", (rates_hbm, rates_ref), after="tokens")
    load("out", (out_hbm, out_w.at[:, own_cols]))
    load("state", (state_hbm.at[0], state), after="units10")
    load("gains2", (gains2_hbm, gains2_ref), after="gains1")
    load(
        "units2",
        (gate2_hbm, units2.at[:, 0:hidden_local]),
        (up2_hbm, units2.at[:, hidden_local : 2 * hidden_local]),
        after="units11",
    )
    load("down2", (down2_hbm, down2), after="units12")
    last = ("state", "gains2", "units2", "down2")
    late = [name for name in loads if name not in early and name not in last]
    barrier = pltpu.get_barrier_semaphore()
    here = 0
    for off in far_first + [here]:
        for core in (tp, 1 - tp) if off is not here else (1 - tp,):
            pl.semaphore_signal(
                barrier, inc=1, device_id={"kv": swapped(off), "tp": core}, device_id_type=MESH
            )
    for name in early:
        start(name)

    sends, receives, width = {}, {}, [0]
    send_after = {"heads": "tokens", "second": "lens", "fin": "red", "own": "out"}
    receive_after = {
        "heads0": "tokens",
        "heads1": "lens",
        "second": "tokens",
        "fin0": "red0",
        "fin1": "red1",
        "own0": "small",
        "own1": "proj",
    }

    def remote(name, src, dst, chip, core, at=0, spread=1):
        base = name.rstrip("01")
        if base not in sends:
            sends[base] = sends[send_after[base]] if base in send_after else len(set(sends.values()))
        if name not in receives:
            if name in receive_after:
                receives[name] = receives[receive_after[name]]
            else:
                receives[name] = width[0]
                width[0] += spread
        copy = pltpu.make_async_remote_copy(
            src_ref=src,
            dst_ref=dst,
            send_sem=send_sems.at[sends[name.rstrip("01")]],
            recv_sem=recv_sems.at[receives[name] + at],
            device_id={"kv": chip, "tp": core},
            device_id_type=MESH,
        )
        copy.start()

    def arrived(name, ref, at=0):
        sem = recv_sems.at[receives[name] + at]
        pltpu.make_async_remote_copy(
            src_ref=ref,
            dst_ref=ref,
            send_sem=sem,
            recv_sem=sem,
            device_id={"kv": kv, "tp": 1 - tp},
            device_id_type=MESH,
        ).wait_recv()

    def all_sent(name, ref):
        sem = send_sems.at[sends[name]]
        pltpu.make_async_remote_copy(
            src_ref=ref,
            dst_ref=ref,
            send_sem=sem,
            recv_sem=sem,
            device_id={"kv": kv, "tp": 1 - tp},
            device_id_type=MESH,
        ).wait_send()

    def to_class(name, src, dst, spread=1):
        for off in far_first:
            chip = swapped(off)
            remote(name, src(off), dst(off), chip, core_of(chip, 0), off if spread > 1 else 0, spread)

    def to_all(name, src, dst, spread=1, near="", far="", order=far_first):
        for off in order:
            chip = swapped(off)
            first = lax.rem(chip + cls, 2)
            for other in (first, 1 - first):
                core = core_of(chip, other)
                remote(
                    name + (near if off is far_first[2] else far),
                    src(other, chip * 2 + core), dst(other), chip, core,
                    off if spread > 1 else 0, spread,
                )
        to_partner(name + near, src(1, kv * 2 + 1 - tp), dst(1))

    def to_partner(name, src, dst):
        remote(name, src, dst, kv, 1 - tp)

    def columns_of(hidden, down, chips):
        right = jnp.concatenate([down[:, chip_rows(chip)] for chip in chips], axis=1)
        both = jnp.dot(hidden, right, preferred_element_type=F32)
        return [both[:, at * wide : (at + 1) * wide] for at in range(len(chips))]

    pairs = [(far_first[0], far_first[1]), (far_first[2], 0)]

    def iota(shape, axis):
        return lax.broadcasted_iota(jnp.int32, shape, axis)

    def dot(a, b):
        return jnp.dot(a, b, preferred_element_type=F32)

    def one_hot(mask):
        return jnp.where(mask, 1.0, 0.0).astype(BF16)

    row = iota((rows, rows), 0)
    col = iota((rows, rows), 1)
    at_class = lax.rem(row, half)
    at_seq = at_class // slots
    which = lax.rem(cls + row // half + at_seq, 2)
    picks = one_hot(col == at_seq * BLK + 2 * lax.rem(at_class, slots) + which)
    loaded("length")
    loaded("tokens")
    lens_all[me] = jnp.broadcast_to(length_ref[...], (1, HEAD))
    chosen = dot(picks, tokens_ref[...]).astype(BF16)
    picked[...] = chosen.reshape(2, half, cols)
    entered[me] = chosen[:half]
    pl.semaphore_wait(barrier, devices - 1)
    to_all("tokens", lambda other, peer: picked.at[other], lambda other: entered.at[me], kv_size)
    to_all("lens", lambda other, peer: lens_all.at[me], lambda other: lens_all.at[me])
    for name in late:
        start(name)
    small_w[2 * HEADS :] = jnp.zeros((HEAD - 2 * HEADS, channels), BF16)

    def ffn_slot(acc, units, gain_ref, chip, portion, index):
        at = chip_rows(chip)
        values = portion.astype(F32)
        scaled = (values * gain_ref[:, at]).astype(BF16)
        term = dot(scaled, units[at, :])
        if index == 0:
            acc[...] = term
        elif index < kv_size - 1:
            acc[...] += term
        else:
            term = acc[...] + term
        return jnp.sum(values * values, axis=1, keepdims=True), term

    def finish(acc, squares):
        row_scale = lax.rsqrt(squares / channels + EPSILON)
        gate = acc[:, 0:hidden_local] * row_scale
        up = acc[:, hidden_local : 2 * hidden_local] * row_scale
        return (jax.nn.silu(gate) * up).astype(BF16)

    def lengths_by(seq):
        found = jnp.zeros(seq.shape, jnp.int32)
        for index in range(devices):
            found = jnp.where(seq == index, lens_all[index], found)
        return found

    def is_live(seq, slot, klass):
        return 2 * slot + lax.rem(klass + seq, 2) < lengths_by(seq)

    def live_column(klass):
        at = iota((half, HEAD), 0)
        return jnp.where(is_live(at // slots, lax.rem(at, slots), klass), 1.0, 0.0)

    def live_row(klass):
        at = iota((1, HEAD), 1)
        live = is_live(at // slots, lax.rem(at, slots), klass) & (at < half)
        return jnp.where(live, 1.0, 0.0)

    def place_lanes(seq, slot, column):
        target = seq * slots + slot
        before = jnp.sum(
            jnp.where(iota((half, HEAD), 0) < target, column, 0.0), axis=0, keepdims=True
        )
        count = jnp.sum(column, axis=0, keepdims=True)
        rest = count + target.astype(F32) - before
        return jnp.where(is_live(seq, slot, cls), before, rest).astype(jnp.int32)

    def place_rows(seq, slot, klass, flags):
        target = seq * slots + slot
        before = jnp.sum(
            jnp.where(iota(seq.shape, 1) < target, flags, 0.0), axis=1, keepdims=True
        )
        count = jnp.sum(flags, axis=1, keepdims=True)
        rest = count + target.astype(F32) - before
        return jnp.where(is_live(seq, slot, klass), before, rest).astype(jnp.int32)

    def chip_tokens(chip):
        return jnp.concatenate([entered[chip * 2], entered[chip * 2 + 1]], axis=1)

    loaded("gains1")
    squares = jnp.zeros((half, 1), F32)
    for index, off in enumerate([0] + near_first):
        chip = swapped(off)
        if index:
            arrived("tokens", entered.at[pl.ds(chip * 2, 2)], off)
        else:
            arrived("tokens", entered.at[kv * 2 + 1 - tp], off)
        loaded(f"units1{index}", units1.at[chip_rows(chip), :])
        if index == kv_size - 1:
            arrived("lens", lens_all.at[pl.ds(0, devices - 1)])
        if index == kv_size - 1:
            column = live_column(cls)
            lane = iota((1, HEAD), 1)
            place = place_lanes(
                jnp.minimum(lane // slots, devices - 1), lax.rem(lane, slots), column
            )
            reorder = one_hot(iota((half, HEAD), 0) == place)[:, :half]
        square, total = ffn_slot(
            unit_acc, units1, gains1_ref, chip, chip_tokens(chip), index
        )
        squares = squares + square
        if index == kv_size - 2:
            loaded("proj", proj.at[:, 0 : 4 * cols])
            for kind in range(4):
                at = kind_cols(kind)
                to_partner("proj", proj.at[:, at], proj.at[:, at])
    hidden = dot(reorder, finish(total, squares)).astype(BF16)
    loaded("down1")
    for pair in pairs:
        chips = [swapped(off) for off in pair]
        for off, chip, term in zip(pair, chips, columns_of(hidden, down1, chips)):
            if off is pairs[1][1]:
                own_term = term
                continue
            red_send[0, off] = term[:pack].astype(BF16)
            red_send[1, off] = term[pack:].astype(BF16)
            remote("red0", red_send.at[0, off], red_recv.at[0, off], chip, core_of(chip, 0))
    loaded("out")
    to_partner("out", out_w.at[:, own_cols], out_w.at[:, own_cols])
    for name in last:
        start(name)
    residual = dot(reorder, chip_tokens(kv))
    flags = live_row(cls)
    other_flags = live_row(1 - cls)
    at = iota((rows, HEAD), 0)
    slot = lax.rem(at, slots)
    place = place_rows(at // BLK, slot, cls, flags)
    kind = lax.rem(at // slots + at // BLK + cls, 2)
    lane = iota((rows, HEAD), 1)
    spread = one_hot(
        (lane // pack == kind) & (lax.rem(lane, pack) == place) & (lane < 2 * pack)
    )[:, : 2 * pack]
    lane = iota((1, devices * 2 * BLK), 1)
    place = place_lanes(lax.rem(lane, rows) // BLK, lax.rem(lane, slots), column)
    at = iota((kv_size * pack, devices * 2 * BLK), 0)
    lane = iota((kv_size * pack, devices * 2 * BLK), 1)
    chip_at = 2 * (lane // rows) + lax.rem(lane // slots, 2)
    gather_heads = one_hot((at // pack == chip_at) & (lax.rem(at, pack) == place))
    at = iota((BLK, HEAD), 0)
    klass = lax.rem(at // slots + me, 2)
    place = place_rows(
        jnp.zeros((BLK, HEAD), jnp.int32) + me,
        lax.rem(at, slots),
        klass,
        jnp.where(klass == cls, flags, other_flags),
    )
    lane = iota((BLK, HEAD), 1)
    pick_small = jnp.where(
        (lax.rem(lane // pack + cls, 2) == klass)
        & (lax.rem(lane, pack) == place)
        & (lane < 2 * pack),
        1.0,
        0.0,
    )[:, : 2 * pack]
    at = iota((rows, HEAD), 0)
    seq, token = at // BLK, lax.rem(at, BLK)
    klass = lax.rem(seq + token, 2)
    place = place_rows(seq, token // 2, klass, jnp.where(klass == cls, flags, other_flags))
    lane = iota((rows, HEAD), 1)
    order_out[...] = one_hot(
        (lax.rem(lane // half + cls, 2) == klass)
        & (lax.rem(lane, half) == place)
        & (lane < rows)
    )[:, :rows]
    for off in far_first:
        chip = swapped(off)
        remote("red1", red_send.at[1, off], red_recv.at[1, off], chip, core_of(chip, 0))

    def first_done(group):
        at = slice(group * pack, (group + 1) * pack)
        arrived(f"red{group}", red_recv.at[group, pl.ds(1, kv_size - 1)])
        total = own_term[at]
        for off in range(1, kv_size):
            total = total + red_recv[group, off].astype(F32)
        middle[group, kv] = (residual[at] + 0.5 * total).astype(BF16)
        to_class(
            f"middle{group}",
            lambda off: middle.at[group, kv],
            lambda off: middle.at[group, kv],
            1 if group else kv_size,
        )

    first_done(0)
    loaded("state")
    for head in range(HEADS):
        high = state[head].astype(BF16)
        state_high[head] = high
        state_low[head] = (state[head] - high.astype(F32)).astype(BF16)
    arrived("proj", proj.at[:, 0 : 4 * cols])
    loaded("small", small_w.at[0 : 2 * HEADS])
    loaded("gains_mix")
    loaded("rates")
    squares = jnp.zeros((pack, 1), F32)
    for index, off in enumerate([0] + near_first):
        chip = swapped(off)
        at = chip_rows(chip)
        if index:
            arrived("middle0", middle.at[0, chip], off)
        values = middle[0, chip].astype(F32)
        squares = squares + jnp.sum(values * values, axis=1, keepdims=True)
        scaled = (values * gains_mix_ref[:, at]).astype(BF16)
        small_term = lax.dot_general(
            scaled, small_w[:, at], (((1,), (1,)), ((), ())), preferred_element_type=F32
        )
        if index == 0:
            proj_acc[...] = dot(scaled, proj[at, :])
            small_acc[0] = small_term
            first_done(1)
        elif index < kv_size - 1:
            proj_acc[...] += dot(scaled, proj[at, :])
            small_acc[0] += small_term
    mix_scale = lax.rsqrt(squares / channels + EPSILON)
    for pair in range(2):
        lanes = slice(pair * 2 * wide, (pair + 1) * 2 * wide)
        projected = proj_acc[:, lanes] + dot(scaled, proj[at, lanes])
        projected = (projected * mix_scale).astype(BF16)
        stacked = jnp.concatenate([projected[:, :wide], projected[:, wide:]], axis=0)
        part = dot(spread, stacked).astype(BF16)
        part_send[pair] = part.reshape(devices, BLK, wide)
        to_all(
            f"part{pair}",
            lambda other, peer: part_send.at[pair, peer],
            lambda other: part_recv.at[pair, kv, cls],
            near="0",
            far="1",
            order=[far_first[2], far_first[0], far_first[1]],
        )
        if pair == 0:
            small_acc[0] = (small_acc[0] + small_term) * mix_scale
            to_partner("small", small_acc.at[0], small_recv.at[0])
    for pair in range(2):
        part_recv[pair, kv, cls] = part_send[pair, me]

    def cut_terms(a):
        high = a.astype(BF16).astype(F32)
        return high, a - high

    def dot_fine(a, b, across=False):
        high_a, low_a = cut_terms(a)
        high_b, low_b = cut_terms(b)
        axis = 1 if across else 0
        left = jnp.concatenate([high_a, high_a, low_a], axis=1).astype(BF16)
        right = jnp.concatenate([high_b, low_b, high_b], axis=axis).astype(BF16)
        return lax.dot_general(
            left, right, (((1,), (axis,)), ((), ())), preferred_element_type=F32
        )

    all_sent("tokens", entered.at[pl.ds(0, devices - 1)])
    all_sent("lens", lens_all.at[pl.ds(0, devices - 1)])
    all_sent("red", red_send.at[:, pl.ds(1, kv_size - 1)])
    all_sent("out", out_w.at[:, own_cols])
    arrived("small", small_recv.at[0])
    small_all = jnp.concatenate([small_acc[0], small_recv[0]], axis=0)
    high, low = cut_terms(small_all)
    picked_small = dot(pick_small.astype(BF16), high.astype(BF16)) + dot(
        pick_small.astype(BF16), low.astype(BF16)
    )
    write_pre = picked_small[:, 0:HEADS]
    forget_pre = picked_small[:, HEADS : 2 * HEADS]

    heads = HEADS // 2
    size = heads * BLK

    def token_of(at):
        at = lax.rem(at, BLK)
        return 2 * lax.rem(at, slots) + at // slots

    row = iota((size, size), 0)
    col = iota((size, size), 1)
    same = (row // BLK) == (col // BLK)
    causal = same & (token_of(row) >= token_of(col))
    strict = same & (token_of(row) > token_of(col))
    diagonal = row == col
    live = jnp.where(token_of(iota((size, 1), 0)) < length_ref[...], 1.0, 0.0)
    upper = iota((BLK, wide), 0) < slots
    even_class = lax.rem(me, 2)
    per_chip = wide // HEAD

    def to_row(column):
        return jnp.sum(jnp.where(diagonal, column, 0.0), axis=0, keepdims=True)

    def gates(side):
        pick = side * heads + iota((size, HEADS), 0) // BLK == iota((size, HEADS), 1)

        def as_column(block):
            return jnp.sum(jnp.where(pick, block, 0.0), axis=1, keepdims=True)

        write_col = as_column(jnp.concatenate([write_pre] * heads, axis=0))
        forget_col = as_column(jnp.concatenate([forget_pre] * heads, axis=0))
        rate_col = as_column(jnp.broadcast_to(rates_ref[...], (size, HEADS)))
        write_gate = jax.nn.sigmoid(write_col) * live
        softplus = jnp.maximum(forget_col, 0.0) + jnp.log1p(jnp.exp(-jnp.abs(forget_col)))
        forget = -jnp.exp(rate_col) * softplus * live
        forget_row = to_row(forget)
        cumulative = jnp.sum(jnp.where(causal, forget_row, 0.0), axis=1, keepdims=True)
        final = jnp.sum(jnp.where(same, forget_row, 0.0), axis=1, keepdims=True)
        decay = jnp.where(
            causal, jnp.exp(jnp.minimum(cumulative - to_row(cumulative), 0.0)), 0.0
        )
        return write_gate, decay, jnp.exp(cumulative), jnp.exp(final - cumulative), jnp.exp(final)

    def by_head(pair, side):
        ahead, behind = [], []
        for at in range(2):
            chip = 2 * side + at
            even = part_recv[pair, chip, even_class].astype(F32)
            odd = part_recv[pair, chip, 1 - even_class].astype(F32)
            front = jnp.where(upper, even, odd)
            back = pltpu.roll(jnp.where(upper, odd, even), slots, 0)
            for start_at in range(0, wide, HEAD):
                ahead.append(front[:, start_at : start_at + HEAD])
                behind.append(back[:, start_at : start_at + HEAD])
        return jnp.concatenate(ahead, axis=0), jnp.concatenate(behind, axis=0)

    kept = []
    sides = [kv // 2, 1 - kv // 2]
    all_gates = [gates(side) for side in sides]
    for group, side in enumerate(sides):
        write_gate, decay, growth, fading, shrink = all_gates[group]
        arrived(f"part0{group}", part_send.at[0, pl.ds(0, 3 + group)])
        query, key_in = by_head(0, side)
        query_unit = (
            query
            * lax.rsqrt(jnp.sum(query * query, axis=1, keepdims=True) + EPSILON)
            * (1.0 / math.sqrt(HEAD))
        )
        key_unit = key_in * lax.rsqrt(
            jnp.sum(key_in * key_in, axis=1, keepdims=True) + EPSILON
        )
        products = dot_fine(jnp.concatenate([key_unit, query_unit], axis=0), key_unit, True)
        lower = jnp.where(strict, write_gate * decay * products[:size], 0.0)
        scores = products[size:] * decay
        key_grown = (write_gate * growth) * key_unit
        query_grown = query_unit * growth
        key_terms, query_terms = [], []
        for head in range(heads):
            at = slice(head * BLK, (head + 1) * BLK)
            high, low = cut_terms(jnp.concatenate([key_grown[at], query_grown[at]], axis=0))
            both = jnp.concatenate([high, low], axis=0).astype(BF16)
            result = dot(both, state_high[side * heads + head])
            result = result[: 2 * BLK] + result[2 * BLK :]
            result = result + dot(both[: 2 * BLK], state_low[side * heads + head])
            key_terms.append(result[:BLK])
            query_terms.append(result[BLK:])
            for token in range(BLK):
                place = head * BLK + slots * (token % 2) + token // 2
                spread_cols[1, head, token] = jnp.broadcast_to(
                    scores[at, place : place + 1], (BLK, HEAD)
                )
                if token < BLK - 1:
                    spread_cols[0, head, token] = jnp.broadcast_to(
                        lower[at, place : place + 1], (BLK, HEAD)
                    )
        arrived(f"part1{group}", part_send.at[1, pl.ds(0, 3 + group)])
        value, gating = by_head(1, side)
        updates, attends = [], []
        for head in range(heads):
            at = slice(head * BLK, (head + 1) * BLK)
            solved = (write_gate * value)[at] - key_terms[head]
            attend = query_terms[head]
            for token in range(BLK):
                place = slots * (token % 2) + token // 2
                known = jnp.broadcast_to(solved[place : place + 1], (BLK, HEAD))
                attend = attend + spread_cols[1, head, token] * known
                if token < BLK - 1:
                    solved = solved - spread_cols[0, head, token] * known
            updates.append(solved)
            attends.append(attend)
        attend = jnp.concatenate(attends, axis=0)
        normed = attend * lax.rsqrt(jnp.mean(attend * attend, axis=1, keepdims=True) + EPSILON)
        normed = normed * jax.nn.silu(gating) * live
        even, odd = [
            jnp.concatenate(
                [
                    normed[(first + at) * BLK : (first + at + 1) * BLK]
                    for at in range(per_chip)
                ],
                axis=1,
            )
            for first in (0, per_chip)
        ]
        heads_send[group, 0] = jnp.where(upper, even, pltpu.roll(odd, slots, 0)).astype(BF16)
        heads_send[group, 1] = jnp.where(upper, pltpu.roll(even, slots, 0), odd).astype(BF16)
        to_all(
            f"heads{group}",
            lambda other, peer: heads_send.at[group, lax.rem(cls + other + me, 2)],
            lambda other: heads_recv.at[side, me],
        )
        heads_recv[side, me] = heads_send[group, lax.rem(cls + me, 2)]
        kept.append((key_unit * fading, updates, shrink))

    for side, (faded, updates, shrink) in zip(sides, kept):
        for head in range(heads):
            at = slice(head * BLK, (head + 1) * BLK)
            key_high, key_low = cut_terms(faded[at])
            value_high, value_low = cut_terms(updates[head])
            outer = lax.dot_general(
                jnp.concatenate([key_high, key_high, key_low], axis=0).astype(BF16),
                jnp.concatenate([value_high, value_low, value_high], axis=0).astype(BF16),
                (((0,), (0,)), ((), ())),
                preferred_element_type=F32,
            )
            index = side * heads + head
            state_out[0, index] = shrink[head * BLK : head * BLK + 1] * state[index] + outer

    def hand_off(group, off):
        chip = swapped(off)
        for other in (0, 1):
            core = core_of(chip, other)
            remote(
                f"fin{group}", fin_send.at[group, off, core],
                fin_recv.at[group, off, other], chip, core,
            )

    def hand_own(group):
        to_partner(f"own{group}", own_send.at[group, 1 - tp], own_recv.at[group])

    def second_down(group, hidden, source, at_once):
        alone = [(far_first[0],), (far_first[1], far_first[2]), (0,)]
        for pair in alone if at_once else pairs:
            chips = [swapped(off) for off in pair]
            for off, chip, term in zip(pair, chips, columns_of(hidden, down2, chips)):
                if off is alone[2][0]:
                    term = source.astype(F32) + 0.5 * term
                    own_send[group, 0] = term[:, :cols]
                    own_send[group, 1] = term[:, cols:]
                    continue
                fin_send[group, off, 0] = term[:, :cols].astype(BF16)
                fin_send[group, off, 1] = term[:, cols:].astype(BF16)
                if at_once:
                    hand_off(group, off)
        if at_once:
            hand_own(group)

    def take_in(group):
        arrived(f"own{group}", own_recv.at[group])
        arrived(f"fin{group}", fin_recv.at[group, pl.ds(1, kv_size - 1)])
        sums = [own_send[group, tp], own_recv[group]]
        for other in (0, 1):
            total = fin_recv[group, 1, other].astype(F32)
            for off in range(2, kv_size):
                total = total + fin_recv[group, off, other].astype(F32)
            sums[other] = sums[other] + 0.5 * total
        return [total.astype(BF16) for total in sums]

    loaded("gains2")
    loaded("units2", units2)
    arrived("middle1", middle.at[1, pl.ds(0, kv_size - 1)])
    values = jnp.concatenate([middle[1, chip] for chip in range(kv_size)], axis=1).astype(F32)
    squares = jnp.sum(values * values, axis=1, keepdims=True)
    dead_hidden = finish(dot((values * gains2_ref[...]).astype(BF16), units2[...]), squares)

    loaded("down2")
    second_down(1, dead_hidden, middle[1, kv], False)
    for group in range(2):
        arrived(f"heads{group}", heads_recv.at[0, pl.ds(0, devices - 1)])
    arrived("out", out_w.at[:, own_cols])
    blocks = heads_recv[...].astype(F32).reshape(devices * 2 * BLK, wide).astype(BF16)
    mixed = dot(gather_heads, blocks).astype(BF16)
    terms = []
    for part in range(2):
        chips = range(part * kv_size // 2, (part + 1) * kv_size // 2)
        left = jnp.concatenate([mixed[chip * pack : (chip + 1) * pack] for chip in chips], axis=1)
        right = out_w[chips[0] * wide : (chips[-1] + 1) * wide, :]
        terms.append(dot(left, right).astype(BF16).astype(F32))
    second_in[kv] = (middle[0, kv].astype(F32) + (terms[0] + terms[1])).astype(BF16)
    to_class("second", lambda off: second_in.at[kv], lambda off: second_in.at[kv], kv_size)

    squares = jnp.zeros((pack, 1), F32)
    for index, off in enumerate([0] + near_first):
        chip = swapped(off)
        if index:
            arrived("second", second_in.at[chip], off)
        square, total = ffn_slot(
            live_acc, units2, gains2_ref, chip, second_in[chip], index
        )
        squares = squares + square
        if index == 1:
            for off in far_first:
                hand_off(1, off)
            hand_own(1)
    hidden = finish(total, squares)
    second_down(0, hidden, second_in[kv], True)
    dead_sums = take_in(1)
    live_sums = take_in(0)
    packed_out[...] = jnp.concatenate(
        [live_sums[0], dead_sums[0], live_sums[1], dead_sums[1]], axis=0
    )
    all_sent("proj", proj.at[:, 0 : 4 * cols])
    all_sent("small", small_acc.at[0])
    all_sent("heads", heads_recv.at[:, pl.ds(0, devices - 1)])
    all_sent("second", second_in.at[pl.ds(0, kv_size - 1)])
    all_sent("middle", middle.at[:, pl.ds(0, kv_size - 1)])
    all_sent("part", part_send.at[:, pl.ds(0, devices - 1)])
    all_sent("fin", fin_send.at[:, pl.ds(1, kv_size - 1)])
    all_sent("own", own_send.at[0])


def fused_call(mesh, *args):
    (
        tokens, lengths, state, gain_first, first_gate, first_up, first_down, gain_mix,
        query_weight, key_weight, value_weight, gating_weight, write_weight, forget_weight,
        forget_rate, out_weight, gain_second, second_gate, second_up, second_down,
    ) = args
    kv_size = mesh.shape["kv"]
    devices = kv_size * mesh.shape["tp"]
    rows, cols = tokens.shape
    wide = 2 * cols
    channels = gain_first.shape[0]
    hidden_local = first_gate.shape[1]
    half, pack = rows // 2, rows // 4
    in_hbm = pl.BlockSpec(memory_space=pltpu.HBM)
    in_vmem = pl.BlockSpec(memory_space=pltpu.VMEM)
    dma = pltpu.SemaphoreType.DMA
    operands = (
        tokens, lengths.reshape(1, 1), gain_first.reshape(1, -1), gain_mix.reshape(1, -1),
        gain_second.reshape(1, -1), forget_rate.reshape(1, -1), state,
        first_gate, first_up, first_down, query_weight, key_weight, value_weight,
        gating_weight, write_weight.T, forget_weight.T, out_weight, second_gate, second_up,
        second_down,
    )
    operands = [
        array if array.dtype == jnp.int32 else pltpu.with_memory_space_constraint(array, pltpu.HBM)
        for array in operands
    ]
    results = pl.pallas_call(
        functools.partial(fused_kernel, kv_size, channels),
        out_shape=(
            pltpu.VMEM(tokens.shape, tokens.dtype),
            pltpu.VMEM((rows, rows), BF16),
            pltpu.VMEM(state.shape, state.dtype),
        ),
        in_specs=[in_hbm] * len(operands),
        out_specs=(in_vmem, in_vmem, in_vmem),
        scratch_shapes=[
            pltpu.VMEM((channels, 2 * hidden_local), BF16),
            pltpu.VMEM((hidden_local, channels), BF16),
            pltpu.VMEM((channels, 2 * hidden_local), BF16),
            pltpu.VMEM((hidden_local, channels), BF16),
            pltpu.VMEM((channels, 4 * wide), BF16),
            pltpu.VMEM((channels, wide), BF16),
            pltpu.VMEM((HEAD, channels), BF16),
            pltpu.VMEM(state.shape[1:], F32),
            pltpu.VMEM(state.shape[1:], BF16),
            pltpu.VMEM(state.shape[1:], BF16),
            pltpu.VMEM((1, channels), F32),
            pltpu.VMEM((1, channels), F32),
            pltpu.VMEM((1, channels), F32),
            pltpu.VMEM((1, HEADS), F32),
            pltpu.VMEM((rows, cols), BF16),
            pltpu.VMEM((1, 1), jnp.int32),
            pltpu.VMEM((devices, 1, HEAD), jnp.int32),
            pltpu.VMEM((2, half, cols), BF16),
            pltpu.VMEM((devices, half, cols), BF16),
            pltpu.VMEM((half, 2 * hidden_local), F32),
            pltpu.VMEM((pack, 2 * hidden_local), F32),
            pltpu.VMEM((pack, 4 * wide), F32),
            pltpu.VMEM((1, pack, HEAD), F32),
            pltpu.VMEM((2, kv_size, pack, wide), BF16),
            pltpu.VMEM((kv_size, pack, wide), BF16),
            pltpu.VMEM((2, 2, BLK, wide), BF16),
            pltpu.VMEM((2, devices, BLK, wide), BF16),
            pltpu.VMEM((2, kv_size, pack, wide), BF16),
            pltpu.VMEM((2, kv_size, pack, wide), BF16),
            pltpu.VMEM((2, devices, BLK, wide), BF16),
            pltpu.VMEM((2, kv_size, 2, BLK, wide), BF16),
            pltpu.VMEM((1, pack, HEAD), F32),
            pltpu.VMEM((2, kv_size, 2, pack, cols), BF16),
            pltpu.VMEM((2, kv_size, 2, pack, cols), BF16),
            pltpu.VMEM((2, 2, pack, cols), F32),
            pltpu.VMEM((2, pack, cols), F32),
            pltpu.VMEM((2, HEADS // 2, BLK, BLK, HEAD), F32),
            dma((kv_size + 7,)),
            dma((8,)),
            dma((2 * kv_size + 11,)),
        ],
        compiler_params=pltpu.CompilerParams(
            collective_id=0, has_side_effects=True, vmem_limit_bytes=VMEM_LIMIT
        ),
    )(*operands)
    return hand_out(*results)


def hand_out_kernel(packed, order, state, mixed_hbm, state_hbm, mixed, sems):
    puts = [pltpu.make_async_copy(state, state_hbm, sems.at[0])]
    puts[0].start()
    restored = jnp.dot(order[...], packed[...], preferred_element_type=F32)
    mixed[...] = restored.astype(BF16)
    puts.append(pltpu.make_async_copy(mixed, mixed_hbm, sems.at[1]))
    puts[-1].start()
    for put in puts:
        put.wait()


def hand_out(packed, order, new_state):
    in_hbm = pl.BlockSpec(memory_space=pltpu.HBM)
    in_vmem = pl.BlockSpec(memory_space=pltpu.VMEM)
    arrays = [
        pltpu.with_memory_space_constraint(array, pltpu.VMEM)
        for array in (packed, order, new_state)
    ]
    return pl.pallas_call(
        hand_out_kernel,
        out_shape=(
            jax.ShapeDtypeStruct(packed.shape, packed.dtype),
            jax.ShapeDtypeStruct(new_state.shape, new_state.dtype),
        ),
        in_specs=[in_vmem] * 3,
        out_specs=(in_hbm, in_hbm),
        scratch_shapes=[
            pltpu.VMEM(packed.shape, packed.dtype),
            pltpu.SemaphoreType.DMA((2,)),
        ],
        compiler_params=pltpu.CompilerParams(vmem_limit_bytes=8 * 1024 * 1024),
    )(*arrays)


def fits_fused(mesh, args):
    tokens, lengths, state, first_gate = args[0], args[1], args[2], args[4]
    rows, cols = tokens.shape
    kv_size = mesh.shape["kv"]
    devices = kv_size * mesh.shape["tp"]
    return (
        mesh.shape["tp"] == 2
        and mesh.shape["kv"] & (mesh.shape["kv"] - 1) == 0
        and lengths.shape[0] == 1
        and rows == devices * BLK
        and devices * 2 * BLK == HEAD
        and kv_size * BLK // 2 == 2 * BLK
        and devices * cols == HEADS * HEAD
        and cols % 256 == 0
        and first_gate.shape[1] % 128 == 0
        and state.shape[1:] == (HEADS, HEAD, HEAD)
    )


def solution(mesh):
    in_specs = (
        P("dp", ("kv", "tp")),
        P(("dp", "kv", "tp")),
        P(("dp", "kv", "tp"), None, None, None),
        P(),
        P(None, "kv"),
        P(None, "kv"),
        P("kv", None),
        P(),
        P(None, ("kv", "tp")),
        P(None, ("kv", "tp")),
        P(None, ("kv", "tp")),
        P(None, ("kv", "tp")),
        P(),
        P(),
        P(),
        P(None, ("kv", "tp")),
        P(),
        P(None, "kv"),
        P(None, "kv"),
        P("kv", None),
    )
    out_specs = (P("dp", ("kv", "tp")), P(("dp", "kv", "tp"), None, None, None))

    def body(*args):
        if fits_fused(mesh, args):
            return fused_call(mesh, *args)
        return per_device(*args)

    return jax.shard_map(
        body, mesh=mesh, in_specs=in_specs, out_specs=out_specs, check_vma=False
    )
```
